32 devices in a mesh: sp: 4 (over z), fs: 4 (over y, x), tp: 2 (over core).
Axes of the slice: x: 2, y: 2, z: 4, core: 2. Of those that a mesh axis runs over, the one named last changes fastest.
Arguments:
- tokens: bfloat16 [4, 1024, 2048], P('fs', 'sp'), may hold values from -6 to 6
- norm_gain: float32 [2048], replicated, may hold values from 0.1 to 1.9
- pool_input: bfloat16 [2048, 2048], P(('sp', 'fs'), 'tp'), may hold values from -0.125 to 0.125
- query_weight: bfloat16 [2048, 2048], P(('sp', 'fs'), 'tp'), may hold values from -20 to 20
- key_weight: bfloat16 [2048, 2048], P(('sp', 'fs'), 'tp'), may hold values from -1 to 1
- value_weight: bfloat16 [2048, 2048], P(('sp', 'fs'), 'tp'), may hold values from -0.125 to 0.125
- pool_map: bfloat16 [8, 256, 256], P('tp'), may hold values from -0.375 to 0.375
- pool_scale: float32 [2048], P('tp'), may hold values from 0.1 to 1.9
- head_gain: float32 [256], replicated, may hold values from 0.1 to 1.9
- diff_lambda: float32 [8], replicated, may hold values from 0.3 to 0.8
- out_pool: bfloat16 [2048, 2048], P('tp', ('sp', 'fs')), may hold values from -0.09375 to 0.09375
- out_heads: bfloat16 [2048, 2048], P('tp', ('sp', 'fs')), may hold values from -0.09375 to 0.09375
Outputs:
- layer_out: bfloat16 [4, 1024, 2048], P('fs', 'sp', 'tp')
The draws below stay inside these ranges and needn't reach their ends.
All inputs are finite; a program needn't handle non-finite values.
Results may differ from the reference program's by a relative error of at most 0.018.
Values may be sent and summed in bfloat16 or wider, within the bound.
A program may use at most 64 MiB of HBM per device.

```python
import math
import jax
import jax.numpy as jnp
from jax import lax

D = 2048
HEADS = 8
HEAD_DIM = 128
POOL_GROUPS = 8
GROUP_DIM = 256
POOL_WIDTH = 2048
SEQ = 1024
SEQS = 4
N_TP = 2


def key_matrix(key):
    normal_part = jax.random.truncated_normal(jax.random.fold_in(key, 11), -6.0, 6.0, (D, 2 * HEADS * HEAD_DIM), jnp.float32)
    return normal_part * D ** (-0.5)


def draw_key_weight(key, part):
    return key_matrix(key).astype(jnp.bfloat16)


def draw_query_weight(key, part):
    normal_part = jax.random.truncated_normal(jax.random.fold_in(key, 12), -6.0, 6.0, (D, 2 * HEADS * HEAD_DIM), jnp.float32)
    result = normal_part * (3.0 / D) ** 0.5
    return result.astype(jnp.bfloat16)


def levels(key, shape, cuts, smallest, high):
    loudness, own = 1.0, jax.random.fold_in(key, 6)
    for dim, shards_of in cuts:
        draws = jnp.exp(jax.random.uniform(jax.random.fold_in(own, dim), (shards_of,), jnp.float32, smallest / len(cuts), high / len(cuts)))
        loudness = loudness * jnp.repeat(draws, shape[dim] // shards_of).reshape([-1 if axis == dim else 1 for axis in range(len(shape))])
    return loudness


def normal_values(key, extent, spread, limit, split=(), kind=jnp.bfloat16):
    array = jax.random.normal(key, extent, jnp.float32) * spread
    if len(split) > 0:
        array = levels(key, extent, split, -0.22, 0.18) * array
    return jnp.clip(array, min=-limit, max=limit).astype(kind)


def setup_inputs(seed: int = 0) -> dict:
    arg_keys = jax.random.split(jax.random.key(seed), 13)
    return {
        "tokens": normal_values(arg_keys[0], (SEQS, SEQ, D), 1.0, 6.0, ((0, 4), (1, 4))),
        "norm_gain": jnp.clip(1.0 + 0.18 * jax.random.normal(arg_keys[1], (D,), jnp.float32), 0.1, 1.9),
        "pool_input": normal_values(arg_keys[2], (D, POOL_WIDTH), D ** -0.5, 0.125, ((0, 16), (1, 2))),
        "query_weight": draw_query_weight(jax.random.fold_in(arg_keys[12], 71), 0),
        "key_weight": draw_key_weight(jax.random.fold_in(arg_keys[12], 71), 0),
        "value_weight": normal_values(arg_keys[5], (D, 2 * HEADS * HEAD_DIM), D ** -0.5, 0.125, ((0, 16), (1, 2))),
        "pool_map": normal_values(arg_keys[6], (POOL_GROUPS, GROUP_DIM, GROUP_DIM), GROUP_DIM ** -0.5, 0.375, ((0, 2),)),
        "pool_scale": jnp.clip(1.0 + 0.18 * jax.random.normal(arg_keys[7], (POOL_WIDTH,), jnp.float32), 0.1, 1.9),
        "head_gain": jnp.clip(1.0 + 0.18 * jax.random.normal(arg_keys[8], (2 * HEAD_DIM,), jnp.float32), 0.1, 1.9),
        "diff_lambda": jnp.clip(jax.random.uniform(arg_keys[9], (HEADS,), jnp.float32, 0.3, 0.8), 0.3, 0.8),
        "out_pool": normal_values(arg_keys[10], (POOL_WIDTH, D), (POOL_WIDTH + 2 * HEADS * HEAD_DIM) ** -0.5, 0.09375, ((0, 2), (1, 16))),
        "out_heads": normal_values(arg_keys[11], (2 * HEADS * HEAD_DIM, D), (POOL_WIDTH + 2 * HEADS * HEAD_DIM) ** -0.5, 0.09375, ((0, 2), (1, 16))),
    }


THETA = 500000.0
HEAD_SCALE = 0.8
NORM_EPS = 1e-06
HEAD_EPS = 1e-05

def rotate(tensor, positions):
    half = HEAD_DIM // 2
    freqs = 1.0 / THETA ** (jnp.arange(half, dtype=jnp.float32) * 2.0 / HEAD_DIM)
    angles = positions[:, None] * freqs[None, :]
    cosine = jnp.cos(angles)[:, None, None, :]
    sine = jnp.sin(angles)[:, None, None, :]
    floated = tensor.astype(jnp.float32)
    first = floated[..., :half]
    second = floated[..., half:]
    turned = jnp.concatenate([first * cosine - second * sine, second * cosine + first * sine], -1)
    return turned.astype(jnp.bfloat16)

def one_sequence(seq_tokens, norm_gain, pool_input, query_weight, key_weight, value_weight, pool_map, pool_scale, head_gain, diff_lambda, out_pool, out_heads):
    length = seq_tokens.shape[0]
    floated = seq_tokens.astype(jnp.float32)
    normed = (floated * lax.rsqrt(lax.optimization_barrier(jnp.mean(floated * floated, -1, keepdims=True)) + NORM_EPS) * norm_gain).astype(jnp.bfloat16)
    pool_in = jnp.dot(normed, pool_input, preferred_element_type=jnp.float32).astype(jnp.bfloat16)
    queries = jnp.dot(normed, query_weight, preferred_element_type=jnp.float32).astype(jnp.bfloat16)
    keys_all = jnp.dot(normed, key_weight, preferred_element_type=jnp.float32).astype(jnp.bfloat16)
    values = jnp.dot(normed, value_weight, preferred_element_type=jnp.float32).astype(jnp.bfloat16)
    positions = jnp.arange(length, dtype=jnp.float32)
    queries = rotate(queries.reshape(length, HEADS, 2, HEAD_DIM), positions)
    keys_all = rotate(keys_all.reshape(length, HEADS, 2, HEAD_DIM), positions)
    values = values.reshape(length, HEADS, 2 * HEAD_DIM)
    span = math.gcd(length, 512)

    def one_head(operands):
        query_head, key_head, value_head, lambda_head = operands
        key_float = key_head.astype(jnp.float32)
        value_float = value_head.astype(jnp.float32)

        def one_block(begin):
            query_block = lax.dynamic_slice_in_dim(query_head, begin, span, 0).astype(jnp.float32)
            scores = jnp.einsum('qcd,kcd->cqk', query_block, key_float) * HEAD_DIM ** (-0.5)
            query_pos = begin + jnp.arange(span, dtype=jnp.int32)
            key_pos = jnp.arange(length, dtype=jnp.int32)
            scores = jnp.where(query_pos[:, None] >= key_pos[None, :], scores, -jnp.inf)
            largest = lax.optimization_barrier(jnp.max(scores, -1, keepdims=True))
            expons = jnp.exp(scores - largest)
            totals = lax.optimization_barrier(jnp.sum(expons, -1))
            expons_low = expons.astype(jnp.bfloat16).astype(jnp.float32)
            map_values = jnp.einsum('cqk,ke->cqe', expons_low, value_float)
            return map_values[0] / totals[0][:, None] - lambda_head * map_values[1] / totals[1][:, None]
        begins = jnp.arange(length // span, dtype=jnp.int32) * span
        return lax.map(one_block, begins).reshape(length, 2 * HEAD_DIM)
    heads_raw = lax.map(one_head, (jnp.moveaxis(queries, 1, 0), jnp.moveaxis(keys_all, 1, 0), jnp.moveaxis(values, 1, 0), diff_lambda))
    heads_raw = jnp.moveaxis(heads_raw, 0, 1)
    attn = (heads_raw * lax.rsqrt(lax.optimization_barrier(jnp.mean(heads_raw * heads_raw, -1, keepdims=True)) + HEAD_EPS) * head_gain * HEAD_SCALE).astype(jnp.bfloat16).reshape(length, 2 * HEADS * HEAD_DIM)
    grouped = pool_in.reshape(length, POOL_GROUPS, GROUP_DIM).astype(jnp.float32)
    running = jnp.concatenate([jnp.zeros((1, POOL_GROUPS, GROUP_DIM), jnp.float32), jnp.cumsum(grouped, 0)], 0)
    windows = 2 ** (1 + jnp.arange(POOL_GROUPS, dtype=jnp.int32) % 4)
    places = jnp.arange(length, dtype=jnp.int32)[:, None]
    lowest = jnp.maximum(places + 1 - windows[None, :], 0)
    counts = jnp.minimum(places + 1, windows[None, :]).astype(jnp.float32)
    low_sums = running[lowest, jnp.arange(POOL_GROUPS, dtype=jnp.int32)[None, :]]
    window_mean = (running[1:] - low_sums) / counts[:, :, None]
    pool_mixed = (window_mean - grouped).astype(jnp.bfloat16)
    pooled = (jnp.einsum('sgc,gce->sge', pool_mixed.astype(jnp.float32), pool_map.astype(jnp.float32)) * pool_scale.reshape(POOL_GROUPS, GROUP_DIM)).astype(jnp.bfloat16).reshape(length, POOL_WIDTH)
    pool_cols = POOL_WIDTH // N_TP
    head_cols = 2 * HEADS * HEAD_DIM // N_TP
    summed = jnp.zeros((length, D), jnp.float32)
    for shard_index in range(N_TP):
        pool_part = pooled[:, shard_index * pool_cols:(shard_index + 1) * pool_cols]
        head_part = attn[:, shard_index * head_cols:(shard_index + 1) * head_cols]
        partial_value = jnp.dot(pool_part, out_pool[shard_index * pool_cols:(shard_index + 1) * pool_cols], preferred_element_type=jnp.float32) + jnp.dot(head_part, out_heads[shard_index * head_cols:(shard_index + 1) * head_cols], preferred_element_type=jnp.float32)
        rounded = lax.optimization_barrier(partial_value.astype(jnp.bfloat16))
        summed = summed + rounded.astype(jnp.float32)
    return summed.astype(jnp.bfloat16)

def reference(tokens, norm_gain, pool_input, query_weight, key_weight, value_weight, pool_map, pool_scale, head_gain, diff_lambda, out_pool, out_heads):

    def apply_one(seq_tokens):
        return one_sequence(seq_tokens, norm_gain, pool_input, query_weight, key_weight, value_weight, pool_map, pool_scale, head_gain, diff_lambda, out_pool, out_heads)
    return lax.map(apply_one, tokens)
```

```python
import math

import jax
import jax.numpy as jnp
import numpy as np
from jax import lax
from jax.experimental import pallas as pl
from jax.experimental.pallas import tpu as pltpu
from jax.sharding import PartitionSpec as P

HEAD_DIM = 128
GROUP_DIM = 256


THETA = 500000.0
HEAD_SCALE = 0.8
NORM_EPS = 1e-06
HEAD_EPS = 1e-05


def from_behind(value, axis, steps):
    count = lax.axis_size(axis)
    first, last = (max(0, -steps), min(count, count - steps))
    return lax.ppermute(value, axis, [(source, source + steps) for source in range(first, last)])


def rotate(tensor, positions):
    half = HEAD_DIM // 2
    freqs = 1.0 / THETA ** (jnp.arange(half, dtype=jnp.float32) * 2.0 / HEAD_DIM)
    angles = positions[:, None] * freqs[None, :]
    cosine = jnp.cos(angles)[:, None, None, :]
    sine = jnp.sin(angles)[:, None, None, :]
    floated = tensor.astype(jnp.float32)
    first = floated[..., :half]
    second = floated[..., half:]
    turned = jnp.concatenate([first * cosine - second * sine, second * cosine + first * sine], -1)
    return turned.astype(jnp.bfloat16)


def local(
    tokens,
    norm_gain,
    pool_input,
    query_weight,
    key_weight,
    value_weight,
    pool_map,
    pool_scale,
    head_gain,
    diff_lambda,
    out_pool,
    out_heads,
):
    out_local = jnp.concatenate([out_pool, out_heads], 0)
    row_count = tokens.shape[1]
    floated = tokens[0].astype(jnp.float32)
    normed = (
        floated * lax.rsqrt(jnp.mean(floated * floated, -1, keepdims=True) + NORM_EPS) * norm_gain
    ).astype(jnp.bfloat16)
    fragments = (
        lax.all_gather(pool_input, ("sp", "fs"), axis=0, tiled=True),
        lax.all_gather(query_weight, ("sp", "fs"), axis=0, tiled=True),
        lax.all_gather(key_weight, ("sp", "fs"), axis=0, tiled=True),
        lax.all_gather(value_weight, ("sp", "fs"), axis=0, tiled=True),
    )
    projected = tuple(
        (jnp.dot(normed, fragment, preferred_element_type=jnp.float32) for fragment in fragments)
    )
    pool_in, queries, keys_flat, values_flat = [
        product.astype(jnp.bfloat16) for product in projected
    ]
    head_count = values_flat.shape[1] // (2 * HEAD_DIM)
    tp_index = lax.axis_index("tp")
    sp_index = lax.axis_index("sp")
    query_pos = sp_index * row_count + jnp.arange(row_count, dtype=jnp.int32)
    positions = query_pos.astype(jnp.float32)
    queries = rotate(queries.reshape(row_count, head_count, 2, HEAD_DIM), positions)
    keys_flat = rotate(keys_flat.reshape(row_count, head_count, 2, HEAD_DIM), positions).reshape(
        row_count, head_count * 2 * HEAD_DIM
    )
    lambdas = lax.dynamic_slice_in_dim(diff_lambda, tp_index * head_count, head_count, 0)

    def online_step(state, key_rows, value_rows, key_offset):
        largest, summed, accum = state
        width = key_rows.shape[0]
        shaped = key_rows.reshape(width, head_count, 2, HEAD_DIM)
        scores = jnp.einsum(
            "qhcd,khcd->chqk", queries, shaped, preferred_element_type=jnp.float32
        ) * HEAD_DIM ** (-0.5)
        key_pos = key_offset + jnp.arange(width, dtype=jnp.int32)
        scores = jnp.where(query_pos[:, None] >= key_pos[None, :], scores, -jnp.inf)
        newest = jnp.maximum(largest, jnp.max(scores, -1))
        anchor = jnp.where(jnp.isfinite(newest), newest, 0.0)
        rescale = jnp.exp(largest - anchor)
        expons = jnp.exp(scores - anchor[..., None])
        summed = summed * rescale + jnp.sum(expons, -1)
        value_shaped = value_rows.reshape(width, head_count, 2 * HEAD_DIM)
        added = jnp.einsum(
            "chqk,khe->chqe",
            expons.astype(jnp.bfloat16),
            value_shaped,
            preferred_element_type=jnp.float32,
        )
        accum = accum * rescale[..., None] + added
        return (newest, summed, accum)

    start_state = (
        jnp.full((2, head_count, row_count), -jnp.inf, jnp.float32),
        jnp.zeros((2, head_count, row_count), jnp.float32),
        jnp.zeros((2, head_count, row_count, 2 * HEAD_DIM), jnp.float32),
    )
    fragments = (
        lax.all_gather(keys_flat, "sp", axis=0, tiled=True),
        lax.all_gather(values_flat, "sp", axis=0, tiled=True),
    )
    span = math.gcd(fragments[0].shape[0], 1024)

    def inner_step(index, inner_state):
        key_rows = lax.dynamic_slice_in_dim(fragments[0], index * span, span, 0)
        value_rows = lax.dynamic_slice_in_dim(fragments[1], index * span, span, 0)
        return online_step(inner_state, key_rows, value_rows, index * span)

    final_state = lax.fori_loop(0, fragments[0].shape[0] // span, inner_step, start_state)
    summed_final = final_state[1]
    accum_final = final_state[2]
    heads_raw = (
        accum_final[0] / summed_final[0][..., None]
        - lambdas[:, None, None] * accum_final[1] / summed_final[1][..., None]
    )
    heads_raw = jnp.moveaxis(heads_raw, 0, 1)
    attn = (
        (
            heads_raw
            * lax.rsqrt(jnp.mean(heads_raw * heads_raw, -1, keepdims=True) + HEAD_EPS)
            * head_gain
            * HEAD_SCALE
        )
        .astype(jnp.bfloat16)
        .reshape(row_count, head_count * 2 * HEAD_DIM)
    )
    reach = 15
    rim_rows = from_behind(pool_in[row_count - reach :], "sp", 1)
    extended = jnp.concatenate([rim_rows, pool_in], 0).astype(jnp.float32)
    pair_sums = extended[1:] + extended[:-1]
    quad_sums = pair_sums[2:] + pair_sums[:-2]
    octet_sums = quad_sums[4:] + quad_sums[:-4]
    sixteen_sums = octet_sums[8:] + octet_sums[:-8]
    group_count = pool_in.shape[1] // GROUP_DIM
    stacked = jnp.stack(
        [
            pair_sums[14 : 14 + row_count],
            quad_sums[12 : 12 + row_count],
            octet_sums[8 : 8 + row_count],
            sixteen_sums,
        ],
        0,
    ).reshape(4, row_count, group_count, GROUP_DIM)
    levels = (tp_index * group_count + jnp.arange(group_count, dtype=jnp.int32)) % 4
    picked = jnp.sum(
        jnp.where(
            levels[None, None, :, None] == jnp.arange(4, dtype=jnp.int32)[:, None, None, None],
            stacked,
            0.0,
        ),
        0,
    )
    windows = 2 ** (1 + levels)
    counts = jnp.minimum(query_pos[:, None] + 1, windows[None, :]).astype(jnp.float32)
    window_mean = picked / counts[:, :, None]
    grouped = pool_in.reshape(row_count, group_count, GROUP_DIM).astype(jnp.float32)
    pool_mixed = (window_mean - grouped).astype(jnp.bfloat16)
    pooled = (
        (
            jnp.einsum("tgc,gce->tge", pool_mixed, pool_map, preferred_element_type=jnp.float32)
            * pool_scale.reshape(group_count, GROUP_DIM)
        )
        .astype(jnp.bfloat16)
        .reshape(row_count, group_count * GROUP_DIM)
    )
    branches = jnp.concatenate([pooled, attn], 1)
    partial_value = jnp.dot(
        branches,
        lax.all_gather(out_local, ("sp", "fs"), axis=1, tiled=True),
        preferred_element_type=jnp.float32,
    )
    layer_out = lax.psum_scatter(
        partial_value.astype(jnp.bfloat16), "tp", scatter_dimension=1, tiled=True
    )
    return layer_out[None]


MESH = pl.DeviceIdType.MESH
PIECES = 4
PARTS = 2

PROJECTED = ((0, 1, 2, 3), (1, 0, 2, 3), (2, 3, 0, 1), (3, 2, 0, 1))
FINISHED = ((1, 3, 2, 0), (0, 3, 2, 1), (0, 1, 3, 2), (0, 1, 2, 3))
ARRIVALS = ((0, 1, 2, 3), (1, 0, 2, 3), (2, 3, 1, 0), (3, 2, 1, 0))
SENDS = ((0, 1, 2, 3), (1, 3, 2, 0), (2, 0, 1, 3), (3, 2, 1, 0))
SLOTS = tuple(
    tuple(ARRIVALS[to].index(place) for to in SENDS[place]) for place in range(len(SENDS))
)


def pick(row, z):
    value = jnp.int32(row[0])
    for place in range(1, len(row)):
        value = jnp.where(z == place, row[place], value)
    return value


def fused_kernel(
    places,
    groups,
    tokens_ref,
    norm_gain_ref,
    freqs_ref,
    pool_ref,
    query_ref,
    key_ref,
    value_ref,
    map_ref,
    scale_ref,
    gain_ref,
    lambda_ref,
    out_pool_ref,
    out_heads_ref,
    out_ref,
    own_tokens,
    own_map,
    cos_ref,
    sin_ref,
    rows_all,
    weights,
    outs,
    queries,
    keys,
    values,
    pools,
    mine,
    to_mate,
    from_mate,
    kept,
    to_peer,
    from_peer,
    merging,
    final,
    *sems,
):
    (
        own_sem,
        in_local,
        in_z_send,
        in_z_recv,
        in_n_send,
        in_n_recv,
        in_f_send,
        in_f_recv,
        out_local,
        out_z_send,
        out_z_recv,
        out_n_send,
        out_n_recv,
        out_f_send,
        out_f_recv,
        right_send,
        right_recv,
        left_send,
        left_recv,
        mate_send,
        mate_recv,
        half_send,
        half_recv,
        peer_send,
        peer_recv,
        merge_send,
        merge_recv,
    ) = sems
    z = lax.axis_index("sp")
    f = lax.axis_index("fs")
    c = lax.axis_index("tp")
    fx = f + 1 - 2 * lax.rem(f, 2)
    fy = lax.rem(f + 2, groups)
    mate = 1 - c
    half_rows = tokens_ref.shape[0] // 2
    row_count = 2 * half_rows
    depth = pool_ref.shape[0]
    width = GROUP_DIM
    out_width = out_pool_ref.shape[1]
    half_out = out_ref.shape[1]
    length = places * row_count

    send_to = [pick([row[d] for row in SENDS], z) for d in range(places)]
    send_slot = [pick([row[d] for row in SLOTS], z) for d in range(places)]
    source = [pick([row[d] for row in ARRIVALS], z) for d in range(places)]

    def block(index, size):
        return pl.ds(pl.multiple_of(index * size, size), size)

    barrier = pltpu.get_barrier_semaphore()
    partners = [{"sp": lax.rem(z + d, places)} for d in range(1, places)]
    partners += [{"fs": fx}, {"fs": fy}, {"tp": mate}]
    for partner in partners:
        pl.semaphore_signal(barrier, inc=1, device_id=partner, device_id_type=MESH)

    def remote(source, target, send, recv, device):
        return pltpu.make_async_remote_copy(
            src_ref=source,
            dst_ref=target,
            send_sem=send,
            recv_sem=recv,
            device_id=device,
            device_id_type=MESH,
        )

    class Gather:
        def __init__(self, sources, cut, view, group):
            self.sources, self.cut, self.view = sources, cut, view
            self.count = len(sources)
            (
                self.local,
                self.z_send,
                self.z_recv,
                self.n_send,
                self.n_recv,
                self.f_send,
                self.f_recv,
            ) = group
            self.low = (0, self.count // 2)
            self.high = (self.count // 2, self.count - self.count // 2)

        def own(self, m):
            return pltpu.make_async_copy(
                self.cut(self.sources[m], z), self.view(z, f, m, 1).at[0], self.local.at[m]
            )

        def across(self, d, m):
            to, slot = send_to[d], send_slot[d]
            return remote(
                self.cut(self.sources[m], to),
                self.view(z, f, m, 1).at[0],
                self.z_send.at[d, m],
                self.z_recv.at[slot, m],
                {"sp": to},
            )

        def arrive(self, d, m):
            view = self.view(source[d], f, m, 1).at[0]
            return remote(
                view, view, self.z_send.at[d, m], self.z_recv.at[d, m], {"sp": source[d]}
            )

        def near(self, d, side, column, half):
            start, size = (self.low, self.high)[half]
            view = self.view(source[d], column, start, size)
            return remote(
                view,
                view,
                self.n_send.at[side, 2 * d + half],
                self.n_recv.at[side, 2 * d + half],
                {"fs": (fx, fy)[side]},
            )

        def forward(self, d, side, column):
            start, size = (self.high, self.low)[side]
            view = self.view(source[d], column, start, size)
            return remote(
                view,
                view,
                self.f_send.at[side, d],
                self.f_recv.at[side, d],
                {"fs": (fx, fy)[side]},
            )

        def start_own(self):
            for m in range(self.count):
                self.own(m).start()

        def start(self, d):
            for m in range(self.count):
                self.across(d, m).start()

        def first(self, d):
            for m in range(self.count):
                if d == 0:
                    self.own(m).wait()
                else:
                    self.arrive(d, m).wait_recv()
            for order in range(2):
                for side in range(2):
                    self.near(d, side, f, side ^ order).start()

        def second(self, d):
            self.near(d, 0, fx, 0).wait_recv()
            self.forward(d, 1, fx).start()
            self.near(d, 1, fy, 1).wait_recv()
            self.forward(d, 0, fy).start()

        def third(self, d):
            diagonal = lax.rem(fx + 2, groups)
            for side in range(2):
                self.forward(d, side, diagonal).wait_recv()
            self.near(d, 0, fx, 1).wait_recv()
            self.near(d, 1, fy, 0).wait_recv()

        def drain(self):
            for d in range(places):
                for m in range(self.count):
                    if d > 0:
                        self.across(d, m).wait_send()
                for side in range(2):
                    for half in range(2):
                        self.near(d, side, f, half).wait_send()
                self.forward(d, 1, fx).wait_send()
                self.forward(d, 0, fy).wait_send()

    inward = Gather(
        (pool_ref, query_ref, key_ref, value_ref),
        lambda ref, to: ref.at[:, block(to, width)],
        lambda zz, ff, m, n: weights.at[pl.ds(m, n), block(zz * groups + ff, depth), :],
        (in_local, in_z_send, in_z_recv, in_n_send, in_n_recv, in_f_send, in_f_recv),
    )
    outward = Gather(
        (out_pool_ref, out_heads_ref),
        lambda ref, to: ref.at[block(to, width), :],
        lambda zz, ff, m, n: outs.at[pl.ds(m, n), :, block(zz * groups + ff, out_width)],
        (out_local, out_z_send, out_z_recv, out_n_send, out_n_recv, out_f_send, out_f_recv),
    )

    piece_rows = half_rows // PIECES

    def chunk(b, side, p):
        return rows_all.at[block((2 * b + side) * PIECES + p, piece_rows), :]

    def right(b, p, step=1):
        view = chunk(b, c, p)
        return remote(view, view, right_send.at[b, p], right_recv.at[b, p], {"sp": z + step})

    def left(b, p, step=-1):
        view = chunk(b, c, p)
        return remote(view, view, left_send.at[b, p], left_recv.at[b, p], {"sp": z + step})

    def share(b, side, p):
        view = chunk(b, side, p)
        return remote(view, view, mate_send.at[b, p], mate_recv.at[b, p], {"tp": mate})

    def each_place(act):
        for place in range(places):
            pl.when(z == place)(lambda place=place: act(place))

    def own_sends(turn):
        def act(place):
            for p in range(PIECES):
                if (place, turn) in ((places - 1, 0), (1, 1), (2, 2)):
                    left(place, p).start()
                if (place, turn) in ((0, 0), (2, 1)):
                    right(place, p).start()
                if turn == 0:
                    share(place, c, p).start()

        each_place(act)

    def take(place, b, p):
        if b < place:
            right(b, p, -1).wait_recv()
            if place < places - 1:
                right(b, p).start()
        else:
            left(b, p, 1).wait_recv()
            if place > 0:
                left(b, p).start()
        share(b, c, p).start()

    def taken(blocks):
        def act(place):
            b = blocks[place]
            if b is None:
                return
            for p in range(PIECES):
                take(place, b, p)
            if place == 1 and b == 0:
                for p in range(PIECES):
                    right(place, p).start()

        each_place(act)

    tokens_in = pltpu.make_async_copy(
        tokens_ref.at[block(c, half_rows), :], own_tokens, own_sem.at[0]
    )
    map_in = pltpu.make_async_copy(map_ref.at[z], own_map, own_sem.at[1])
    tokens_in.start()
    inward.start_own()
    outward.start_own()
    map_in.start()
    pl.semaphore_wait(barrier, len(partners))
    for d in range(1, places):
        inward.start(d)
    tokens_in.wait()
    floated = own_tokens[...].astype(jnp.float32)
    rows_all[block(2 * z + c, half_rows), :] = (
        floated
        * lax.rsqrt(jnp.mean(floated * floated, -1, keepdims=True) + NORM_EPS)
        * norm_gain_ref[...]
    ).astype(jnp.bfloat16)
    inward.first(0)
    pools[0:16, :] = jnp.zeros((16, width), jnp.bfloat16)
    keys[...] = jnp.zeros_like(keys)
    values[...] = jnp.zeros_like(values)
    own_sends(0)

    def table(index, carry):
        rows = block(index, row_count)
        half = HEAD_DIM // 2
        count = (
            index * row_count + lax.broadcasted_iota(jnp.int32, (row_count, HEAD_DIM), 0)
        ).astype(jnp.float32)
        lane = lax.broadcasted_iota(jnp.int32, (row_count, HEAD_DIM), 1)
        angles = count * freqs_ref[...]
        cos_ref[rows, :] = jnp.cos(angles)
        sine = jnp.sin(angles)
        sin_ref[rows, :] = jnp.where(lane < half, -sine, sine)
        return carry

    lax.fori_loop(0, places, table, 0)

    def turned(raw, cosine, sine):
        floated = raw.astype(jnp.float32)
        return (floated * cosine + pltpu.roll(floated, HEAD_DIM // 2, 1) * sine).astype(
            jnp.bfloat16
        )

    projected = [pick([row[i] for row in PROJECTED], z) for i in range(places)]
    finished = [pick([row[i] for row in FINISHED], z) for i in range(places)]

    def project(index):
        for p in range(PIECES):
            share(index, mate, p).wait_recv()
        rows = block(index, row_count)
        normed = rows_all[rows, :]
        cosine = cos_ref[rows, :]
        sine = sin_ref[rows, :]

        def product(m):
            return jnp.dot(normed, weights[m], preferred_element_type=jnp.float32).astype(
                jnp.bfloat16
            )

        pools[pl.ds(pl.multiple_of(index * row_count + 16, 16), row_count), :] = product(0)
        raw = product(1)
        for m in range(2):
            part = slice(m * HEAD_DIM, (m + 1) * HEAD_DIM)
            queries[rows, part] = turned(raw[:, part], cosine, sine)
        raw = product(2)
        for m in range(2):
            part = slice(m * HEAD_DIM, (m + 1) * HEAD_DIM)
            keys[rows, part] = turned(raw[:, part], cosine, sine)
        values[rows, :] = product(3)

    def project_early(i, carry):
        project(jnp.where(i == 0, projected[0], projected[1]))
        return carry

    inward.first(1)
    own_sends(1)
    inward.second(0)
    inward.first(2)
    for d in range(1, places):
        outward.start(d)
    own_sends(2)
    inward.second(1)
    inward.first(3)
    inward.second(2)
    taken((1, 0, 3, 2))
    inward.second(3)
    outward.first(0)
    outward.first(1)
    taken((None, 2, None, None))
    for d in range(places):
        inward.third(d)
    outward.first(2)
    outward.first(3)
    lax.fori_loop(0, 2, project_early, 0)
    outward.second(0)
    taken((2, None, 0, 0))
    outward.second(1)
    outward.second(2)
    project(projected[2])
    outward.second(3)
    taken((None, 3, 1, None))
    map_in.wait()
    for d in range(places):
        outward.third(d)

    level = lax.rem(c * map_ref.shape[0] + z, 4)
    window = jnp.where(
        level == 0, 2, jnp.where(level == 1, 4, jnp.where(level == 2, 8, 16))
    )
    head_lambda = lambda_ref[c * map_ref.shape[0] + z]

    part_rows = row_count // PARTS

    def to_sibling(step):
        return remote(
            to_mate.at[step],
            from_mate.at[step],
            half_send.at[step],
            half_recv.at[step],
            {"tp": mate},
        )

    outer = (z == 0) | (z == places - 1)
    pair = z + 1 - 2 * lax.rem(z, 2)

    def crossing(to, h):
        return lax.rem(to, 2) * PARTS + h

    def to_inner(to, h):
        return remote(
            to_peer.at[to * PARTS + h],
            merging.at[crossing(to, h)],
            merge_send.at[crossing(to, h)],
            merge_recv.at[crossing(to, h)],
            {"sp": pair},
        )

    def to_place(to, h):
        return remote(
            to_peer.at[to * PARTS + h],
            from_peer.at[h],
            peer_send.at[crossing(to, h)],
            peer_recv.at[h],
            {"sp": to},
        )

    def to_pair(h):
        return remote(
            to_peer.at[pair * PARTS + h],
            from_peer.at[PARTS + h],
            peer_send.at[2 * PARTS + h],
            peer_recv.at[PARTS + h],
            {"sp": pair},
        )

    def step_place(step):
        turn = step // PARTS
        to = finished[places - 1]
        for i in range(places - 1):
            to = jnp.where(turn == i, finished[i], to)
        return to, lax.rem(step, PARTS)

    def compute(step):
        to, h = step_place(step)
        slot = to * PARTS + h
        rows = block(slot, part_rows)
        query_pos = slot * part_rows + lax.broadcasted_iota(jnp.int32, (part_rows, length), 0)
        key_pos = lax.broadcasted_iota(jnp.int32, (part_rows, length), 1)
        seen = query_pos >= key_pos
        mapped = []
        for m in range(2):
            part = slice(m * HEAD_DIM, (m + 1) * HEAD_DIM)
            scores = lax.dot_general(
                queries[rows, part],
                keys[:, part],
                (((1,), (1,)), ((), ())),
                preferred_element_type=jnp.float32,
            ) * HEAD_DIM ** (-0.5)
            scores = jnp.where(seen, scores, -jnp.inf)
            expons = jnp.exp(scores - jnp.max(scores, -1, keepdims=True))
            totals = jnp.sum(expons, -1, keepdims=True)
            mapped.append(
                jnp.dot(
                    expons.astype(jnp.bfloat16), values[...], preferred_element_type=jnp.float32
                )
                / totals
            )
        raw = mapped[0] - head_lambda * mapped[1]
        attn = (
            raw
            * lax.rsqrt(jnp.mean(raw * raw, -1, keepdims=True) + HEAD_EPS)
            * gain_ref[...]
            * HEAD_SCALE
        ).astype(jnp.bfloat16)
        extended = pools[
            pl.ds(pl.multiple_of(slot * part_rows, 16), part_rows + 16), :
        ].astype(jnp.float32)
        picked = extended + pltpu.roll(extended, 1, 0)
        sums = picked
        for shift in (2, 4, 8):
            sums = sums + pltpu.roll(sums, shift, 0)
            picked = lax.select_n(window >= 2 * shift, picked, sums)
        places_of = slot * part_rows + lax.broadcasted_iota(jnp.int32, (part_rows, 1), 0)
        counts = jnp.minimum(places_of + 1, window).astype(jnp.float32)
        mixed = (picked[16:] / counts - extended[16:]).astype(jnp.bfloat16)
        pooled = (
            jnp.dot(mixed, own_map[...], preferred_element_type=jnp.float32) * scale_ref[z]
        ).astype(jnp.bfloat16)

        def partial_of(side):
            columns = block(side, half_out)
            return jnp.dot(
                pooled, outs[0, :, columns], preferred_element_type=jnp.float32
            ) + jnp.dot(attn, outs[1, :, columns], preferred_element_type=jnp.float32)

        to_mate[step] = partial_of(mate).astype(jnp.bfloat16)
        to_sibling(step).start()
        mine[lax.rem(step, 2)] = partial_of(c)

    def finish(step):
        to, h = step_place(step)
        slot = to * PARTS + h
        crosses = to // 2 != z // 2
        to_sibling(step).wait_recv()
        summed = mine[lax.rem(step, 2)] + from_mate[step].astype(jnp.float32)

        @pl.when(to == z)
        def _():
            final[h] = summed

        @pl.when(to == pair)
        def _():
            to_peer[slot] = summed.astype(jnp.bfloat16)
            to_pair(h).start()

        @pl.when(crosses & outer)
        def _():
            to_peer[slot] = summed.astype(jnp.bfloat16)
            to_inner(to, h).start()

        @pl.when(crosses & jnp.logical_not(outer))
        def _():
            kept[crossing(to, h)] = summed

    def merge(turn):
        place = turn // PARTS
        to = jnp.where(z < places // 2, places - 1 - place, place)
        h = lax.rem(turn, PARTS)
        to_inner(to, h).wait_recv()
        to_peer[to * PARTS + h] = (
            kept[crossing(to, h)] + merging[crossing(to, h)].astype(jnp.float32)
        ).astype(jnp.bfloat16)
        to_place(to, h).start()

    upper_inner = z == places // 2

    def body(step, carry):
        @pl.when(step == PARTS)
        def _():
            taken((3, None, None, 1))
            project(projected[3])

        compute(step)

        @pl.when(step > 0)
        def _():
            finish(step - 1)

        @pl.when(upper_inner & (step > 2) & (lax.rem(step, 2) == 1))
        def _():
            merge((step - 3) // 2)

        return carry

    lax.fori_loop(0, places * PARTS, body, 0)
    finish(places * PARTS - 1)

    def merge_more(turn, carry):
        merge(turn)
        return carry

    @pl.when(z == places // 2 - 1)
    def _():
        lax.fori_loop(0, 2 * PARTS, merge_more, 0)

    @pl.when(upper_inner)
    def _():
        merge(2 * PARTS - 1)

    for h in range(PARTS):
        to_pair(h).wait_recv()
        total = final[h] + from_peer[PARTS + h].astype(jnp.float32)
        to_place(z, h).wait_recv()
        out_ref[h * part_rows : (h + 1) * part_rows, :] = (
            total + from_peer[h].astype(jnp.float32)
        ).astype(out_ref.dtype)

    inward.drain()
    outward.drain()

    def drain(place):
        for b in range(places):
            for p in range(PIECES):
                if b <= place < places - 1:
                    right(b, p).wait_send()
                if b >= place > 0:
                    left(b, p).wait_send()
                share(b, c, p).wait_send()
        for h in range(PARTS):
            to_pair(h).wait_send()
            for to in range(places):
                if to // 2 != place // 2:
                    if place in (0, places - 1):
                        to_inner(to, h).wait_send()
                    else:
                        to_place(to, h).wait_send()

    each_place(drain)
    for step in range(places * PARTS):
        to_sibling(step).wait_send()


def fused(
    tokens,
    norm_gain,
    pool_input,
    query_weight,
    key_weight,
    value_weight,
    pool_map,
    pool_scale,
    head_gain,
    diff_lambda,
    out_pool,
    out_heads,
):
    places = lax.axis_size("sp")
    groups = lax.axis_size("fs")
    row_count, model = tokens.shape[1], tokens.shape[2]
    length = places * row_count
    half = HEAD_DIM // 2
    freqs = np.float32(1.0) / np.float32(THETA) ** (
        np.arange(half, dtype=np.float32) * np.float32(2.0) / np.float32(HEAD_DIM)
    )
    freqs = jnp.asarray(np.concatenate([freqs, freqs])[None, :], jnp.float32)
    group_count = pool_map.shape[0]
    half_out = model // 2
    vmem = pl.BlockSpec(memory_space=pltpu.VMEM)
    smem = pl.BlockSpec(memory_space=pltpu.SMEM)
    hbm = pl.BlockSpec(memory_space=pl.ANY)
    dma = pltpu.SemaphoreType.DMA
    low = jnp.bfloat16

    def gather_sems(count):
        return [
            dma((count,)),
            dma((places, count)),
            dma((places, count)),
            dma((2, 2 * places)),
            dma((2, 2 * places)),
            dma((2, places)),
            dma((2, places)),
        ]

    out = pl.pallas_call(
        lambda *refs: fused_kernel(places, groups, *refs),
        out_shape=jax.ShapeDtypeStruct((row_count, half_out), low),
        in_specs=[hbm, vmem, vmem] + [hbm] * 5 + [vmem] * 2 + [smem] + [hbm] * 2,
        out_specs=vmem,
        scratch_shapes=[
            pltpu.VMEM((row_count // 2, model), low),
            pltpu.VMEM((GROUP_DIM, GROUP_DIM), low),
            pltpu.VMEM((length, HEAD_DIM), jnp.float32),
            pltpu.VMEM((length, HEAD_DIM), jnp.float32),
            pltpu.VMEM((length, model), low),
            pltpu.VMEM((4, model, GROUP_DIM), low),
            pltpu.VMEM((2, GROUP_DIM, model), low),
            pltpu.VMEM((length, GROUP_DIM), low),
            pltpu.VMEM((length, GROUP_DIM), low),
            pltpu.VMEM((length, GROUP_DIM), low),
            pltpu.VMEM((length + 16, GROUP_DIM), low),
            pltpu.VMEM((2, row_count // PARTS, half_out), jnp.float32),
            pltpu.VMEM((places * PARTS, row_count // PARTS, half_out), low),
            pltpu.VMEM((places * PARTS, row_count // PARTS, half_out), low),
            pltpu.VMEM((2 * PARTS, row_count // PARTS, half_out), jnp.float32),
            pltpu.VMEM((places * PARTS, row_count // PARTS, half_out), low),
            pltpu.VMEM((2 * PARTS, row_count // PARTS, half_out), low),
            pltpu.VMEM((2 * PARTS, row_count // PARTS, half_out), low),
            pltpu.VMEM((PARTS, row_count // PARTS, half_out), jnp.float32),
            dma((2,)),
            *gather_sems(4),
            *gather_sems(2),
            dma((places, PIECES)),
            dma((places, PIECES)),
            dma((places, PIECES)),
            dma((places, PIECES)),
            dma((places, PIECES)),
            dma((places, PIECES)),
            dma((places * PARTS,)),
            dma((places * PARTS,)),
            dma((3 * PARTS,)),
            dma((2 * PARTS,)),
            dma((2 * PARTS,)),
            dma((2 * PARTS,)),
        ],
        compiler_params=pltpu.CompilerParams(
            collective_id=0, has_side_effects=True, vmem_limit_bytes=56 * 1024 * 1024
        ),
    )(
        tokens[0],
        norm_gain.reshape(1, model),
        freqs,
        pool_input,
        query_weight,
        key_weight,
        value_weight,
        pool_map,
        pool_scale.reshape(group_count, 1, GROUP_DIM),
        head_gain.reshape(1, 2 * HEAD_DIM),
        diff_lambda,
        out_pool,
        out_heads,
    )
    return out[None]


def solution(mesh):
    placed = (
        P("fs", "sp", None),
        P(),
        P(("sp", "fs"), "tp"),
        P(("sp", "fs"), "tp"),
        P(("sp", "fs"), "tp"),
        P(("sp", "fs"), "tp"),
        P("tp", None, None),
        P("tp"),
        P(),
        P(),
        P("tp", ("sp", "fs")),
        P("tp", ("sp", "fs")),
    )
    shape = dict(mesh.shape)

    def body(tokens, *rest):
        head_count = rest[3].shape[1] // (2 * HEAD_DIM)
        group_count = rest[5].shape[0]
        fits = (
            shape["fs"] == 4
            and shape["tp"] == 2
            and shape["sp"] == head_count == group_count == 4
            and tokens.shape[0] == 1
        )
        return (fused if fits else local)(tokens, *rest)

    return jax.shard_map(
        body, mesh=mesh, in_specs=placed, out_specs=P("fs", "sp", "tp"), check_vma=False
    )
```

```python
import math

import jax
import jax.numpy as jnp
import numpy as np
from jax import lax
from jax.experimental import pallas as pl
from jax.experimental.pallas import tpu as pltpu
from jax.sharding import PartitionSpec as P

HEAD_DIM = 128
GROUP_DIM = 256


THETA = 500000.0
HEAD_SCALE = 0.8
NORM_EPS = 1e-06
HEAD_EPS = 1e-05


def from_behind(value, axis, steps):
    count = lax.axis_size(axis)
    first, last = (max(0, -steps), min(count, count - steps))
    return lax.ppermute(value, axis, [(source, source + steps) for source in range(first, last)])


def rotate(tensor, positions):
    half = HEAD_DIM // 2
    freqs = 1.0 / THETA ** (jnp.arange(half, dtype=jnp.float32) * 2.0 / HEAD_DIM)
    angles = positions[:, None] * freqs[None, :]
    cosine = jnp.cos(angles)[:, None, None, :]
    sine = jnp.sin(angles)[:, None, None, :]
    floated = tensor.astype(jnp.float32)
    first = floated[..., :half]
    second = floated[..., half:]
    turned = jnp.concatenate([first * cosine - second * sine, second * cosine + first * sine], -1)
    return turned.astype(jnp.bfloat16)


def local(
    tokens,
    norm_gain,
    pool_input,
    query_weight,
    key_weight,
    value_weight,
    pool_map,
    pool_scale,
    head_gain,
    diff_lambda,
    out_pool,
    out_heads,
):
    out_local = jnp.concatenate([out_pool, out_heads], 0)
    row_count = tokens.shape[1]
    floated = tokens[0].astype(jnp.float32)
    normed = (
        floated * lax.rsqrt(jnp.mean(floated * floated, -1, keepdims=True) + NORM_EPS) * norm_gain
    ).astype(jnp.bfloat16)
    fragments = (
        lax.all_gather(pool_input, ("sp", "fs"), axis=0, tiled=True),
        lax.all_gather(query_weight, ("sp", "fs"), axis=0, tiled=True),
        lax.all_gather(key_weight, ("sp", "fs"), axis=0, tiled=True),
        lax.all_gather(value_weight, ("sp", "fs"), axis=0, tiled=True),
    )
    projected = tuple(
        (jnp.dot(normed, fragment, preferred_element_type=jnp.float32) for fragment in fragments)
    )
    pool_in, queries, keys_flat, values_flat = [
        product.astype(jnp.bfloat16) for product in projected
    ]
    head_count = values_flat.shape[1] // (2 * HEAD_DIM)
    tp_index = lax.axis_index("tp")
    sp_index = lax.axis_index("sp")
    query_pos = sp_index * row_count + jnp.arange(row_count, dtype=jnp.int32)
    positions = query_pos.astype(jnp.float32)
    queries = rotate(queries.reshape(row_count, head_count, 2, HEAD_DIM), positions)
    keys_flat = rotate(keys_flat.reshape(row_count, head_count, 2, HEAD_DIM), positions).reshape(
        row_count, head_count * 2 * HEAD_DIM
    )
    lambdas = lax.dynamic_slice_in_dim(diff_lambda, tp_index * head_count, head_count, 0)

    def online_step(state, key_rows, value_rows, key_offset):
        largest, summed, accum = state
        width = key_rows.shape[0]
        shaped = key_rows.reshape(width, head_count, 2, HEAD_DIM)
        scores = jnp.einsum(
            "qhcd,khcd->chqk", queries, shaped, preferred_element_type=jnp.float32
        ) * HEAD_DIM ** (-0.5)
        key_pos = key_offset + jnp.arange(width, dtype=jnp.int32)
        scores = jnp.where(query_pos[:, None] >= key_pos[None, :], scores, -jnp.inf)
        newest = jnp.maximum(largest, jnp.max(scores, -1))
        anchor = jnp.where(jnp.isfinite(newest), newest, 0.0)
        rescale = jnp.exp(largest - anchor)
        expons = jnp.exp(scores - anchor[..., None])
        summed = summed * rescale + jnp.sum(expons, -1)
        value_shaped = value_rows.reshape(width, head_count, 2 * HEAD_DIM)
        added = jnp.einsum(
            "chqk,khe->chqe",
            expons.astype(jnp.bfloat16),
            value_shaped,
            preferred_element_type=jnp.float32,
        )
        accum = accum * rescale[..., None] + added
        return (newest, summed, accum)

    start_state = (
        jnp.full((2, head_count, row_count), -jnp.inf, jnp.float32),
        jnp.zeros((2, head_count, row_count), jnp.float32),
        jnp.zeros((2, head_count, row_count, 2 * HEAD_DIM), jnp.float32),
    )
    fragments = (
        lax.all_gather(keys_flat, "sp", axis=0, tiled=True),
        lax.all_gather(values_flat, "sp", axis=0, tiled=True),
    )
    span = math.gcd(fragments[0].shape[0], 1024)

    def inner_step(index, inner_state):
        key_rows = lax.dynamic_slice_in_dim(fragments[0], index * span, span, 0)
        value_rows = lax.dynamic_slice_in_dim(fragments[1], index * span, span, 0)
        return online_step(inner_state, key_rows, value_rows, index * span)

    final_state = lax.fori_loop(0, fragments[0].shape[0] // span, inner_step, start_state)
    summed_final = final_state[1]
    accum_final = final_state[2]
    heads_raw = (
        accum_final[0] / summed_final[0][..., None]
        - lambdas[:, None, None] * accum_final[1] / summed_final[1][..., None]
    )
    heads_raw = jnp.moveaxis(heads_raw, 0, 1)
    attn = (
        (
            heads_raw
            * lax.rsqrt(jnp.mean(heads_raw * heads_raw, -1, keepdims=True) + HEAD_EPS)
            * head_gain
            * HEAD_SCALE
        )
        .astype(jnp.bfloat16)
        .reshape(row_count, head_count * 2 * HEAD_DIM)
    )
    reach = 15
    rim_rows = from_behind(pool_in[row_count - reach :], "sp", 1)
    extended = jnp.concatenate([rim_rows, pool_in], 0).astype(jnp.float32)
    pair_sums = extended[1:] + extended[:-1]
    quad_sums = pair_sums[2:] + pair_sums[:-2]
    octet_sums = quad_sums[4:] + quad_sums[:-4]
    sixteen_sums = octet_sums[8:] + octet_sums[:-8]
    group_count = pool_in.shape[1] // GROUP_DIM
    stacked = jnp.stack(
        [
            pair_sums[14 : 14 + row_count],
            quad_sums[12 : 12 + row_count],
            octet_sums[8 : 8 + row_count],
            sixteen_sums,
        ],
        0,
    ).reshape(4, row_count, group_count, GROUP_DIM)
    levels = (tp_index * group_count + jnp.arange(group_count, dtype=jnp.int32)) % 4
    picked = jnp.sum(
        jnp.where(
            levels[None, None, :, None] == jnp.arange(4, dtype=jnp.int32)[:, None, None, None],
            stacked,
            0.0,
        ),
        0,
    )
    windows = 2 ** (1 + levels)
    counts = jnp.minimum(query_pos[:, None] + 1, windows[None, :]).astype(jnp.float32)
    window_mean = picked / counts[:, :, None]
    grouped = pool_in.reshape(row_count, group_count, GROUP_DIM).astype(jnp.float32)
    pool_mixed = (window_mean - grouped).astype(jnp.bfloat16)
    pooled = (
        (
            jnp.einsum("tgc,gce->tge", pool_mixed, pool_map, preferred_element_type=jnp.float32)
            * pool_scale.reshape(group_count, GROUP_DIM)
        )
        .astype(jnp.bfloat16)
        .reshape(row_count, group_count * GROUP_DIM)
    )
    branches = jnp.concatenate([pooled, attn], 1)
    partial_value = jnp.dot(
        branches,
        lax.all_gather(out_local, ("sp", "fs"), axis=1, tiled=True),
        preferred_element_type=jnp.float32,
    )
    layer_out = lax.psum_scatter(
        partial_value.astype(jnp.bfloat16), "tp", scatter_dimension=1, tiled=True
    )
    return layer_out[None]


MESH = pl.DeviceIdType.MESH
PIECES = 4
PARTS = 2

PROJECTED = ((0, 1, 2, 3), (1, 0, 2, 3), (2, 3, 0, 1), (3, 2, 0, 1))
LATE = ((1, 3), (2, 4), (-1, 2), (-1, 2))
FINISHED = (
    (2, 4, 5, 6, 7, 3, 0, 1),
    (2, 3, 4, 5, 6, 7, 0, 1),
    (0, 1, 2, 3, 6, 7, 4, 5),
    (0, 1, 2, 3, 4, 5, 6, 7),
)
ARRIVALS = ((0, 1, 2, 3), (1, 0, 3, 2), (2, 3, 0, 1), (3, 2, 1, 0))
SENDS = ((0, 1, 2, 3), (1, 3, 2, 0), (2, 0, 1, 3), (3, 2, 1, 0))
SLOTS = tuple(
    tuple(ARRIVALS[to].index(place) for to in SENDS[place]) for place in range(len(SENDS))
)


def pick(row, z):
    value = jnp.int32(row[0])
    for place in range(1, len(row)):
        value = jnp.where(z == place, row[place], value)
    return value


def fused_kernel(
    places,
    groups,
    tokens_ref,
    norm_gain_ref,
    freqs_ref,
    pool_ref,
    query_ref,
    key_ref,
    value_ref,
    map_ref,
    scale_ref,
    gain_ref,
    lambda_ref,
    out_pool_ref,
    out_heads_ref,
    out_ref,
    own_tokens,
    own_map,
    cos_ref,
    sin_ref,
    rows_all,
    weights,
    outs,
    queries,
    keys,
    values,
    pools,
    mine,
    to_mate,
    from_mate,
    kept,
    to_peer,
    from_peer,
    merging,
    final,
    *sems,
):
    (
        own_sem,
        in_local,
        in_z_send,
        in_z_recv,
        in_n_send,
        in_n_recv,
        in_rest,
        out_local,
        out_z_send,
        out_z_recv,
        out_n_send,
        out_n_recv,
        out_rest,
        token_send,
        token_recv,
        mate_recv,
        half_send,
        half_recv,
        peer_send,
        peer_recv,
        merge_recv,
    ) = sems
    z = lax.axis_index("sp")
    f = lax.axis_index("fs")
    c = lax.axis_index("tp")
    fx = f + 1 - 2 * lax.rem(f, 2)
    fy = lax.rem(f + 2, groups)
    mate = 1 - c
    half_rows = tokens_ref.shape[0] // 2
    row_count = 2 * half_rows
    depth = pool_ref.shape[0]
    width = GROUP_DIM
    out_width = out_pool_ref.shape[1]
    half_out = out_ref.shape[1]
    length = places * row_count

    send_to = [pick([row[d] for row in SENDS], z) for d in range(places)]
    send_slot = [pick([row[d] for row in SLOTS], z) for d in range(places)]
    source = [pick([row[d] for row in ARRIVALS], z) for d in range(places)]

    def block(index, size):
        return pl.ds(pl.multiple_of(index * size, size), size)

    barrier = pltpu.get_barrier_semaphore()
    partners = [{"sp": lax.rem(z + d, places)} for d in range(1, places)]
    partners += [{"fs": fx}, {"fs": fy}, {"tp": mate}]
    for partner in partners:
        pl.semaphore_signal(barrier, inc=1, device_id=partner, device_id_type=MESH)

    def remote(source, target, send, recv, device):
        return pltpu.make_async_remote_copy(
            src_ref=source,
            dst_ref=target,
            send_sem=send,
            recv_sem=recv,
            device_id=device,
            device_id_type=MESH,
        )

    class Gather:
        def __init__(self, sources, cut, view, sent, received, group):
            self.sources, self.cut, self.view = sources, cut, view
            self.sent, self.received = sent, received
            self.count = len(sources)
            (
                self.local,
                self.z_send,
                self.z_recv,
                self.n_send,
                self.n_recv,
                self.rest,
            ) = group
            self.low = (0, self.count // 2)
            self.high = (self.count // 2, self.count - self.count // 2)

        def own(self, m):
            return pltpu.make_async_copy(
                self.cut(self.sources[m], z), self.view(z, f, m, 1).at[0], self.local.at[m]
            )

        def across(self, d, m):
            to, slot = send_to[d], send_slot[d]
            return remote(
                self.cut(self.sources[m], to),
                self.view(z, f, m, 1).at[0],
                self.z_send.at[d],
                self.z_recv.at[slot],
                {"sp": to},
            )

        def arrive(self, d):
            view = self.view(source[d], f, 0, self.count)
            return remote(view, view, self.z_send.at[d], self.z_recv.at[d], {"sp": source[d]})

        def near(self, d, side, column, half):
            start, size = (self.low, self.high)[half]
            view = self.view(source[d], column, start, size)
            early = half == side
            return remote(
                view,
                view,
                self.n_send.at[side],
                self.n_recv.at[side, d] if early else self.rest.at[0],
                {"fs": (fx, fy)[side]},
            )

        def forward(self, d, side, column):
            start, size = (self.high, self.low)[side]
            view = self.view(source[d], column, start, size)
            return remote(
                view, view, self.n_send.at[side], self.rest.at[0], {"fs": (fx, fy)[side]}
            )

        def start_own(self):
            for m in range(self.count):
                self.own(m).start()

        def start(self, d):
            for m in range(self.count):
                self.across(d, m).start()

        def first(self, d):
            if d == 0:
                for m in range(self.count):
                    self.own(m).wait()
            else:
                self.arrive(d).wait_recv()
            for order in range(2):
                for side in range(2):
                    self.near(d, side, f, side ^ order).start()

        def second(self, d):
            self.near(d, 0, fx, 0).wait_recv()
            self.forward(d, 1, fx).start()
            self.near(d, 1, fy, 1).wait_recv()
            self.forward(d, 0, fy).start()

        def third(self):
            remote(
                self.received, self.received, self.n_send.at[0], self.rest.at[0], {"fs": fx}
            ).wait_recv()

        def drain(self):
            for d in range(1, places):
                self.arrive(d).wait_send()
            for side in range(2):
                remote(
                    self.sent, self.sent, self.n_send.at[side], self.rest.at[0], {"fs": fx}
                ).wait_send()

    filled = places * groups
    inward = Gather(
        (pool_ref, query_ref, key_ref, value_ref),
        lambda ref, to: ref.at[:, block(to, width)],
        lambda zz, ff, m, n: weights.at[pl.ds(m, n), block(zz * groups + ff, depth), :],
        weights.at[:, pl.ds(0, filled * 3 // 8 * depth), :],
        weights.at[:, pl.ds(0, filled // 2 * depth), :],
        (in_local, in_z_send, in_z_recv, in_n_send, in_n_recv, in_rest),
    )
    outward = Gather(
        (out_pool_ref, out_heads_ref),
        lambda ref, to: ref.at[block(to, width), :],
        lambda zz, ff, m, n: outs.at[pl.ds(m, n), :, block(zz * groups + ff, out_width)],
        outs.at[:, :, pl.ds(0, filled * 3 // 8 * out_width)],
        outs.at[:, :, pl.ds(0, filled // 2 * out_width)],
        (out_local, out_z_send, out_z_recv, out_n_send, out_n_recv, out_rest),
    )

    piece_rows = half_rows // PIECES

    def chunk(b, side, p):
        return rows_all.at[block((2 * b + side) * PIECES + p, piece_rows), :]

    def right(b, p, step=1):
        view = chunk(b, c, p)
        return remote(view, view, token_send.at[0], token_recv.at[b, p], {"sp": z + step})

    def left(b, p, step=-1):
        view = chunk(b, c, p)
        return remote(view, view, token_send.at[1], token_recv.at[b, p], {"sp": z + step})

    def share(b, side, p):
        view = chunk(b, side, p)
        return remote(view, view, token_send.at[2], mate_recv.at[b], {"tp": mate})

    def sent_tokens(kind, blocks):
        view = rows_all.at[pl.ds(0, blocks * half_rows), :]
        return remote(view, view, token_send.at[kind], mate_recv.at[0], {"tp": mate})

    def each_place(act):
        for place in range(places):
            pl.when(z == place)(lambda place=place: act(place))

    def send_right(place):
        for p in range(PIECES):
            right(place, p).start()

    def send_left(place):
        for p in range(PIECES):
            left(place, p).start()

    def take(place, b, pieces=range(PIECES)):
        for p in pieces:
            if b < place:
                right(b, p, -1).wait_recv()
                if place < places - 1:
                    right(b, p).start()
            else:
                left(b, p, 1).wait_recv()
                if place > 0:
                    left(b, p).start()
            share(b, c, p).start()

    first_half, second_half = range(PIECES // 2), range(PIECES // 2, PIECES)

    def prepare(place):
        for d in range(1, places):
            inward.start(d)
        for d in range(1, places) if place in (1, 2) else (1,):
            outward.start(d)

    def begin(place):
        if place == 0:
            send_right(place)
        if place == places - 1:
            send_left(place)
        if place in (0, places - 1):
            for d in range(2, places):
                outward.start(d)
        for p in range(PIECES):
            share(place, c, p).start()

    def gather(place):
        taken = (1, 0, 3, 2)[place]
        inward.second(0)
        outward.second(0)
        inward.first(1)
        inward.first(2)
        if place in (1, 2):
            if place == 1:
                send_left(place)
            else:
                send_right(place)
                send_left(place)
            inward.second(1)
            outward.first(1)
            inward.second(2)
            take(place, taken, first_half)
            inward.first(3)
            outward.first(3)
            take(place, taken, second_half)
            if place == 1:
                send_right(place)
            outward.second(1)
            inward.second(3)
            outward.first(2)
            take(place, (None, 2, 0, None)[place], first_half)
        else:
            inward.second(1)
            inward.first(3)
            outward.first(1)
            inward.second(2)
            outward.first(2)
            inward.second(3)
            outward.second(1)
            take(place, taken)
            outward.first(3)
        inward.third()

    def relay(place):
        if place in (1, 2):
            take(place, (None, 2, 0, None)[place], second_half)
            outward.second(3)
            outward.second(2)
        else:
            outward.second(2)
            outward.second(3)
        if place == 3:
            take(place, 0)

    def finish_gather(place):
        if place in (1, 2):
            take(place, (None, 3, 1, None)[place], first_half)
        outward.third()
        if place in (1, 2):
            take(place, (None, 3, 1, None)[place], second_half)

    tokens_in = pltpu.make_async_copy(
        tokens_ref.at[block(c, half_rows), :], own_tokens, own_sem.at[0]
    )
    map_in = pltpu.make_async_copy(map_ref.at[z], own_map, own_sem.at[1])
    tokens_in.start()
    inward.start_own()
    outward.start_own()
    map_in.start()
    pl.semaphore_wait(barrier, len(partners))
    each_place(prepare)
    tokens_in.wait()
    floated = own_tokens[...].astype(jnp.float32)
    rows_all[block(2 * z + c, half_rows), :] = (
        floated
        * lax.rsqrt(jnp.mean(floated * floated, -1, keepdims=True) + NORM_EPS)
        * norm_gain_ref[...]
    ).astype(jnp.bfloat16)
    inward.first(0)
    outward.first(0)
    pools[0:16, :] = jnp.zeros((16, width), jnp.bfloat16)
    keys[...] = jnp.zeros_like(keys)
    values[...] = jnp.zeros_like(values)
    each_place(begin)

    def table(index, carry):
        rows = block(index, row_count)
        half = HEAD_DIM // 2
        count = (
            index * row_count + lax.broadcasted_iota(jnp.int32, (row_count, HEAD_DIM), 0)
        ).astype(jnp.float32)
        lane = lax.broadcasted_iota(jnp.int32, (row_count, HEAD_DIM), 1)
        angles = count * freqs_ref[...]
        cos_ref[rows, :] = jnp.cos(angles)
        sine = jnp.sin(angles)
        sin_ref[rows, :] = jnp.where(lane < half, -sine, sine)
        return carry

    lax.fori_loop(0, places, table, 0)

    def turned(raw, cosine, sine):
        floated = raw.astype(jnp.float32)
        return (floated * cosine + pltpu.roll(floated, HEAD_DIM // 2, 1) * sine).astype(
            jnp.bfloat16
        )

    projected = [pick([row[i] for row in PROJECTED], z) for i in range(places)]
    late = [pick([row[i] for row in LATE], z) for i in range(2)]
    finished = [pick([row[i] for row in FINISHED], z) for i in range(places * PARTS)]

    def project(index):
        theirs = rows_all.at[block(2 * index + mate, half_rows), :]
        remote(theirs, theirs, token_send.at[2], mate_recv.at[index], {"tp": mate}).wait_recv()
        rows = block(index, row_count)
        normed = rows_all[rows, :]
        cosine = cos_ref[rows, :]
        sine = sin_ref[rows, :]

        def product(m):
            return jnp.dot(normed, weights[m], preferred_element_type=jnp.float32).astype(
                jnp.bfloat16
            )

        pools[pl.ds(pl.multiple_of(index * row_count + 16, 16), row_count), :] = product(0)
        raw = product(1)
        for m in range(2):
            part = slice(m * HEAD_DIM, (m + 1) * HEAD_DIM)
            queries[rows, part] = turned(raw[:, part], cosine, sine)
        raw = product(2)
        for m in range(2):
            part = slice(m * HEAD_DIM, (m + 1) * HEAD_DIM)
            keys[rows, part] = turned(raw[:, part], cosine, sine)
        values[rows, :] = product(3)

    upper = z >= places // 2

    def project_early(i, carry):
        project(jnp.where(i == 0, projected[0], projected[1]))
        return carry

    each_place(gather)
    lax.fori_loop(0, 2, project_early, 0)
    each_place(relay)

    @pl.when(upper)
    def _():
        project(projected[2])

    each_place(finish_gather)
    map_in.wait()

    level = lax.rem(c * map_ref.shape[0] + z, 4)
    window = jnp.where(
        level == 0, 2, jnp.where(level == 1, 4, jnp.where(level == 2, 8, 16))
    )
    head_lambda = lambda_ref[c * map_ref.shape[0] + z]

    part_rows = row_count // PARTS

    def to_sibling(step):
        return remote(
            to_mate.at[step],
            from_mate.at[step],
            half_send.at[0],
            half_recv.at[step],
            {"tp": mate},
        )

    outer = (z == 0) | (z == places - 1)
    pair = z + 1 - 2 * lax.rem(z, 2)

    def crossing(to, h):
        return lax.rem(to, 2) * PARTS + h

    def to_inner(to, h):
        return remote(
            to_peer.at[to * PARTS + h],
            merging.at[crossing(to, h)],
            peer_send.at[0],
            merge_recv.at[crossing(to, h)],
            {"sp": pair},
        )

    def to_place(to, h):
        return remote(
            to_peer.at[to * PARTS + h],
            from_peer.at[h],
            peer_send.at[0],
            peer_recv.at[h],
            {"sp": to},
        )

    def to_pair(h):
        return remote(
            to_peer.at[pair * PARTS + h],
            from_peer.at[PARTS + h],
            peer_send.at[0],
            peer_recv.at[PARTS + h],
            {"sp": pair},
        )

    def step_place(step):
        slot = finished[0]
        for i in range(1, places * PARTS):
            slot = jnp.where(step == i, finished[i], slot)
        return slot // PARTS, lax.rem(slot, PARTS)

    def compute(step):
        to, h = step_place(step)
        slot = to * PARTS + h
        rows = block(slot, part_rows)
        query_pos = slot * part_rows + lax.broadcasted_iota(jnp.int32, (part_rows, length), 0)
        key_pos = lax.broadcasted_iota(jnp.int32, (part_rows, length), 1)
        seen = query_pos >= key_pos
        mapped = []
        for m in range(2):
            part = slice(m * HEAD_DIM, (m + 1) * HEAD_DIM)
            scores = lax.dot_general(
                queries[rows, part],
                keys[:, part],
                (((1,), (1,)), ((), ())),
                preferred_element_type=jnp.float32,
            ) * HEAD_DIM ** (-0.5)
            scores = jnp.where(seen, scores, -jnp.inf)
            expons = jnp.exp(scores - jnp.max(scores, -1, keepdims=True))
            totals = jnp.sum(expons, -1, keepdims=True)
            mapped.append(
                jnp.dot(
                    expons.astype(jnp.bfloat16), values[...], preferred_element_type=jnp.float32
                )
                / totals
            )
        raw = mapped[0] - head_lambda * mapped[1]
        attn = (
            raw
            * lax.rsqrt(jnp.mean(raw * raw, -1, keepdims=True) + HEAD_EPS)
            * gain_ref[...]
            * HEAD_SCALE
        ).astype(jnp.bfloat16)
        extended = pools[
            pl.ds(pl.multiple_of(slot * part_rows, 16), part_rows + 16), :
        ].astype(jnp.float32)
        picked = extended + pltpu.roll(extended, 1, 0)
        sums = picked
        for shift in (2, 4, 8):
            sums = sums + pltpu.roll(sums, shift, 0)
            picked = lax.select_n(window >= 2 * shift, picked, sums)
        places_of = slot * part_rows + lax.broadcasted_iota(jnp.int32, (part_rows, 1), 0)
        counts = jnp.minimum(places_of + 1, window).astype(jnp.float32)
        mixed = (picked[16:] / counts - extended[16:]).astype(jnp.bfloat16)
        pooled = (
            jnp.dot(mixed, own_map[...], preferred_element_type=jnp.float32) * scale_ref[z]
        ).astype(jnp.bfloat16)

        def partial_of(side):
            columns = block(side, half_out)
            return jnp.dot(
                pooled, outs[0, :, columns], preferred_element_type=jnp.float32
            ) + jnp.dot(attn, outs[1, :, columns], preferred_element_type=jnp.float32)

        to_mate[step] = partial_of(mate).astype(jnp.bfloat16)
        to_sibling(step).start()
        mine[lax.rem(step, 2)] = partial_of(c)

    def finish(step):
        to, h = step_place(step)
        slot = to * PARTS + h
        crosses = to // 2 != z // 2
        to_sibling(step).wait_recv()
        summed = mine[lax.rem(step, 2)] + from_mate[step].astype(jnp.float32)

        @pl.when(to == z)
        def _():
            final[h] = summed

        @pl.when(to == pair)
        def _():
            to_peer[slot] = summed.astype(jnp.bfloat16)
            to_pair(h).start()

        @pl.when(crosses & outer)
        def _():
            to_peer[slot] = summed.astype(jnp.bfloat16)
            to_inner(to, h).start()

        @pl.when(crosses & jnp.logical_not(outer))
        def _():
            kept[crossing(to, h)] = summed

    def merge(turn):
        place = turn // PARTS
        to = jnp.where(upper, place, places // 2 + place)
        h = lax.rem(turn, PARTS)
        to_inner(to, h).wait_recv()
        to_peer[to * PARTS + h] = (
            kept[crossing(to, h)] + merging[crossing(to, h)].astype(jnp.float32)
        ).astype(jnp.bfloat16)
        to_place(to, h).start()

    upper_inner = z == places // 2

    def body(step, carry):
        grows = (step == late[0]) | (step == late[1])

        @pl.when(grows)
        def _():
            finish(step - 1)

            @pl.when((z == 0) & (step == late[0]))
            def _():
                take(0, 2)

            @pl.when((z == 0) & (step == late[1]))
            def _():
                take(0, 3)

            @pl.when(z == places - 1)
            def _():
                take(places - 1, 1)

            project(jnp.where(step == late[1], projected[3], projected[2]))

        compute(step)

        @pl.when(jnp.logical_not(grows) & (step > 0))
        def _():
            finish(step - 1)

        @pl.when(upper_inner & (step == 5))
        def _():
            merge(0)

        return carry

    lax.fori_loop(0, places * PARTS, body, 0)
    finish(places * PARTS - 1)

    def merge_more(turn, carry):
        merge(turn)
        return carry

    @pl.when(jnp.logical_not(outer))
    def _():
        lax.fori_loop(jnp.where(upper, 1, 0), 2 * PARTS, merge_more, 0)

    for h in range(PARTS):
        to_pair(h).wait_recv()
        total = final[h] + from_peer[PARTS + h].astype(jnp.float32)
        to_place(z, h).wait_recv()
        out_ref[h * part_rows : (h + 1) * part_rows, :] = (
            total + from_peer[h].astype(jnp.float32)
        ).astype(out_ref.dtype)

    inward.drain()
    outward.drain()

    def drain(place):
        if place < places - 1:
            sent_tokens(0, place + 1).wait_send()
        if place > 0:
            sent_tokens(1, places - place).wait_send()

    each_place(drain)
    sent_tokens(2, places).wait_send()
    remote(to_mate, from_mate, half_send.at[0], half_recv.at[0], {"tp": mate}).wait_send()
    sent = to_peer.at[pl.ds(0, (places - 1) * PARTS)]
    remote(sent, sent, peer_send.at[0], peer_recv.at[0], {"sp": pair}).wait_send()


def fused(
    tokens,
    norm_gain,
    pool_input,
    query_weight,
    key_weight,
    value_weight,
    pool_map,
    pool_scale,
    head_gain,
    diff_lambda,
    out_pool,
    out_heads,
):
    places = lax.axis_size("sp")
    groups = lax.axis_size("fs")
    row_count, model = tokens.shape[1], tokens.shape[2]
    length = places * row_count
    half = HEAD_DIM // 2
    freqs = np.float32(1.0) / np.float32(THETA) ** (
        np.arange(half, dtype=np.float32) * np.float32(2.0) / np.float32(HEAD_DIM)
    )
    freqs = jnp.asarray(np.concatenate([freqs, freqs])[None, :], jnp.float32)
    group_count = pool_map.shape[0]
    half_out = model // 2
    vmem = pl.BlockSpec(memory_space=pltpu.VMEM)
    smem = pl.BlockSpec(memory_space=pltpu.SMEM)
    hbm = pl.BlockSpec(memory_space=pl.ANY)
    dma = pltpu.SemaphoreType.DMA
    low = jnp.bfloat16

    def gather_sems(count):
        return [
            dma((count,)),
            dma((places,)),
            dma((places,)),
            dma((2,)),
            dma((2, places)),
            dma((1,)),
        ]

    out = pl.pallas_call(
        lambda *refs: fused_kernel(places, groups, *refs),
        out_shape=jax.ShapeDtypeStruct((row_count, half_out), low),
        in_specs=[hbm, vmem, vmem] + [hbm] * 5 + [vmem] * 2 + [smem] + [hbm] * 2,
        out_specs=vmem,
        scratch_shapes=[
            pltpu.VMEM((row_count // 2, model), low),
            pltpu.VMEM((GROUP_DIM, GROUP_DIM), low),
            pltpu.VMEM((length, HEAD_DIM), jnp.float32),
            pltpu.VMEM((length, HEAD_DIM), jnp.float32),
            pltpu.VMEM((length, model), low),
            pltpu.VMEM((4, model, GROUP_DIM), low),
            pltpu.VMEM((2, GROUP_DIM, model), low),
            pltpu.VMEM((length, GROUP_DIM), low),
            pltpu.VMEM((length, GROUP_DIM), low),
            pltpu.VMEM((length, GROUP_DIM), low),
            pltpu.VMEM((length + 16, GROUP_DIM), low),
            pltpu.VMEM((2, row_count // PARTS, half_out), jnp.float32),
            pltpu.VMEM((places * PARTS, row_count // PARTS, half_out), low),
            pltpu.VMEM((places * PARTS, row_count // PARTS, half_out), low),
            pltpu.VMEM((2 * PARTS, row_count // PARTS, half_out), jnp.float32),
            pltpu.VMEM((places * PARTS, row_count // PARTS, half_out), low),
            pltpu.VMEM((2 * PARTS, row_count // PARTS, half_out), low),
            pltpu.VMEM((2 * PARTS, row_count // PARTS, half_out), low),
            pltpu.VMEM((PARTS, row_count // PARTS, half_out), jnp.float32),
            dma((2,)),
            *gather_sems(4),
            *gather_sems(2),
            dma((3,)),
            dma((places, PIECES)),
            dma((places,)),
            dma((1,)),
            dma((places * PARTS,)),
            dma((1,)),
            dma((2 * PARTS,)),
            dma((2 * PARTS,)),
        ],
        compiler_params=pltpu.CompilerParams(
            collective_id=0, has_side_effects=True, vmem_limit_bytes=56 * 1024 * 1024
        ),
    )(
        tokens[0],
        norm_gain.reshape(1, model),
        freqs,
        pool_input,
        query_weight,
        key_weight,
        value_weight,
        pool_map,
        pool_scale.reshape(group_count, 1, GROUP_DIM),
        head_gain.reshape(1, 2 * HEAD_DIM),
        diff_lambda,
        out_pool,
        out_heads,
    )
    return out[None]


def solution(mesh):
    placed = (
        P("fs", "sp", None),
        P(),
        P(("sp", "fs"), "tp"),
        P(("sp", "fs"), "tp"),
        P(("sp", "fs"), "tp"),
        P(("sp", "fs"), "tp"),
        P("tp", None, None),
        P("tp"),
        P(),
        P(),
        P("tp", ("sp", "fs")),
        P("tp", ("sp", "fs")),
    )
    shape = dict(mesh.shape)

    def body(tokens, *rest):
        head_count = rest[3].shape[1] // (2 * HEAD_DIM)
        group_count = rest[5].shape[0]
        fits = (
            shape["fs"] == 4
            and shape["tp"] == 2
            and shape["sp"] == head_count == group_count == 4
            and tokens.shape[0] == 1
        )
        return (fused if fits else local)(tokens, *rest)

    return jax.shard_map(
        body, mesh=mesh, in_specs=placed, out_specs=P("fs", "sp", "tp"), check_vma=False
    )
```

```python
import math

import jax
import jax.numpy as jnp
import numpy as np
from jax import lax
from jax.experimental import pallas as pl
from jax.experimental.pallas import tpu as pltpu
from jax.sharding import PartitionSpec as P

HEAD_DIM = 128
GROUP_DIM = 256


THETA = 500000.0
HEAD_SCALE = 0.8
NORM_EPS = 1e-06
HEAD_EPS = 1e-05


def from_behind(value, axis, steps):
    count = lax.axis_size(axis)
    first, last = (max(0, -steps), min(count, count - steps))
    return lax.ppermute(value, axis, [(source, source + steps) for source in range(first, last)])


def rotate(tensor, positions):
    half = HEAD_DIM // 2
    freqs = 1.0 / THETA ** (jnp.arange(half, dtype=jnp.float32) * 2.0 / HEAD_DIM)
    angles = positions[:, None] * freqs[None, :]
    cosine = jnp.cos(angles)[:, None, None, :]
    sine = jnp.sin(angles)[:, None, None, :]
    floated = tensor.astype(jnp.float32)
    first = floated[..., :half]
    second = floated[..., half:]
    turned = jnp.concatenate([first * cosine - second * sine, second * cosine + first * sine], -1)
    return turned.astype(jnp.bfloat16)


def local(
    tokens,
    norm_gain,
    pool_input,
    query_weight,
    key_weight,
    value_weight,
    pool_map,
    pool_scale,
    head_gain,
    diff_lambda,
    out_pool,
    out_heads,
):
    out_local = jnp.concatenate([out_pool, out_heads], 0)
    row_count = tokens.shape[1]
    floated = tokens[0].astype(jnp.float32)
    normed = (
        floated * lax.rsqrt(jnp.mean(floated * floated, -1, keepdims=True) + NORM_EPS) * norm_gain
    ).astype(jnp.bfloat16)
    fragments = (
        lax.all_gather(pool_input, ("sp", "fs"), axis=0, tiled=True),
        lax.all_gather(query_weight, ("sp", "fs"), axis=0, tiled=True),
        lax.all_gather(key_weight, ("sp", "fs"), axis=0, tiled=True),
        lax.all_gather(value_weight, ("sp", "fs"), axis=0, tiled=True),
    )
    projected = tuple(
        (jnp.dot(normed, fragment, preferred_element_type=jnp.float32) for fragment in fragments)
    )
    pool_in, queries, keys_flat, values_flat = [
        product.astype(jnp.bfloat16) for product in projected
    ]
    head_count = values_flat.shape[1] // (2 * HEAD_DIM)
    tp_index = lax.axis_index("tp")
    sp_index = lax.axis_index("sp")
    query_pos = sp_index * row_count + jnp.arange(row_count, dtype=jnp.int32)
    positions = query_pos.astype(jnp.float32)
    queries = rotate(queries.reshape(row_count, head_count, 2, HEAD_DIM), positions)
    keys_flat = rotate(keys_flat.reshape(row_count, head_count, 2, HEAD_DIM), positions).reshape(
        row_count, head_count * 2 * HEAD_DIM
    )
    lambdas = lax.dynamic_slice_in_dim(diff_lambda, tp_index * head_count, head_count, 0)

    def online_step(state, key_rows, value_rows, key_offset):
        largest, summed, accum = state
        width = key_rows.shape[0]
        shaped = key_rows.reshape(width, head_count, 2, HEAD_DIM)
        scores = jnp.einsum(
            "qhcd,khcd->chqk", queries, shaped, preferred_element_type=jnp.float32
        ) * HEAD_DIM ** (-0.5)
        key_pos = key_offset + jnp.arange(width, dtype=jnp.int32)
        scores = jnp.where(query_pos[:, None] >= key_pos[None, :], scores, -jnp.inf)
        newest = jnp.maximum(largest, jnp.max(scores, -1))
        anchor = jnp.where(jnp.isfinite(newest), newest, 0.0)
        rescale = jnp.exp(largest - anchor)
        expons = jnp.exp(scores - anchor[..., None])
        summed = summed * rescale + jnp.sum(expons, -1)
        value_shaped = value_rows.reshape(width, head_count, 2 * HEAD_DIM)
        added = jnp.einsum(
            "chqk,khe->chqe",
            expons.astype(jnp.bfloat16),
            value_shaped,
            preferred_element_type=jnp.float32,
        )
        accum = accum * rescale[..., None] + added
        return (newest, summed, accum)

    start_state = (
        jnp.full((2, head_count, row_count), -jnp.inf, jnp.float32),
        jnp.zeros((2, head_count, row_count), jnp.float32),
        jnp.zeros((2, head_count, row_count, 2 * HEAD_DIM), jnp.float32),
    )
    fragments = (
        lax.all_gather(keys_flat, "sp", axis=0, tiled=True),
        lax.all_gather(values_flat, "sp", axis=0, tiled=True),
    )
    span = math.gcd(fragments[0].shape[0], 1024)

    def inner_step(index, inner_state):
        key_rows = lax.dynamic_slice_in_dim(fragments[0], index * span, span, 0)
        value_rows = lax.dynamic_slice_in_dim(fragments[1], index * span, span, 0)
        return online_step(inner_state, key_rows, value_rows, index * span)

    final_state = lax.fori_loop(0, fragments[0].shape[0] // span, inner_step, start_state)
    summed_final = final_state[1]
    accum_final = final_state[2]
    heads_raw = (
        accum_final[0] / summed_final[0][..., None]
        - lambdas[:, None, None] * accum_final[1] / summed_final[1][..., None]
    )
    heads_raw = jnp.moveaxis(heads_raw, 0, 1)
    attn = (
        (
            heads_raw
            * lax.rsqrt(jnp.mean(heads_raw * heads_raw, -1, keepdims=True) + HEAD_EPS)
            * head_gain
            * HEAD_SCALE
        )
        .astype(jnp.bfloat16)
        .reshape(row_count, head_count * 2 * HEAD_DIM)
    )
    reach = 15
    rim_rows = from_behind(pool_in[row_count - reach :], "sp", 1)
    extended = jnp.concatenate([rim_rows, pool_in], 0).astype(jnp.float32)
    pair_sums = extended[1:] + extended[:-1]
    quad_sums = pair_sums[2:] + pair_sums[:-2]
    octet_sums = quad_sums[4:] + quad_sums[:-4]
    sixteen_sums = octet_sums[8:] + octet_sums[:-8]
    group_count = pool_in.shape[1] // GROUP_DIM
    stacked = jnp.stack(
        [
            pair_sums[14 : 14 + row_count],
            quad_sums[12 : 12 + row_count],
            octet_sums[8 : 8 + row_count],
            sixteen_sums,
        ],
        0,
    ).reshape(4, row_count, group_count, GROUP_DIM)
    levels = (tp_index * group_count + jnp.arange(group_count, dtype=jnp.int32)) % 4
    picked = jnp.sum(
        jnp.where(
            levels[None, None, :, None] == jnp.arange(4, dtype=jnp.int32)[:, None, None, None],
            stacked,
            0.0,
        ),
        0,
    )
    windows = 2 ** (1 + levels)
    counts = jnp.minimum(query_pos[:, None] + 1, windows[None, :]).astype(jnp.float32)
    window_mean = picked / counts[:, :, None]
    grouped = pool_in.reshape(row_count, group_count, GROUP_DIM).astype(jnp.float32)
    pool_mixed = (window_mean - grouped).astype(jnp.bfloat16)
    pooled = (
        (
            jnp.einsum("tgc,gce->tge", pool_mixed, pool_map, preferred_element_type=jnp.float32)
            * pool_scale.reshape(group_count, GROUP_DIM)
        )
        .astype(jnp.bfloat16)
        .reshape(row_count, group_count * GROUP_DIM)
    )
    branches = jnp.concatenate([pooled, attn], 1)
    partial_value = jnp.dot(
        branches,
        lax.all_gather(out_local, ("sp", "fs"), axis=1, tiled=True),
        preferred_element_type=jnp.float32,
    )
    layer_out = lax.psum_scatter(
        partial_value.astype(jnp.bfloat16), "tp", scatter_dimension=1, tiled=True
    )
    return layer_out[None]


MESH = pl.DeviceIdType.MESH
PIECES = 4
PARTS = 2

PROJECTED = ((0, 1, 2, 3), (1, 0, 2, 3), (2, 0, 3, 1), (3, 0, 2, 1))
LATE = ((1, 3), (2, 6), (2, 2), (2, 2))
FINISHED = (
    (2, 4, 5, 6, 7, 3, 0, 1),
    (2, 3, 4, 5, 0, 1, 6, 7),
    (0, 1, 6, 7, 2, 3, 4, 5),
    (0, 1, 2, 3, 4, 5, 6, 7),
)
EARLY = (3, 2, 2, 2)
ARRIVALS = ((0, 1, 2, 3), (1, 0, 3, 2), (2, 3, 0, 1), (3, 2, 1, 0))
SENDS = ((0, 1, 2, 3), (1, 3, 2, 0), (2, 0, 1, 3), (3, 2, 1, 0))
SLOTS = tuple(
    tuple(ARRIVALS[to].index(place) for to in SENDS[place]) for place in range(len(SENDS))
)


def pick(row, z):
    value = jnp.int32(row[0])
    for place in range(1, len(row)):
        value = jnp.where(z == place, row[place], value)
    return value


def fused_kernel(
    places,
    groups,
    tokens_ref,
    norm_gain_ref,
    freqs_ref,
    pool_ref,
    query_ref,
    key_ref,
    value_ref,
    map_ref,
    scale_ref,
    gain_ref,
    lambda_ref,
    out_pool_ref,
    out_heads_ref,
    out_ref,
    own_tokens,
    own_map,
    cos_ref,
    sin_ref,
    rows_all,
    weights,
    outs,
    queries,
    keys,
    values,
    pools,
    features,
    mine,
    to_mate,
    from_mate,
    kept,
    to_peer,
    from_peer,
    merging,
    final,
    *sems,
):
    (
        own_sem,
        in_local,
        in_z_send,
        in_z_recv,
        in_n_send,
        in_n_recv,
        in_rest,
        out_local,
        out_z_send,
        out_z_recv,
        out_n_send,
        out_n_recv,
        out_rest,
        token_send,
        token_recv,
        mate_recv,
        half_send,
        half_recv,
        peer_send,
        peer_recv,
        merge_recv,
    ) = sems
    z = lax.axis_index("sp")
    f = lax.axis_index("fs")
    c = lax.axis_index("tp")
    fx = f + 1 - 2 * lax.rem(f, 2)
    fy = lax.rem(f + 2, groups)
    mate = 1 - c
    half_rows = tokens_ref.shape[0] // 2
    row_count = 2 * half_rows
    depth = pool_ref.shape[0]
    width = GROUP_DIM
    out_width = out_pool_ref.shape[1]
    half_out = out_ref.shape[1]
    length = places * row_count

    send_to = [pick([row[d] for row in SENDS], z) for d in range(places)]
    send_slot = [pick([row[d] for row in SLOTS], z) for d in range(places)]
    source = [pick([row[d] for row in ARRIVALS], z) for d in range(places)]

    def block(index, size):
        return pl.ds(pl.multiple_of(index * size, size), size)

    barrier = pltpu.get_barrier_semaphore()
    partners = [{"sp": lax.rem(z + d, places)} for d in range(1, places)]
    partners += [{"fs": fx}, {"fs": fy}, {"tp": mate}]
    for partner in partners:
        pl.semaphore_signal(barrier, inc=1, device_id=partner, device_id_type=MESH)

    def remote(source, target, send, recv, device):
        return pltpu.make_async_remote_copy(
            src_ref=source,
            dst_ref=target,
            send_sem=send,
            recv_sem=recv,
            device_id=device,
            device_id_type=MESH,
        )

    class Gather:
        def __init__(self, sources, cut, view, sent, received, group):
            self.sources, self.cut, self.view = sources, cut, view
            self.sent, self.received = sent, received
            self.count = len(sources)
            (
                self.local,
                self.z_send,
                self.z_recv,
                self.n_send,
                self.n_recv,
                self.rest,
            ) = group
            self.low = (0, self.count // 2)
            self.high = (self.count // 2, self.count - self.count // 2)

        def own(self, m):
            return pltpu.make_async_copy(
                self.cut(self.sources[m], z), self.view(z, f, m, 1).at[0], self.local.at[m]
            )

        def across(self, d, m):
            to, slot = send_to[d], send_slot[d]
            return remote(
                self.cut(self.sources[m], to),
                self.view(z, f, m, 1).at[0],
                self.z_send.at[d],
                self.z_recv.at[slot],
                {"sp": to},
            )

        def arrive(self, d):
            view = self.view(source[d], f, 0, self.count)
            return remote(view, view, self.z_send.at[d], self.z_recv.at[d], {"sp": source[d]})

        def near(self, d, side, column, half):
            start, size = (self.low, self.high)[half]
            view = self.view(source[d], column, start, size)
            early = half == side
            return remote(
                view,
                view,
                self.n_send.at[side],
                self.n_recv.at[side, d] if early else self.rest.at[d // 2],
                {"fs": (fx, fy)[side]},
            )

        def forward(self, d, side, column):
            start, size = (self.high, self.low)[side]
            view = self.view(source[d], column, start, size)
            return remote(
                view, view, self.n_send.at[side], self.rest.at[d // 2], {"fs": (fx, fy)[side]}
            )

        def start_own(self):
            for m in range(self.count):
                self.own(m).start()

        def start(self, d):
            for m in range(self.count):
                self.across(d, m).start()

        def first(self, d):
            if d == 0:
                for m in range(self.count):
                    self.own(m).wait()
            else:
                self.arrive(d).wait_recv()
            for order in range(2):
                for side in range(2):
                    self.near(d, side, f, side ^ order).start()

        def second(self, d):
            self.near(d, 0, fx, 0).wait_recv()
            self.forward(d, 1, fx).start()
            self.near(d, 1, fy, 1).wait_recv()
            self.forward(d, 0, fy).start()

        def third(self, part):
            remote(
                self.received, self.received, self.n_send.at[0], self.rest.at[part], {"fs": fx}
            ).wait_recv()

        def drain(self):
            for d in range(1, places):
                self.arrive(d).wait_send()
            for side in range(2):
                remote(
                    self.sent, self.sent, self.n_send.at[side], self.rest.at[0], {"fs": fx}
                ).wait_send()

    filled = places * groups
    inward = Gather(
        (pool_ref, query_ref, key_ref, value_ref),
        lambda ref, to: ref.at[:, block(to, width)],
        lambda zz, ff, m, n: weights.at[pl.ds(m, n), block(zz * groups + ff, depth), :],
        weights.at[:, pl.ds(0, filled * 3 // 8 * depth), :],
        weights.at[:, pl.ds(0, filled // 4 * depth), :],
        (in_local, in_z_send, in_z_recv, in_n_send, in_n_recv, in_rest),
    )
    outward = Gather(
        (out_pool_ref, out_heads_ref),
        lambda ref, to: ref.at[block(to, width), :],
        lambda zz, ff, m, n: outs.at[pl.ds(m, n), :, block(zz * groups + ff, out_width)],
        outs.at[:, :, pl.ds(0, filled * 3 // 8 * out_width)],
        outs.at[:, :, pl.ds(0, filled // 4 * out_width)],
        (out_local, out_z_send, out_z_recv, out_n_send, out_n_recv, out_rest),
    )

    piece_rows = half_rows // PIECES

    def chunk(b, side, p):
        return rows_all.at[block((2 * b + side) * PIECES + p, piece_rows), :]

    def right(b, p, step=1):
        view = chunk(b, c, p)
        return remote(view, view, token_send.at[0], token_recv.at[b, p], {"sp": z + step})

    def left(b, p, step=-1):
        view = chunk(b, c, p)
        return remote(view, view, token_send.at[1], token_recv.at[b, p], {"sp": z + step})

    def share(b, side, p):
        view = chunk(b, side, p)
        return remote(view, view, token_send.at[2], mate_recv.at[b], {"tp": mate})

    def sent_tokens(kind, blocks):
        view = rows_all.at[pl.ds(0, blocks * half_rows), :]
        return remote(view, view, token_send.at[kind], mate_recv.at[0], {"tp": mate})

    def each_place(act):
        for place in range(places):
            pl.when(z == place)(lambda place=place: act(place))

    def send_right(place, pieces=range(PIECES)):
        for p in pieces:
            right(place, p).start()

    def send_left(place):
        for p in range(PIECES):
            left(place, p).start()

    def take(place, b, pieces=range(PIECES)):
        for p in pieces:
            if b < place:
                right(b, p, -1).wait_recv()
                if place < places - 1:
                    right(b, p).start()
            else:
                left(b, p, 1).wait_recv()
                if place > 0:
                    left(b, p).start()
            share(b, c, p).start()

    first_half, second_half = range(PIECES // 2), range(PIECES // 2, PIECES)

    def prepare(place):
        for d in range(1, places):
            inward.start(d)
        for d in range(1, 2 if place == 0 else places):
            outward.start(d)

    def begin(place):
        if place == 0:
            send_right(place)
            for d in range(2, places):
                outward.start(d)
        if place == places - 1:
            send_left(place)
        for p in range(PIECES):
            share(place, c, p).start()

    def gather(place):
        inward.second(0)
        outward.second(0)
        inward.first(1)
        inward.first(2)
        if place == 0:
            inward.second(1)
            inward.first(3)
            inward.second(2)
            inward.second(3)
            outward.first(1)
            outward.first(2)
            take(place, 1)
        if place == 1:
            send_left(place)
            inward.second(1)
            outward.first(1)
            inward.second(2)
            take(place, 0, first_half)
            inward.first(3)
            outward.first(3)
            take(place, 0, second_half)
            send_right(place)
            outward.second(1)
            inward.second(3)
            outward.first(2)
            take(place, 2, first_half)
            outward.second(3)
            take(place, 2, second_half)
        if place == 2:
            send_right(place)
            send_left(place)
            inward.second(1)
            outward.first(1)
            inward.second(2)
            inward.first(3)
            outward.first(3)
            outward.second(1)
            take(place, 3, first_half)
            inward.second(3)
            take(place, 3, second_half)
            take(place, 0, first_half)
            outward.second(3)
            outward.first(2)
            take(place, 0, second_half)
        if place == 3:
            inward.second(1)
            inward.first(3)
            outward.first(1)
            inward.second(2)
            outward.first(2)
            inward.second(3)
            outward.second(1)
            outward.first(3)
            take(place, 2)
            outward.second(2)
        inward.third(0)
        inward.third(1)

    def more(place):
        if place == 0:
            outward.second(1)
            outward.first(3)
        if place in (1, 2):
            outward.second(2)
        if place == 3:
            outward.second(3)
            take(place, 0)

    def relay(place):
        if place == 0:
            outward.second(2)
        if place in (1, 2):
            take(place, (None, 3, 1, None)[place], first_half)

    def finish_gather(place):
        if place in (1, 2):
            take(place, (None, 3, 1, None)[place], second_half)
        outward.third(1)

    tokens_in = pltpu.make_async_copy(
        tokens_ref.at[block(c, half_rows), :], own_tokens, own_sem.at[0]
    )
    map_in = pltpu.make_async_copy(map_ref.at[z], own_map, own_sem.at[1])
    tokens_in.start()
    inward.start_own()
    outward.start_own()
    map_in.start()
    pl.semaphore_wait(barrier, len(partners))
    each_place(prepare)
    tokens_in.wait()
    floated = own_tokens[...].astype(jnp.float32)
    rows_all[block(2 * z + c, half_rows), :] = (
        floated
        * lax.rsqrt(jnp.mean(floated * floated, -1, keepdims=True) + NORM_EPS)
        * norm_gain_ref[...]
    ).astype(jnp.bfloat16)
    inward.first(0)
    outward.first(0)
    pools[0:16, :] = jnp.zeros((16, width), jnp.bfloat16)
    keys[...] = jnp.zeros_like(keys)
    values[...] = jnp.zeros_like(values)
    each_place(begin)

    def table(index, carry):
        rows = block(index, row_count)
        half = HEAD_DIM // 2
        count = (
            index * row_count + lax.broadcasted_iota(jnp.int32, (row_count, HEAD_DIM), 0)
        ).astype(jnp.float32)
        lane = lax.broadcasted_iota(jnp.int32, (row_count, HEAD_DIM), 1)
        angles = count * freqs_ref[...]
        cos_ref[rows, :] = jnp.cos(angles)
        sine = jnp.sin(angles)
        sin_ref[rows, :] = jnp.where(lane < half, -sine, sine)
        return carry

    lax.fori_loop(0, places, table, 0)

    def turned(raw, cosine, sine):
        floated = raw.astype(jnp.float32)
        return (floated * cosine + pltpu.roll(floated, HEAD_DIM // 2, 1) * sine).astype(
            jnp.bfloat16
        )

    projected = [pick([row[i] for row in PROJECTED], z) for i in range(places)]
    late = [pick([row[i] for row in LATE], z) for i in range(2)]
    finished = [pick([row[i] for row in FINISHED], z) for i in range(places * PARTS)]

    def project(index):
        theirs = rows_all.at[block(2 * index + mate, half_rows), :]
        remote(theirs, theirs, token_send.at[2], mate_recv.at[index], {"tp": mate}).wait_recv()
        rows = block(index, row_count)
        normed = rows_all[rows, :]
        cosine = cos_ref[rows, :]
        sine = sin_ref[rows, :]

        def product(m):
            return jnp.dot(normed, weights[m], preferred_element_type=jnp.float32).astype(
                jnp.bfloat16
            )

        pools[pl.ds(pl.multiple_of(index * row_count + 16, 16), row_count), :] = product(0)
        raw = product(1)
        for m in range(2):
            part = slice(m * HEAD_DIM, (m + 1) * HEAD_DIM)
            queries[rows, part] = turned(raw[:, part], cosine, sine)
        raw = product(2)
        for m in range(2):
            part = slice(m * HEAD_DIM, (m + 1) * HEAD_DIM)
            keys[rows, part] = turned(raw[:, part], cosine, sine)
        values[rows, :] = product(3)

    upper = z >= places // 2

    each_place(gather)
    project(projected[0])
    each_place(more)
    project(projected[1])
    each_place(relay)

    map_in.wait()
    outward.third(0)

    level = lax.rem(c * map_ref.shape[0] + z, 4)
    window = jnp.where(
        level == 0, 2, jnp.where(level == 1, 4, jnp.where(level == 2, 8, 16))
    )
    head_lambda = lambda_ref[c * map_ref.shape[0] + z]

    part_rows = row_count // PARTS

    def to_sibling(step):
        return remote(
            to_mate.at[step],
            from_mate.at[step],
            half_send.at[0],
            half_recv.at[step],
            {"tp": mate},
        )

    outer = (z == 0) | (z == places - 1)
    pair = z + 1 - 2 * lax.rem(z, 2)

    def crossing(to, h):
        return lax.rem(to, 2) * PARTS + h

    def to_inner(to, h):
        return remote(
            to_peer.at[to * PARTS + h],
            merging.at[crossing(to, h)],
            peer_send.at[0],
            merge_recv.at[crossing(to, h)],
            {"sp": pair},
        )

    def to_place(to, h):
        return remote(
            to_peer.at[to * PARTS + h],
            from_peer.at[h],
            peer_send.at[0],
            peer_recv.at[h],
            {"sp": to},
        )

    def to_pair(h):
        return remote(
            to_peer.at[pair * PARTS + h],
            from_peer.at[PARTS + h],
            peer_send.at[0],
            peer_recv.at[PARTS + h],
            {"sp": pair},
        )

    def step_place(step):
        slot = finished[0]
        for i in range(1, places * PARTS):
            slot = jnp.where(step == i, finished[i], slot)
        return slot // PARTS, lax.rem(slot, PARTS)

    def compute(step):
        to, h = step_place(step)
        slot = to * PARTS + h
        rows = block(slot, part_rows)
        query_pos = slot * part_rows + lax.broadcasted_iota(jnp.int32, (part_rows, length), 0)
        key_pos = lax.broadcasted_iota(jnp.int32, (part_rows, length), 1)
        seen = query_pos >= key_pos
        mapped = []
        for m in range(2):
            part = slice(m * HEAD_DIM, (m + 1) * HEAD_DIM)
            scores = lax.dot_general(
                queries[rows, part],
                keys[:, part],
                (((1,), (1,)), ((), ())),
                preferred_element_type=jnp.float32,
            ) * HEAD_DIM ** (-0.5)
            scores = jnp.where(seen, scores, -jnp.inf)
            expons = jnp.exp(scores - jnp.max(scores, -1, keepdims=True))
            totals = jnp.sum(expons, -1, keepdims=True)
            mapped.append(
                jnp.dot(
                    expons.astype(jnp.bfloat16), values[...], preferred_element_type=jnp.float32
                )
                / totals
            )
        raw = mapped[0] - head_lambda * mapped[1]
        attn = (
            raw
            * lax.rsqrt(jnp.mean(raw * raw, -1, keepdims=True) + HEAD_EPS)
            * gain_ref[...]
            * HEAD_SCALE
        ).astype(jnp.bfloat16)
        extended = pools[
            pl.ds(pl.multiple_of(slot * part_rows, 16), part_rows + 16), :
        ].astype(jnp.float32)
        picked = extended + pltpu.roll(extended, 1, 0)
        sums = picked
        for shift in (2, 4, 8):
            sums = sums + pltpu.roll(sums, shift, 0)
            picked = lax.select_n(window >= 2 * shift, picked, sums)
        places_of = slot * part_rows + lax.broadcasted_iota(jnp.int32, (part_rows, 1), 0)
        counts = jnp.minimum(places_of + 1, window).astype(jnp.float32)
        mixed = (picked[16:] / counts - extended[16:]).astype(jnp.bfloat16)
        pooled = (
            jnp.dot(mixed, own_map[...], preferred_element_type=jnp.float32) * scale_ref[z]
        ).astype(jnp.bfloat16)

        features[step] = jnp.concatenate([pooled, attn], 1)
        return pooled, attn

    def partial_of(step, pooled, attn, side):
        columns = block(side, half_out)
        value = jnp.dot(
            pooled, outs[0, :, columns], preferred_element_type=jnp.float32
        ) + jnp.dot(attn, outs[1, :, columns], preferred_element_type=jnp.float32)

        @pl.when(side == c)
        def _():
            mine[lax.rem(step, 2)] = value

        @pl.when(side != c)
        def _():
            to_mate[step] = value.astype(jnp.bfloat16)
            to_sibling(step).start()

    def finish(step):
        to, h = step_place(step)
        slot = to * PARTS + h
        crosses = to // 2 != z // 2
        to_sibling(step).wait_recv()
        summed = mine[lax.rem(step, 2)] + from_mate[step].astype(jnp.float32)

        @pl.when(to == z)
        def _():
            final[h] = summed

        @pl.when(to == pair)
        def _():
            to_peer[slot] = summed.astype(jnp.bfloat16)
            to_pair(h).start()

        @pl.when(crosses & outer)
        def _():
            to_peer[slot] = summed.astype(jnp.bfloat16)
            to_inner(to, h).start()

        @pl.when(crosses & jnp.logical_not(outer))
        def _():
            kept[crossing(to, h)] = summed

    def merge(turn):
        place = turn // PARTS
        to = jnp.where(upper, place, places // 2 + place)
        h = lax.rem(turn, PARTS)
        to_inner(to, h).wait_recv()
        to_peer[to * PARTS + h] = (
            kept[crossing(to, h)] + merging[crossing(to, h)].astype(jnp.float32)
        ).astype(jnp.bfloat16)
        to_place(to, h).start()

    side = z // (places // 2)
    eager = side == c
    early = pick(EARLY, z)
    merged = jnp.where(upper, jnp.where(eager, 3, 4), jnp.where(eager, 5, places * PARTS))

    def grow(step):
        @pl.when((step == late[0]) | (step == late[1]))
        def _():
            @pl.when((z == 0) & (step == late[0]))
            def _():
                outward.second(3)
                take(0, 2)

            @pl.when((z == 0) & (step == late[1]))
            def _():
                take(0, 3)

            @pl.when((z == places - 1) & (step == late[0]))
            def _():
                take(places - 1, 1)

            def project_late(i, carry):
                project(jnp.where(i == 2, projected[2], projected[3]))
                return carry

            lax.fori_loop(
                jnp.where(step == late[0], 2, 3), jnp.where(step == late[1], 4, 3), project_late, 0
            )

    def first_side(step, carry):
        grow(step)
        partial_of(step, *compute(step), side)

        @pl.when(eager & (step > 0))
        def _():
            finish(step - 1)

        return carry

    def second_side(step):
        pooled, attn = features[step, :, :width], features[step, :, width:]
        partial_of(step, pooled, attn, 1 - side)

    def other_side(step, carry):
        second_side(step)

        @pl.when(jnp.logical_not(eager) & (step > 0))
        def _():
            finish(step - 1)

        return carry

    def both_sides(step, carry):
        grow(step)
        partial_of(step, *compute(step), side)
        second_side(step)

        @pl.when(step > early)
        def _():
            finish(step - 1)

        @pl.when(jnp.logical_not(outer) & ((step == merged) | (step == merged + 1)))
        def _():
            merge(step - merged)

        return carry

    lax.fori_loop(0, early, first_side, 0)

    @pl.when(eager)
    def _():
        finish(early - 1)

    each_place(finish_gather)
    lax.fori_loop(0, early, other_side, 0)

    @pl.when(jnp.logical_not(eager))
    def _():
        finish(early - 1)

    def merge_more(turn, carry):
        merge(turn)
        return carry

    lax.fori_loop(early, places * PARTS, both_sides, 0)
    finish(places * PARTS - 1)

    @pl.when(jnp.logical_not(outer))
    def _():
        lax.fori_loop(jnp.where(upper | eager, PARTS, 0), 2 * PARTS, merge_more, 0)

    for h in range(PARTS):
        to_pair(h).wait_recv()
        total = final[h] + from_peer[PARTS + h].astype(jnp.float32)
        to_place(z, h).wait_recv()
        out_ref[h * part_rows : (h + 1) * part_rows, :] = (
            total + from_peer[h].astype(jnp.float32)
        ).astype(out_ref.dtype)

    inward.drain()
    outward.drain()

    def drain(place):
        if place < places - 1:
            sent_tokens(0, place + 1).wait_send()
        if place > 0:
            sent_tokens(1, places - place).wait_send()

    each_place(drain)
    sent_tokens(2, places).wait_send()
    remote(to_mate, from_mate, half_send.at[0], half_recv.at[0], {"tp": mate}).wait_send()
    sent = to_peer.at[pl.ds(0, (places - 1) * PARTS)]
    remote(sent, sent, peer_send.at[0], peer_recv.at[0], {"sp": pair}).wait_send()


def fused(
    tokens,
    norm_gain,
    pool_input,
    query_weight,
    key_weight,
    value_weight,
    pool_map,
    pool_scale,
    head_gain,
    diff_lambda,
    out_pool,
    out_heads,
):
    places = lax.axis_size("sp")
    groups = lax.axis_size("fs")
    row_count, model = tokens.shape[1], tokens.shape[2]
    length = places * row_count
    half = HEAD_DIM // 2
    freqs = np.float32(1.0) / np.float32(THETA) ** (
        np.arange(half, dtype=np.float32) * np.float32(2.0) / np.float32(HEAD_DIM)
    )
    freqs = jnp.asarray(np.concatenate([freqs, freqs])[None, :], jnp.float32)
    group_count = pool_map.shape[0]
    half_out = model // 2
    vmem = pl.BlockSpec(memory_space=pltpu.VMEM)
    smem = pl.BlockSpec(memory_space=pltpu.SMEM)
    hbm = pl.BlockSpec(memory_space=pl.ANY)
    dma = pltpu.SemaphoreType.DMA
    low = jnp.bfloat16

    def gather_sems(count):
        return [
            dma((count,)),
            dma((places,)),
            dma((places,)),
            dma((2,)),
            dma((2, places)),
            dma((2,)),
        ]

    out = pl.pallas_call(
        lambda *refs: fused_kernel(places, groups, *refs),
        out_shape=jax.ShapeDtypeStruct((row_count, half_out), low),
        in_specs=[hbm, vmem, vmem] + [hbm] * 5 + [vmem] * 2 + [smem] + [hbm] * 2,
        out_specs=vmem,
        scratch_shapes=[
            pltpu.VMEM((row_count // 2, model), low),
            pltpu.VMEM((GROUP_DIM, GROUP_DIM), low),
            pltpu.VMEM((length, HEAD_DIM), jnp.float32),
            pltpu.VMEM((length, HEAD_DIM), jnp.float32),
            pltpu.VMEM((length, model), low),
            pltpu.VMEM((4, model, GROUP_DIM), low),
            pltpu.VMEM((2, GROUP_DIM, model), low),
            pltpu.VMEM((length, GROUP_DIM), low),
            pltpu.VMEM((length, GROUP_DIM), low),
            pltpu.VMEM((length, GROUP_DIM), low),
            pltpu.VMEM((length + 16, GROUP_DIM), low),
            pltpu.VMEM((places * PARTS, row_count // PARTS, 2 * GROUP_DIM), low),
            pltpu.VMEM((2, row_count // PARTS, half_out), jnp.float32),
            pltpu.VMEM((places * PARTS, row_count // PARTS, half_out), low),
            pltpu.VMEM((places * PARTS, row_count // PARTS, half_out), low),
            pltpu.VMEM((2 * PARTS, row_count // PARTS, half_out), jnp.float32),
            pltpu.VMEM((places * PARTS, row_count // PARTS, half_out), low),
            pltpu.VMEM((2 * PARTS, row_count // PARTS, half_out), low),
            pltpu.VMEM((2 * PARTS, row_count // PARTS, half_out), low),
            pltpu.VMEM((PARTS, row_count // PARTS, half_out), jnp.float32),
            dma((2,)),
            *gather_sems(4),
            *gather_sems(2),
            dma((3,)),
            dma((places, PIECES)),
            dma((places,)),
            dma((1,)),
            dma((places * PARTS,)),
            dma((1,)),
            dma((2 * PARTS,)),
            dma((2 * PARTS,)),
        ],
        compiler_params=pltpu.CompilerParams(
            collective_id=0, has_side_effects=True, vmem_limit_bytes=56 * 1024 * 1024
        ),
    )(
        tokens[0],
        norm_gain.reshape(1, model),
        freqs,
        pool_input,
        query_weight,
        key_weight,
        value_weight,
        pool_map,
        pool_scale.reshape(group_count, 1, GROUP_DIM),
        head_gain.reshape(1, 2 * HEAD_DIM),
        diff_lambda,
        out_pool,
        out_heads,
    )
    return out[None]


def solution(mesh):
    placed = (
        P("fs", "sp", None),
        P(),
        P(("sp", "fs"), "tp"),
        P(("sp", "fs"), "tp"),
        P(("sp", "fs"), "tp"),
        P(("sp", "fs"), "tp"),
        P("tp", None, None),
        P("tp"),
        P(),
        P(),
        P("tp", ("sp", "fs")),
        P("tp", ("sp", "fs")),
    )
    shape = dict(mesh.shape)

    def body(tokens, *rest):
        head_count = rest[3].shape[1] // (2 * HEAD_DIM)
        group_count = rest[5].shape[0]
        fits = (
            shape["fs"] == 4
            and shape["tp"] == 2
            and shape["sp"] == head_count == group_count == 4
            and tokens.shape[0] == 1
        )
        return (fused if fits else local)(tokens, *rest)

    return jax.shard_map(
        body, mesh=mesh, in_specs=placed, out_specs=P("fs", "sp", "tp"), check_vma=False
    )
```

```python
import math

import jax
import jax.numpy as jnp
import numpy as np
from jax import lax
from jax.experimental import pallas as pl
from jax.experimental.pallas import tpu as pltpu
from jax.sharding import PartitionSpec as P

HEAD_DIM = 128
GROUP_DIM = 256


THETA = 500000.0
HEAD_SCALE = 0.8
NORM_EPS = 1e-06
HEAD_EPS = 1e-05


def from_behind(value, axis, steps):
    count = lax.axis_size(axis)
    first, last = (max(0, -steps), min(count, count - steps))
    return lax.ppermute(value, axis, [(source, source + steps) for source in range(first, last)])


def rotate(tensor, positions):
    half = HEAD_DIM // 2
    freqs = 1.0 / THETA ** (jnp.arange(half, dtype=jnp.float32) * 2.0 / HEAD_DIM)
    angles = positions[:, None] * freqs[None, :]
    cosine = jnp.cos(angles)[:, None, None, :]
    sine = jnp.sin(angles)[:, None, None, :]
    floated = tensor.astype(jnp.float32)
    first = floated[..., :half]
    second = floated[..., half:]
    turned = jnp.concatenate([first * cosine - second * sine, second * cosine + first * sine], -1)
    return turned.astype(jnp.bfloat16)


def local(
    tokens,
    norm_gain,
    pool_input,
    query_weight,
    key_weight,
    value_weight,
    pool_map,
    pool_scale,
    head_gain,
    diff_lambda,
    out_pool,
    out_heads,
):
    out_local = jnp.concatenate([out_pool, out_heads], 0)
    row_count = tokens.shape[1]
    floated = tokens[0].astype(jnp.float32)
    normed = (
        floated * lax.rsqrt(jnp.mean(floated * floated, -1, keepdims=True) + NORM_EPS) * norm_gain
    ).astype(jnp.bfloat16)
    fragments = (
        lax.all_gather(pool_input, ("sp", "fs"), axis=0, tiled=True),
        lax.all_gather(query_weight, ("sp", "fs"), axis=0, tiled=True),
        lax.all_gather(key_weight, ("sp", "fs"), axis=0, tiled=True),
        lax.all_gather(value_weight, ("sp", "fs"), axis=0, tiled=True),
    )
    projected = tuple(
        (jnp.dot(normed, fragment, preferred_element_type=jnp.float32) for fragment in fragments)
    )
    pool_in, queries, keys_flat, values_flat = [
        product.astype(jnp.bfloat16) for product in projected
    ]
    head_count = values_flat.shape[1] // (2 * HEAD_DIM)
    tp_index = lax.axis_index("tp")
    sp_index = lax.axis_index("sp")
    query_pos = sp_index * row_count + jnp.arange(row_count, dtype=jnp.int32)
    positions = query_pos.astype(jnp.float32)
    queries = rotate(queries.reshape(row_count, head_count, 2, HEAD_DIM), positions)
    keys_flat = rotate(keys_flat.reshape(row_count, head_count, 2, HEAD_DIM), positions).reshape(
        row_count, head_count * 2 * HEAD_DIM
    )
    lambdas = lax.dynamic_slice_in_dim(diff_lambda, tp_index * head_count, head_count, 0)

    def online_step(state, key_rows, value_rows, key_offset):
        largest, summed, accum = state
        width = key_rows.shape[0]
        shaped = key_rows.reshape(width, head_count, 2, HEAD_DIM)
        scores = jnp.einsum(
            "qhcd,khcd->chqk", queries, shaped, preferred_element_type=jnp.float32
        ) * HEAD_DIM ** (-0.5)
        key_pos = key_offset + jnp.arange(width, dtype=jnp.int32)
        scores = jnp.where(query_pos[:, None] >= key_pos[None, :], scores, -jnp.inf)
        newest = jnp.maximum(largest, jnp.max(scores, -1))
        anchor = jnp.where(jnp.isfinite(newest), newest, 0.0)
        rescale = jnp.exp(largest - anchor)
        expons = jnp.exp(scores - anchor[..., None])
        summed = summed * rescale + jnp.sum(expons, -1)
        value_shaped = value_rows.reshape(width, head_count, 2 * HEAD_DIM)
        added = jnp.einsum(
            "chqk,khe->chqe",
            expons.astype(jnp.bfloat16),
            value_shaped,
            preferred_element_type=jnp.float32,
        )
        accum = accum * rescale[..., None] + added
        return (newest, summed, accum)

    start_state = (
        jnp.full((2, head_count, row_count), -jnp.inf, jnp.float32),
        jnp.zeros((2, head_count, row_count), jnp.float32),
        jnp.zeros((2, head_count, row_count, 2 * HEAD_DIM), jnp.float32),
    )
    fragments = (
        lax.all_gather(keys_flat, "sp", axis=0, tiled=True),
        lax.all_gather(values_flat, "sp", axis=0, tiled=True),
    )
    span = math.gcd(fragments[0].shape[0], 1024)

    def inner_step(index, inner_state):
        key_rows = lax.dynamic_slice_in_dim(fragments[0], index * span, span, 0)
        value_rows = lax.dynamic_slice_in_dim(fragments[1], index * span, span, 0)
        return online_step(inner_state, key_rows, value_rows, index * span)

    final_state = lax.fori_loop(0, fragments[0].shape[0] // span, inner_step, start_state)
    summed_final = final_state[1]
    accum_final = final_state[2]
    heads_raw = (
        accum_final[0] / summed_final[0][..., None]
        - lambdas[:, None, None] * accum_final[1] / summed_final[1][..., None]
    )
    heads_raw = jnp.moveaxis(heads_raw, 0, 1)
    attn = (
        (
            heads_raw
            * lax.rsqrt(jnp.mean(heads_raw * heads_raw, -1, keepdims=True) + HEAD_EPS)
            * head_gain
            * HEAD_SCALE
        )
        .astype(jnp.bfloat16)
        .reshape(row_count, head_count * 2 * HEAD_DIM)
    )
    reach = 15
    rim_rows = from_behind(pool_in[row_count - reach :], "sp", 1)
    extended = jnp.concatenate([rim_rows, pool_in], 0).astype(jnp.float32)
    pair_sums = extended[1:] + extended[:-1]
    quad_sums = pair_sums[2:] + pair_sums[:-2]
    octet_sums = quad_sums[4:] + quad_sums[:-4]
    sixteen_sums = octet_sums[8:] + octet_sums[:-8]
    group_count = pool_in.shape[1] // GROUP_DIM
    stacked = jnp.stack(
        [
            pair_sums[14 : 14 + row_count],
            quad_sums[12 : 12 + row_count],
            octet_sums[8 : 8 + row_count],
            sixteen_sums,
        ],
        0,
    ).reshape(4, row_count, group_count, GROUP_DIM)
    levels = (tp_index * group_count + jnp.arange(group_count, dtype=jnp.int32)) % 4
    picked = jnp.sum(
        jnp.where(
            levels[None, None, :, None] == jnp.arange(4, dtype=jnp.int32)[:, None, None, None],
            stacked,
            0.0,
        ),
        0,
    )
    windows = 2 ** (1 + levels)
    counts = jnp.minimum(query_pos[:, None] + 1, windows[None, :]).astype(jnp.float32)
    window_mean = picked / counts[:, :, None]
    grouped = pool_in.reshape(row_count, group_count, GROUP_DIM).astype(jnp.float32)
    pool_mixed = (window_mean - grouped).astype(jnp.bfloat16)
    pooled = (
        (
            jnp.einsum("tgc,gce->tge", pool_mixed, pool_map, preferred_element_type=jnp.float32)
            * pool_scale.reshape(group_count, GROUP_DIM)
        )
        .astype(jnp.bfloat16)
        .reshape(row_count, group_count * GROUP_DIM)
    )
    branches = jnp.concatenate([pooled, attn], 1)
    partial_value = jnp.dot(
        branches,
        lax.all_gather(out_local, ("sp", "fs"), axis=1, tiled=True),
        preferred_element_type=jnp.float32,
    )
    layer_out = lax.psum_scatter(
        partial_value.astype(jnp.bfloat16), "tp", scatter_dimension=1, tiled=True
    )
    return layer_out[None]


MESH = pl.DeviceIdType.MESH
PIECES = 4
PARTS = 2

PROJECTED = ((0, 1, 2, 3), (1, 0, 2, 3), (2, 0, 3, 1), (3, 0, 2, 1))
LATE = ((2, 4), (0, 4), (2, 2), (2, 2))
FINISHED = (
    (2, 3, 4, 5, 6, 7, 0, 1),
    (4, 5, 0, 1, 6, 7, 2, 3),
    (0, 1, 6, 7, 2, 3, 4, 5),
    (0, 1, 2, 3, 4, 5, 6, 7),
)
EARLY = (4, 2, 2, 2)
SECOND = ((2, 3, 4, 5, 0, 1, 6, 7),) + 3 * ((0, 1, 2, 3, 4, 5, 6, 7),)
AHEAD = (2, 2, 2, 2)
ARRIVALS = ((0, 1, 2, 3), (1, 0, 3, 2), (2, 3, 0, 1), (3, 2, 1, 0))
SENDS = ((0, 1, 2, 3), (1, 3, 2, 0), (2, 0, 1, 3), (3, 2, 1, 0))
SLOTS = tuple(
    tuple(ARRIVALS[to].index(place) for to in SENDS[place]) for place in range(len(SENDS))
)


def pick(row, z):
    value = jnp.int32(row[0])
    for place in range(1, len(row)):
        value = jnp.where(z == place, row[place], value)
    return value


def fused_kernel(
    places,
    groups,
    tokens_ref,
    norm_gain_hbm,
    freqs_hbm,
    pool_ref,
    query_ref,
    key_ref,
    value_ref,
    map_ref,
    scale_hbm,
    gain_hbm,
    lambda_ref,
    out_pool_ref,
    out_heads_ref,
    out_ref,
    own_tokens,
    own_map,
    norm_gain_ref,
    freqs_ref,
    scale_ref,
    gain_ref,
    cos_ref,
    sin_ref,
    rows_all,
    weights,
    outs,
    queries,
    keys,
    values,
    pools,
    features,
    mine,
    to_mate,
    from_mate,
    kept,
    to_peer,
    from_peer,
    merging,
    final,
    *sems,
):
    (
        own_sem,
        small_sem,
        in_local,
        in_z_send,
        in_z_recv,
        in_n_send,
        in_n_recv,
        in_rest,
        out_local,
        out_z_send,
        out_z_recv,
        out_n_send,
        out_n_recv,
        out_rest,
        token_send,
        token_recv,
        mate_recv,
        half_send,
        half_recv,
        peer_send,
        peer_recv,
        merge_recv,
    ) = sems
    z = lax.axis_index("sp")
    f = lax.axis_index("fs")
    c = lax.axis_index("tp")
    fx = f + 1 - 2 * lax.rem(f, 2)
    fy = lax.rem(f + 2, groups)
    mate = 1 - c
    half_rows = tokens_ref.shape[0] // 2
    row_count = 2 * half_rows
    depth = pool_ref.shape[0]
    width = GROUP_DIM
    out_width = out_pool_ref.shape[1]
    half_out = out_ref.shape[1]
    length = places * row_count

    send_to = [pick([row[d] for row in SENDS], z) for d in range(places)]
    send_slot = [pick([row[d] for row in SLOTS], z) for d in range(places)]
    source = [pick([row[d] for row in ARRIVALS], z) for d in range(places)]

    def block(index, size):
        return pl.ds(pl.multiple_of(index * size, size), size)

    small = [
        pltpu.make_async_copy(source, target, small_sem.at[i])
        for i, (source, target) in enumerate(
            (
                (norm_gain_hbm, norm_gain_ref),
                (freqs_hbm, freqs_ref),
                (scale_hbm, scale_ref),
                (gain_hbm, gain_ref),
            )
        )
    ]
    barrier = pltpu.get_barrier_semaphore()
    partners = [{"sp": lax.rem(z + d, places)} for d in range(1, places)]
    partners += [{"fs": fx}, {"fs": fy}, {"tp": mate}]
    for partner in partners:
        pl.semaphore_signal(barrier, inc=1, device_id=partner, device_id_type=MESH)

    def remote(source, target, send, recv, device):
        return pltpu.make_async_remote_copy(
            src_ref=source,
            dst_ref=target,
            send_sem=send,
            recv_sem=recv,
            device_id=device,
            device_id_type=MESH,
        )

    class Gather:
        def __init__(self, sources, cut, view, sent, received, group):
            self.sources, self.cut, self.view = sources, cut, view
            self.sent, self.received = sent, received
            self.count = len(sources)
            (
                self.local,
                self.z_send,
                self.z_recv,
                self.n_send,
                self.n_recv,
                self.rest,
            ) = group
            self.low = (0, self.count // 2)
            self.high = (self.count // 2, self.count - self.count // 2)

        def own(self, m):
            return pltpu.make_async_copy(
                self.cut(self.sources[m], z), self.view(z, f, m, 1).at[0], self.local.at[m]
            )

        def across(self, d, m):
            to, slot = send_to[d], send_slot[d]
            return remote(
                self.cut(self.sources[m], to),
                self.view(z, f, m, 1).at[0],
                self.z_send.at[d],
                self.z_recv.at[slot],
                {"sp": to},
            )

        def arrive(self, d):
            view = self.view(source[d], f, 0, self.count)
            return remote(view, view, self.z_send.at[d], self.z_recv.at[d], {"sp": source[d]})

        def near(self, d, side, column, half):
            start, size = (self.low, self.high)[half]
            view = self.view(source[d], column, start, size)
            early = half == side
            return remote(
                view,
                view,
                self.n_send.at[side],
                self.n_recv.at[side, d] if early else self.rest.at[d // 2],
                {"fs": (fx, fy)[side]},
            )

        def forward(self, d, side, column):
            start, size = (self.high, self.low)[side]
            view = self.view(source[d], column, start, size)
            return remote(
                view, view, self.n_send.at[side], self.rest.at[d // 2], {"fs": (fx, fy)[side]}
            )

        def start_own(self):
            for m in range(self.count):
                self.own(m).start()

        def start(self, d):
            for m in range(self.count):
                self.across(d, m).start()

        def first(self, d):
            if d == 0:
                for m in range(self.count):
                    self.own(m).wait()
            else:
                self.arrive(d).wait_recv()
            for order in range(2):
                for side in range(2):
                    self.near(d, side, f, side ^ order).start()

        def second(self, d):
            self.near(d, 0, fx, 0).wait_recv()
            self.forward(d, 1, fx).start()
            self.near(d, 1, fy, 1).wait_recv()
            self.forward(d, 0, fy).start()

        def third(self, part):
            remote(
                self.received, self.received, self.n_send.at[0], self.rest.at[part], {"fs": fx}
            ).wait_recv()

        def drain(self):
            for d in range(1, places):
                self.arrive(d).wait_send()
            for side in range(2):
                remote(
                    self.sent, self.sent, self.n_send.at[side], self.rest.at[0], {"fs": fx}
                ).wait_send()

    filled = places * groups
    inward = Gather(
        (pool_ref, query_ref, key_ref, value_ref),
        lambda ref, to: ref.at[:, block(to, width)],
        lambda zz, ff, m, n: weights.at[pl.ds(m, n), block(zz * groups + ff, depth), :],
        weights.at[:, pl.ds(0, filled * 3 // 8 * depth), :],
        weights.at[:, pl.ds(0, filled // 4 * depth), :],
        (in_local, in_z_send, in_z_recv, in_n_send, in_n_recv, in_rest),
    )
    outward = Gather(
        (out_pool_ref, out_heads_ref),
        lambda ref, to: ref.at[block(to, width), :],
        lambda zz, ff, m, n: outs.at[pl.ds(m, n), :, block(zz * groups + ff, out_width)],
        outs.at[:, :, pl.ds(0, filled * 3 // 8 * out_width)],
        outs.at[:, :, pl.ds(0, filled // 4 * out_width)],
        (out_local, out_z_send, out_z_recv, out_n_send, out_n_recv, out_rest),
    )

    piece_rows = half_rows // PIECES

    def chunk(b, side, p):
        return rows_all.at[block((2 * b + side) * PIECES + p, piece_rows), :]

    def right(b, p, step=1):
        view = chunk(b, c, p)
        return remote(view, view, token_send.at[0], token_recv.at[b, p], {"sp": z + step})

    def left(b, p, step=-1):
        view = chunk(b, c, p)
        return remote(view, view, token_send.at[1], token_recv.at[b, p], {"sp": z + step})

    def share(b, side, p):
        view = chunk(b, side, p)
        return remote(view, view, token_send.at[2], mate_recv.at[b], {"tp": mate})

    def sent_tokens(kind, blocks):
        view = rows_all.at[pl.ds(0, blocks * half_rows), :]
        return remote(view, view, token_send.at[kind], mate_recv.at[0], {"tp": mate})

    def each_place(act):
        for place in range(places):
            pl.when(z == place)(lambda place=place: act(place))

    def send_right(place, pieces=range(PIECES)):
        for p in pieces:
            right(place, p).start()

    def send_left(place):
        for p in range(PIECES):
            left(place, p).start()

    def take(place, b, pieces=range(PIECES)):
        for p in pieces:
            if b < place:
                right(b, p, -1).wait_recv()
                if place < places - 1:
                    right(b, p).start()
            else:
                left(b, p, 1).wait_recv()
                if place > 0:
                    left(b, p).start()
            share(b, c, p).start()

    first_half, second_half = range(PIECES // 2), range(PIECES // 2, PIECES)

    def prepare(place):
        for d in range(1, places):
            inward.start(d)
        for d in range(1, 2 if place == 0 else places):
            outward.start(d)

    def begin(place):
        if place == 0:
            send_right(place)
        if place == places - 1:
            send_left(place)
        for p in range(PIECES):
            share(place, c, p).start()

    def gather(place):
        inward.second(0)
        outward.second(0)
        inward.first(1)
        inward.first(2)
        if place == 0:
            inward.second(1)
            inward.first(3)
            inward.second(2)
            inward.second(3)
            outward.first(1)
            outward.first(2)
            take(place, 1)
            outward.second(1)
            for d in range(2, places):
                outward.start(d)
        if place == 1:
            send_left(place)
            inward.second(1)
            outward.first(1)
            inward.second(2)
            take(place, 0, first_half)
            inward.first(3)
            take(place, 0, second_half)
            send_right(place)
            outward.first(3)
            outward.second(1)
            inward.second(3)
            outward.first(2)
            take(place, 2, first_half)
            outward.second(3)
            take(place, 2, second_half)
        if place == 2:
            send_right(place)
            send_left(place)
            inward.second(1)
            outward.first(1)
            inward.second(2)
            inward.first(3)
            outward.first(3)
            outward.second(1)
            take(place, 0, first_half)
            inward.second(3)
            take(place, 0, second_half)
            outward.second(3)
            take(place, 3)
        if place == 3:
            inward.second(1)
            inward.first(3)
            outward.first(1)
            inward.second(2)
            outward.first(2)
            inward.second(3)
            outward.second(1)
            take(place, 2)
            outward.second(2)
        inward.third(0)
        inward.third(1)

    def relay_piece(p):
        def act(place):
            if place in (1, 2):
                take(place, (None, 3, 1, None)[place], (p,))

        each_place(act)

    def more(place):
        if place == 0:
            outward.first(3)
        if place == 1:
            outward.second(2)
        if place == 2:
            outward.first(2)
        if place == 3:
            take(place, 0)

    def relay(place):
        if place in (0, 2):
            outward.second(2)
        if place == 3:
            outward.first(3)

    def finish_gather(place):
        if place in (1, 2):
            take(place, (None, 3, 1, None)[place], second_half[1:])
        if place == places - 1:
            outward.second(3)
        outward.third(1)

    tokens_in = pltpu.make_async_copy(
        tokens_ref.at[block(c, half_rows), :], own_tokens, own_sem.at[0]
    )
    map_in = pltpu.make_async_copy(map_ref.at[z], own_map, own_sem.at[1])
    tokens_in.start()
    for copy in small:
        copy.start()
    inward.start_own()
    outward.start_own()
    map_in.start()
    pl.semaphore_wait(barrier, len(partners))
    each_place(prepare)
    tokens_in.wait()
    for copy in small:
        copy.wait()
    floated = own_tokens[...].astype(jnp.float32)
    rows_all[block(2 * z + c, half_rows), :] = (
        floated
        * lax.rsqrt(jnp.mean(floated * floated, -1, keepdims=True) + NORM_EPS)
        * norm_gain_ref[...]
    ).astype(jnp.bfloat16)
    inward.first(0)
    outward.first(0)
    pools[0:16, :] = jnp.zeros((16, width), jnp.bfloat16)
    keys[...] = jnp.zeros_like(keys)
    values[...] = jnp.zeros_like(values)
    each_place(begin)

    def table(index, carry):
        rows = block(index, row_count)
        half = HEAD_DIM // 2
        count = (
            index * row_count + lax.broadcasted_iota(jnp.int32, (row_count, HEAD_DIM), 0)
        ).astype(jnp.float32)
        lane = lax.broadcasted_iota(jnp.int32, (row_count, HEAD_DIM), 1)
        angles = count * freqs_ref[...]
        cos_ref[rows, :] = jnp.cos(angles)
        sine = jnp.sin(angles)
        sin_ref[rows, :] = jnp.where(lane < half, -sine, sine)
        return carry

    lax.fori_loop(0, places, table, 0)

    def turned(raw, cosine, sine):
        floated = raw.astype(jnp.float32)
        return (floated * cosine + pltpu.roll(floated, HEAD_DIM // 2, 1) * sine).astype(
            jnp.bfloat16
        )

    projected = [pick([row[i] for row in PROJECTED], z) for i in range(places)]
    late = [pick([row[i] for row in LATE], z) for i in range(2)]
    finished = [pick([row[i] for row in FINISHED], z) for i in range(places * PARTS)]

    def project(index):
        theirs = rows_all.at[block(2 * index + mate, half_rows), :]
        remote(theirs, theirs, token_send.at[2], mate_recv.at[index], {"tp": mate}).wait_recv()
        rows = block(index, row_count)
        normed = rows_all[rows, :]
        cosine = cos_ref[rows, :]
        sine = sin_ref[rows, :]

        def product(m):
            return jnp.dot(normed, weights[m], preferred_element_type=jnp.float32).astype(
                jnp.bfloat16
            )

        pools[pl.ds(pl.multiple_of(index * row_count + 16, 16), row_count), :] = product(0)
        raw = product(1)
        for m in range(2):
            part = slice(m * HEAD_DIM, (m + 1) * HEAD_DIM)
            queries[rows, part] = turned(raw[:, part], cosine, sine)
        raw = product(2)
        for m in range(2):
            part = slice(m * HEAD_DIM, (m + 1) * HEAD_DIM)
            keys[rows, part] = turned(raw[:, part], cosine, sine)
        values[rows, :] = product(3)

    upper = z >= places // 2

    each_place(gather)
    project(projected[0])
    each_place(more)
    relay_piece(0)
    project(projected[1])
    each_place(relay)
    relay_piece(1)

    map_in.wait()
    outward.third(0)

    level = lax.rem(c * map_ref.shape[0] + z, 4)
    window = jnp.where(
        level == 0, 2, jnp.where(level == 1, 4, jnp.where(level == 2, 8, 16))
    )
    head_lambda = lambda_ref[c * map_ref.shape[0] + z]

    part_rows = row_count // PARTS

    def to_sibling(step):
        return remote(
            to_mate.at[step],
            from_mate.at[step],
            half_send.at[0],
            half_recv.at[step],
            {"tp": mate},
        )

    outer = (z == 0) | (z == places - 1)
    pair = z + 1 - 2 * lax.rem(z, 2)

    def crossing(to, h):
        return lax.rem(to, 2) * PARTS + h

    def to_inner(to, h):
        return remote(
            to_peer.at[to * PARTS + h],
            merging.at[crossing(to, h)],
            peer_send.at[0],
            merge_recv.at[crossing(to, h)],
            {"sp": pair},
        )

    def to_place(to, h):
        return remote(
            to_peer.at[to * PARTS + h],
            from_peer.at[h],
            peer_send.at[0],
            peer_recv.at[h],
            {"sp": to},
        )

    def to_pair(h):
        return remote(
            to_peer.at[pair * PARTS + h],
            from_peer.at[PARTS + h],
            peer_send.at[0],
            peer_recv.at[PARTS + h],
            {"sp": pair},
        )

    def step_place(step):
        slot = finished[0]
        for i in range(1, places * PARTS):
            slot = jnp.where(step == i, finished[i], slot)
        return slot // PARTS, lax.rem(slot, PARTS)

    def compute(step):
        to, h = step_place(step)
        slot = to * PARTS + h
        rows = block(slot, part_rows)
        query_pos = slot * part_rows + lax.broadcasted_iota(jnp.int32, (part_rows, length), 0)
        key_pos = lax.broadcasted_iota(jnp.int32, (part_rows, length), 1)
        seen = query_pos >= key_pos
        mapped = []
        for m in range(2):
            part = slice(m * HEAD_DIM, (m + 1) * HEAD_DIM)
            scores = lax.dot_general(
                queries[rows, part],
                keys[:, part],
                (((1,), (1,)), ((), ())),
                preferred_element_type=jnp.float32,
            ) * HEAD_DIM ** (-0.5)
            scores = jnp.where(seen, scores, -jnp.inf)
            expons = jnp.exp(scores - jnp.max(scores, -1, keepdims=True))
            totals = jnp.sum(expons, -1, keepdims=True)
            mapped.append(
                jnp.dot(
                    expons.astype(jnp.bfloat16), values[...], preferred_element_type=jnp.float32
                )
                / totals
            )
        raw = mapped[0] - head_lambda * mapped[1]
        attn = (
            raw
            * lax.rsqrt(jnp.mean(raw * raw, -1, keepdims=True) + HEAD_EPS)
            * gain_ref[...]
            * HEAD_SCALE
        ).astype(jnp.bfloat16)
        extended = pools[
            pl.ds(pl.multiple_of(slot * part_rows, 16), part_rows + 16), :
        ].astype(jnp.float32)
        picked = extended + pltpu.roll(extended, 1, 0)
        sums = picked
        for shift in (2, 4, 8):
            sums = sums + pltpu.roll(sums, shift, 0)
            picked = lax.select_n(window >= 2 * shift, picked, sums)
        places_of = slot * part_rows + lax.broadcasted_iota(jnp.int32, (part_rows, 1), 0)
        counts = jnp.minimum(places_of + 1, window).astype(jnp.float32)
        mixed = (picked[16:] / counts - extended[16:]).astype(jnp.bfloat16)
        pooled = (
            jnp.dot(mixed, own_map[...], preferred_element_type=jnp.float32) * scale_ref[z]
        ).astype(jnp.bfloat16)

        features[step] = jnp.concatenate([pooled, attn], 1)
        return pooled, attn

    def partial_of(step, turn, pooled, attn, side):
        columns = block(side, half_out)
        value = jnp.dot(
            pooled, outs[0, :, columns], preferred_element_type=jnp.float32
        ) + jnp.dot(attn, outs[1, :, columns], preferred_element_type=jnp.float32)

        @pl.when(side == c)
        def _():
            mine[lax.rem(turn, 2)] = value

        @pl.when(side != c)
        def _():
            to_mate[step] = value.astype(jnp.bfloat16)
            to_sibling(step).start()

    def finish(step, turn):
        to, h = step_place(step)
        slot = to * PARTS + h
        crosses = to // 2 != z // 2
        to_sibling(step).wait_recv()
        summed = mine[lax.rem(turn, 2)] + from_mate[step].astype(jnp.float32)

        @pl.when(to == z)
        def _():
            final[h] = summed

        @pl.when(to == pair)
        def _():
            to_peer[slot] = summed.astype(jnp.bfloat16)
            to_pair(h).start()

        @pl.when(crosses & outer)
        def _():
            to_peer[slot] = summed.astype(jnp.bfloat16)
            to_inner(to, h).start()

        @pl.when(crosses & jnp.logical_not(outer))
        def _():
            kept[crossing(to, h)] = summed

    def merge(turn):
        place = turn // PARTS
        to = jnp.where(upper, place, places // 2 + place)
        h = lax.rem(turn, PARTS)
        to_inner(to, h).wait_recv()
        to_peer[to * PARTS + h] = (
            kept[crossing(to, h)] + merging[crossing(to, h)].astype(jnp.float32)
        ).astype(jnp.bfloat16)
        to_place(to, h).start()

    side = z // (places // 2)
    eager = side == c
    early = pick(EARLY, z)
    merged = jnp.where(upper, jnp.where(eager, 2, 3), jnp.where(eager, 3, 5))
    lag = jnp.where(outer, 0, 1)

    def grow(step):
        @pl.when((step == late[0]) | (step == late[1]))
        def _():
            @pl.when((z == 0) & (step == late[0]))
            def _():
                outward.second(3)
                take(0, 2)

            @pl.when((z == 0) & (step == late[1]))
            def _():
                take(0, 3)

            def project_late(i, carry):
                @pl.when((z == places - 1) & (i == 3))
                def _():
                    take(places - 1, 1)

                project(jnp.where(i == 2, projected[2], projected[3]))
                return carry

            lax.fori_loop(
                jnp.where(step == late[0], 2, 3), jnp.where(step == late[1], 4, 3), project_late, 0
            )

    ahead = pick(AHEAD, z)
    last = places * PARTS - 1
    seconds = [pick([row[i] for row in SECOND], z) for i in range(places * PARTS)]

    def second_step(turn):
        step = seconds[0]
        for i in range(1, places * PARTS):
            step = jnp.where(turn == i, seconds[i], step)
        return step

    def first_side(step, carry):
        grow(step)

        @pl.when(step == 1)
        def _():
            relay_piece(2)

        partial_of(step, step, *compute(step), side)

        @pl.when(eager & (step >= lag))
        def _():
            finish(step - lag, step - lag)

        return carry

    def second_side(turn):
        step = second_step(turn)
        pooled, attn = features[step, :, :width], features[step, :, width:]
        partial_of(step, turn, pooled, attn, 1 - side)

    def other_side(turn, carry):
        second_side(turn)

        @pl.when(jnp.logical_not(eager) & (turn > 0))
        def _():
            finish(second_step(turn - 1), turn - 1)

        return carry

    def both_sides(step, carry):
        grow(step)
        partial_of(step, step, *compute(step), side)
        at_once = eager & outer & (step == early)

        @pl.when(at_once)
        def _():
            finish(step, step)

        second_side(step - early + ahead)

        @pl.when((step != early + 1 - lag) & jnp.logical_not(at_once))
        def _():
            first = jnp.where(step == early, step, step - 1)
            turn = first - early + ahead
            finish(jnp.where(eager, first, second_step(turn)), jnp.where(eager, first, turn))

        again = upper & (step == last)

        @pl.when(jnp.logical_not(outer) & ((step == merged) | (step == merged + 1) | again))
        def _():
            merge(jnp.where(again, PARTS, step - merged))

        return carry

    lax.fori_loop(0, early, first_side, 0)
    each_place(finish_gather)

    @pl.when(eager & jnp.logical_not(outer))
    def _():
        finish(early - 1, early - 1)

    lax.fori_loop(0, ahead, other_side, 0)

    @pl.when(jnp.logical_not(eager))
    def _():
        finish(second_step(ahead - 1), ahead - 1)

    def merge_more(turn, carry):
        merge(turn)
        return carry

    lax.fori_loop(early, places * PARTS, both_sides, 0)
    def second_more(turn, carry):
        second_side(turn)

        @pl.when(jnp.logical_not(eager))
        def _():
            finish(second_step(turn - 1), turn - 1)

        return carry

    lax.fori_loop(last + 1 - early + ahead, last + 1, second_more, 0)
    finish(jnp.where(eager, last, second_step(last)), last)

    @pl.when(jnp.logical_not(outer))
    def _():
        lax.fori_loop(jnp.where(upper, PARTS + 1, PARTS), 2 * PARTS, merge_more, 0)

    for h in range(PARTS):
        to_pair(h).wait_recv()
        total = final[h] + from_peer[PARTS + h].astype(jnp.float32)
        to_place(z, h).wait_recv()
        out_ref[h * part_rows : (h + 1) * part_rows, :] = (
            total + from_peer[h].astype(jnp.float32)
        ).astype(out_ref.dtype)

    inward.drain()
    outward.drain()

    def drain(place):
        if place < places - 1:
            sent_tokens(0, place + 1).wait_send()
        if place > 0:
            sent_tokens(1, places - place).wait_send()

    each_place(drain)
    sent_tokens(2, places).wait_send()
    remote(to_mate, from_mate, half_send.at[0], half_recv.at[0], {"tp": mate}).wait_send()
    sent = to_peer.at[pl.ds(0, (places - 1) * PARTS)]
    remote(sent, sent, peer_send.at[0], peer_recv.at[0], {"sp": pair}).wait_send()


def fused(
    tokens,
    norm_gain,
    pool_input,
    query_weight,
    key_weight,
    value_weight,
    pool_map,
    pool_scale,
    head_gain,
    diff_lambda,
    out_pool,
    out_heads,
):
    places = lax.axis_size("sp")
    groups = lax.axis_size("fs")
    row_count, model = tokens.shape[1], tokens.shape[2]
    length = places * row_count
    half = HEAD_DIM // 2
    freqs = np.float32(1.0) / np.float32(THETA) ** (
        np.arange(half, dtype=np.float32) * np.float32(2.0) / np.float32(HEAD_DIM)
    )
    freqs = jnp.asarray(np.concatenate([freqs, freqs])[None, :], jnp.float32)
    group_count = pool_map.shape[0]
    half_out = model // 2
    vmem = pl.BlockSpec(memory_space=pltpu.VMEM)
    smem = pl.BlockSpec(memory_space=pltpu.SMEM)
    hbm = pl.BlockSpec(memory_space=pl.ANY)
    dma = pltpu.SemaphoreType.DMA
    low = jnp.bfloat16

    def gather_sems(count):
        return [
            dma((count,)),
            dma((places,)),
            dma((places,)),
            dma((2,)),
            dma((2, places)),
            dma((2,)),
        ]

    out = pl.pallas_call(
        lambda *refs: fused_kernel(places, groups, *refs),
        out_shape=jax.ShapeDtypeStruct((row_count, half_out), low),
        in_specs=[hbm] * 10 + [smem] + [hbm] * 2,
        out_specs=vmem,
        scratch_shapes=[
            pltpu.VMEM((row_count // 2, model), low),
            pltpu.VMEM((GROUP_DIM, GROUP_DIM), low),
            pltpu.VMEM((1, model), jnp.float32),
            pltpu.VMEM((1, HEAD_DIM), jnp.float32),
            pltpu.VMEM((group_count, 1, GROUP_DIM), jnp.float32),
            pltpu.VMEM((1, 2 * HEAD_DIM), jnp.float32),
            pltpu.VMEM((length, HEAD_DIM), jnp.float32),
            pltpu.VMEM((length, HEAD_DIM), jnp.float32),
            pltpu.VMEM((length, model), low),
            pltpu.VMEM((4, model, GROUP_DIM), low),
            pltpu.VMEM((2, GROUP_DIM, model), low),
            pltpu.VMEM((length, GROUP_DIM), low),
            pltpu.VMEM((length, GROUP_DIM), low),
            pltpu.VMEM((length, GROUP_DIM), low),
            pltpu.VMEM((length + 16, GROUP_DIM), low),
            pltpu.VMEM((places * PARTS, row_count // PARTS, 2 * GROUP_DIM), low),
            pltpu.VMEM((2, row_count // PARTS, half_out), jnp.float32),
            pltpu.VMEM((places * PARTS, row_count // PARTS, half_out), low),
            pltpu.VMEM((places * PARTS, row_count // PARTS, half_out), low),
            pltpu.VMEM((2 * PARTS, row_count // PARTS, half_out), jnp.float32),
            pltpu.VMEM((places * PARTS, row_count // PARTS, half_out), low),
            pltpu.VMEM((2 * PARTS, row_count // PARTS, half_out), low),
            pltpu.VMEM((2 * PARTS, row_count // PARTS, half_out), low),
            pltpu.VMEM((PARTS, row_count // PARTS, half_out), jnp.float32),
            dma((2,)),
            dma((4,)),
            *gather_sems(4),
            *gather_sems(2),
            dma((3,)),
            dma((places, PIECES)),
            dma((places,)),
            dma((1,)),
            dma((places * PARTS,)),
            dma((1,)),
            dma((2 * PARTS,)),
            dma((2 * PARTS,)),
        ],
        compiler_params=pltpu.CompilerParams(
            collective_id=0, has_side_effects=True, vmem_limit_bytes=56 * 1024 * 1024
        ),
    )(
        tokens[0],
        norm_gain.reshape(1, model),
        freqs,
        pool_input,
        query_weight,
        key_weight,
        value_weight,
        pool_map,
        pool_scale.reshape(group_count, 1, GROUP_DIM),
        head_gain.reshape(1, 2 * HEAD_DIM),
        diff_lambda,
        out_pool,
        out_heads,
    )
    return out[None]


def solution(mesh):
    placed = (
        P("fs", "sp", None),
        P(),
        P(("sp", "fs"), "tp"),
        P(("sp", "fs"), "tp"),
        P(("sp", "fs"), "tp"),
        P(("sp", "fs"), "tp"),
        P("tp", None, None),
        P("tp"),
        P(),
        P(),
        P("tp", ("sp", "fs")),
        P("tp", ("sp", "fs")),
    )
    shape = dict(mesh.shape)

    def body(tokens, *rest):
        head_count = rest[3].shape[1] // (2 * HEAD_DIM)
        group_count = rest[5].shape[0]
        fits = (
            shape["fs"] == 4
            and shape["tp"] == 2
            and shape["sp"] == head_count == group_count == 4
            and tokens.shape[0] == 1
        )
        return (fused if fits else local)(tokens, *rest)

    return jax.shard_map(
        body, mesh=mesh, in_specs=placed, out_specs=P("fs", "sp", "tp"), check_vma=False
    )
```

```python
import math

import jax
import jax.numpy as jnp
import numpy as np
from jax import lax
from jax.experimental import pallas as pl
from jax.experimental.pallas import tpu as pltpu
from jax.sharding import PartitionSpec as P

HEAD_DIM = 128
GROUP_DIM = 256


THETA = 500000.0
HEAD_SCALE = 0.8
NORM_EPS = 1e-06
HEAD_EPS = 1e-05


def from_behind(value, axis, steps):
    count = lax.axis_size(axis)
    first, last = (max(0, -steps), min(count, count - steps))
    return lax.ppermute(value, axis, [(source, source + steps) for source in range(first, last)])


def rotate(tensor, positions):
    half = HEAD_DIM // 2
    freqs = 1.0 / THETA ** (jnp.arange(half, dtype=jnp.float32) * 2.0 / HEAD_DIM)
    angles = positions[:, None] * freqs[None, :]
    cosine = jnp.cos(angles)[:, None, None, :]
    sine = jnp.sin(angles)[:, None, None, :]
    floated = tensor.astype(jnp.float32)
    first = floated[..., :half]
    second = floated[..., half:]
    turned = jnp.concatenate([first * cosine - second * sine, second * cosine + first * sine], -1)
    return turned.astype(jnp.bfloat16)


def local(
    tokens,
    norm_gain,
    pool_input,
    query_weight,
    key_weight,
    value_weight,
    pool_map,
    pool_scale,
    head_gain,
    diff_lambda,
    out_pool,
    out_heads,
):
    out_local = jnp.concatenate([out_pool, out_heads], 0)
    row_count = tokens.shape[1]
    floated = tokens[0].astype(jnp.float32)
    normed = (
        floated * lax.rsqrt(jnp.mean(floated * floated, -1, keepdims=True) + NORM_EPS) * norm_gain
    ).astype(jnp.bfloat16)
    fragments = (
        lax.all_gather(pool_input, ("sp", "fs"), axis=0, tiled=True),
        lax.all_gather(query_weight, ("sp", "fs"), axis=0, tiled=True),
        lax.all_gather(key_weight, ("sp", "fs"), axis=0, tiled=True),
        lax.all_gather(value_weight, ("sp", "fs"), axis=0, tiled=True),
    )
    projected = tuple(
        (jnp.dot(normed, fragment, preferred_element_type=jnp.float32) for fragment in fragments)
    )
    pool_in, queries, keys_flat, values_flat = [
        product.astype(jnp.bfloat16) for product in projected
    ]
    head_count = values_flat.shape[1] // (2 * HEAD_DIM)
    tp_index = lax.axis_index("tp")
    sp_index = lax.axis_index("sp")
    query_pos = sp_index * row_count + jnp.arange(row_count, dtype=jnp.int32)
    positions = query_pos.astype(jnp.float32)
    queries = rotate(queries.reshape(row_count, head_count, 2, HEAD_DIM), positions)
    keys_flat = rotate(keys_flat.reshape(row_count, head_count, 2, HEAD_DIM), positions).reshape(
        row_count, head_count * 2 * HEAD_DIM
    )
    lambdas = lax.dynamic_slice_in_dim(diff_lambda, tp_index * head_count, head_count, 0)

    def online_step(state, key_rows, value_rows, key_offset):
        largest, summed, accum = state
        width = key_rows.shape[0]
        shaped = key_rows.reshape(width, head_count, 2, HEAD_DIM)
        scores = jnp.einsum(
            "qhcd,khcd->chqk", queries, shaped, preferred_element_type=jnp.float32
        ) * HEAD_DIM ** (-0.5)
        key_pos = key_offset + jnp.arange(width, dtype=jnp.int32)
        scores = jnp.where(query_pos[:, None] >= key_pos[None, :], scores, -jnp.inf)
        newest = jnp.maximum(largest, jnp.max(scores, -1))
        anchor = jnp.where(jnp.isfinite(newest), newest, 0.0)
        rescale = jnp.exp(largest - anchor)
        expons = jnp.exp(scores - anchor[..., None])
        summed = summed * rescale + jnp.sum(expons, -1)
        value_shaped = value_rows.reshape(width, head_count, 2 * HEAD_DIM)
        added = jnp.einsum(
            "chqk,khe->chqe",
            expons.astype(jnp.bfloat16),
            value_shaped,
            preferred_element_type=jnp.float32,
        )
        accum = accum * rescale[..., None] + added
        return (newest, summed, accum)

    start_state = (
        jnp.full((2, head_count, row_count), -jnp.inf, jnp.float32),
        jnp.zeros((2, head_count, row_count), jnp.float32),
        jnp.zeros((2, head_count, row_count, 2 * HEAD_DIM), jnp.float32),
    )
    fragments = (
        lax.all_gather(keys_flat, "sp", axis=0, tiled=True),
        lax.all_gather(values_flat, "sp", axis=0, tiled=True),
    )
    span = math.gcd(fragments[0].shape[0], 1024)

    def inner_step(index, inner_state):
        key_rows = lax.dynamic_slice_in_dim(fragments[0], index * span, span, 0)
        value_rows = lax.dynamic_slice_in_dim(fragments[1], index * span, span, 0)
        return online_step(inner_state, key_rows, value_rows, index * span)

    final_state = lax.fori_loop(0, fragments[0].shape[0] // span, inner_step, start_state)
    summed_final = final_state[1]
    accum_final = final_state[2]
    heads_raw = (
        accum_final[0] / summed_final[0][..., None]
        - lambdas[:, None, None] * accum_final[1] / summed_final[1][..., None]
    )
    heads_raw = jnp.moveaxis(heads_raw, 0, 1)
    attn = (
        (
            heads_raw
            * lax.rsqrt(jnp.mean(heads_raw * heads_raw, -1, keepdims=True) + HEAD_EPS)
            * head_gain
            * HEAD_SCALE
        )
        .astype(jnp.bfloat16)
        .reshape(row_count, head_count * 2 * HEAD_DIM)
    )
    reach = 15
    rim_rows = from_behind(pool_in[row_count - reach :], "sp", 1)
    extended = jnp.concatenate([rim_rows, pool_in], 0).astype(jnp.float32)
    pair_sums = extended[1:] + extended[:-1]
    quad_sums = pair_sums[2:] + pair_sums[:-2]
    octet_sums = quad_sums[4:] + quad_sums[:-4]
    sixteen_sums = octet_sums[8:] + octet_sums[:-8]
    group_count = pool_in.shape[1] // GROUP_DIM
    stacked = jnp.stack(
        [
            pair_sums[14 : 14 + row_count],
            quad_sums[12 : 12 + row_count],
            octet_sums[8 : 8 + row_count],
            sixteen_sums,
        ],
        0,
    ).reshape(4, row_count, group_count, GROUP_DIM)
    levels = (tp_index * group_count + jnp.arange(group_count, dtype=jnp.int32)) % 4
    picked = jnp.sum(
        jnp.where(
            levels[None, None, :, None] == jnp.arange(4, dtype=jnp.int32)[:, None, None, None],
            stacked,
            0.0,
        ),
        0,
    )
    windows = 2 ** (1 + levels)
    counts = jnp.minimum(query_pos[:, None] + 1, windows[None, :]).astype(jnp.float32)
    window_mean = picked / counts[:, :, None]
    grouped = pool_in.reshape(row_count, group_count, GROUP_DIM).astype(jnp.float32)
    pool_mixed = (window_mean - grouped).astype(jnp.bfloat16)
    pooled = (
        (
            jnp.einsum("tgc,gce->tge", pool_mixed, pool_map, preferred_element_type=jnp.float32)
            * pool_scale.reshape(group_count, GROUP_DIM)
        )
        .astype(jnp.bfloat16)
        .reshape(row_count, group_count * GROUP_DIM)
    )
    branches = jnp.concatenate([pooled, attn], 1)
    partial_value = jnp.dot(
        branches,
        lax.all_gather(out_local, ("sp", "fs"), axis=1, tiled=True),
        preferred_element_type=jnp.float32,
    )
    layer_out = lax.psum_scatter(
        partial_value.astype(jnp.bfloat16), "tp", scatter_dimension=1, tiled=True
    )
    return layer_out[None]


MESH = pl.DeviceIdType.MESH
PIECES = 4
PARTS = 2

PROJECTED = ((0, 1, 2, 3), (1, 0, 2, 3), (2, 0, 3, 1), (3, 0, 2, 1))
LATE = ((2, 4), (0, 4), (2, 2), (2, 2))
FINISHED = (
    (2, 3, 4, 5, 6, 7, 0, 1),
    (4, 5, 0, 1, 6, 7, 2, 3),
    (0, 1, 6, 7, 2, 3, 4, 5),
    (0, 1, 2, 3, 4, 5, 6, 7),
)
EARLY = (4, 2, 2, 2)
SECOND = ((2, 3, 4, 5, 0, 1, 6, 7),) + 3 * ((0, 1, 2, 3, 4, 5, 6, 7),)
AHEAD = (2, 2, 2, 2)
ARRIVALS = ((0, 1, 2, 3), (1, 0, 3, 2), (2, 3, 0, 1), (3, 2, 1, 0))
SENDS = ((0, 1, 2, 3), (1, 3, 2, 0), (2, 0, 1, 3), (3, 2, 1, 0))
SLOTS = tuple(
    tuple(ARRIVALS[to].index(place) for to in SENDS[place]) for place in range(len(SENDS))
)


def pick(row, z):
    value = jnp.int32(row[0])
    for place in range(1, len(row)):
        value = jnp.where(z == place, row[place], value)
    return value


def fused_kernel(
    places,
    groups,
    tokens_ref,
    norm_gain_hbm,
    freqs_hbm,
    pool_ref,
    query_ref,
    key_ref,
    value_ref,
    map_ref,
    scale_hbm,
    gain_hbm,
    lambda_hbm,
    out_pool_ref,
    out_heads_ref,
    out_ref,
    own_tokens,
    own_map,
    norm_gain_ref,
    freqs_ref,
    scale_ref,
    gain_ref,
    lambda_ref,
    cos_ref,
    sin_ref,
    rows_all,
    weights,
    outs,
    queries,
    keys,
    values,
    pools,
    features,
    mine,
    to_mate,
    from_mate,
    kept,
    to_peer,
    from_peer,
    merging,
    final,
    *sems,
):
    (
        own_sem,
        small_sem,
        in_local,
        in_z_send,
        in_z_recv,
        in_n_send,
        in_n_recv,
        in_rest,
        out_local,
        out_z_send,
        out_z_recv,
        out_n_send,
        out_n_recv,
        out_rest,
        token_send,
        token_recv,
        mate_recv,
        half_send,
        half_recv,
        peer_send,
        peer_recv,
        merge_recv,
    ) = sems
    z = lax.axis_index("sp")
    f = lax.axis_index("fs")
    c = lax.axis_index("tp")
    fx = f + 1 - 2 * lax.rem(f, 2)
    fy = lax.rem(f + 2, groups)
    mate = 1 - c
    half_rows = tokens_ref.shape[0] // 2
    row_count = 2 * half_rows
    depth = pool_ref.shape[0]
    width = GROUP_DIM
    out_width = out_pool_ref.shape[1]
    half_out = out_ref.shape[1]
    length = places * row_count

    send_to = [pick([row[d] for row in SENDS], z) for d in range(places)]
    send_slot = [pick([row[d] for row in SLOTS], z) for d in range(places)]
    source = [pick([row[d] for row in ARRIVALS], z) for d in range(places)]

    def block(index, size):
        return pl.ds(pl.multiple_of(index * size, size), size)

    small = [
        pltpu.make_async_copy(source, target, small_sem.at[i])
        for i, (source, target) in enumerate(
            (
                (norm_gain_hbm, norm_gain_ref),
                (freqs_hbm, freqs_ref),
                (scale_hbm, scale_ref),
                (gain_hbm, gain_ref),
                (lambda_hbm, lambda_ref),
            )
        )
    ]
    barrier = pltpu.get_barrier_semaphore()
    partners = [{"sp": lax.rem(z + d, places)} for d in range(1, places)]
    partners += [{"fs": fx}, {"fs": fy}, {"tp": mate}]
    for partner in partners:
        pl.semaphore_signal(barrier, inc=1, device_id=partner, device_id_type=MESH)

    def remote(source, target, send, recv, device):
        return pltpu.make_async_remote_copy(
            src_ref=source,
            dst_ref=target,
            send_sem=send,
            recv_sem=recv,
            device_id=device,
            device_id_type=MESH,
        )

    class Gather:
        def __init__(self, sources, cut, view, sent, received, group):
            self.sources, self.cut, self.view = sources, cut, view
            self.sent, self.received = sent, received
            self.count = len(sources)
            (
                self.local,
                self.z_send,
                self.z_recv,
                self.n_send,
                self.n_recv,
                self.rest,
            ) = group
            self.low = (0, self.count // 2)
            self.high = (self.count // 2, self.count - self.count // 2)

        def own(self, m):
            return pltpu.make_async_copy(
                self.cut(self.sources[m], z), self.view(z, f, m, 1).at[0], self.local.at[m]
            )

        def across(self, d, m):
            to, slot = send_to[d], send_slot[d]
            return remote(
                self.cut(self.sources[m], to),
                self.view(z, f, m, 1).at[0],
                self.z_send.at[d],
                self.z_recv.at[slot],
                {"sp": to},
            )

        def arrive(self, d):
            view = self.view(source[d], f, 0, self.count)
            return remote(view, view, self.z_send.at[d], self.z_recv.at[d], {"sp": source[d]})

        def near(self, d, side, column, half):
            start, size = (self.low, self.high)[half]
            view = self.view(source[d], column, start, size)
            early = half == side
            return remote(
                view,
                view,
                self.n_send.at[side],
                self.n_recv.at[side, d] if early else self.rest.at[d // 2],
                {"fs": (fx, fy)[side]},
            )

        def forward(self, d, side, column):
            start, size = (self.high, self.low)[side]
            view = self.view(source[d], column, start, size)
            return remote(
                view, view, self.n_send.at[side], self.rest.at[d // 2], {"fs": (fx, fy)[side]}
            )

        def start_own(self):
            for m in range(self.count):
                self.own(m).start()

        def start(self, d):
            for m in range(self.count):
                self.across(d, m).start()

        def first(self, d):
            if d == 0:
                for m in range(self.count):
                    self.own(m).wait()
            else:
                self.arrive(d).wait_recv()
            for order in range(2):
                for side in range(2):
                    self.near(d, side, f, side ^ order).start()

        def second(self, d):
            self.near(d, 0, fx, 0).wait_recv()
            self.forward(d, 1, fx).start()
            self.near(d, 1, fy, 1).wait_recv()
            self.forward(d, 0, fy).start()

        def third(self, part):
            remote(
                self.received, self.received, self.n_send.at[0], self.rest.at[part], {"fs": fx}
            ).wait_recv()

        def drain(self):
            for d in range(1, places):
                self.arrive(d).wait_send()
            for side in range(2):
                remote(
                    self.sent, self.sent, self.n_send.at[side], self.rest.at[0], {"fs": fx}
                ).wait_send()

    filled = places * groups
    inward = Gather(
        (pool_ref, query_ref, key_ref, value_ref),
        lambda ref, to: ref.at[:, block(to, width)],
        lambda zz, ff, m, n: weights.at[pl.ds(m, n), block(zz * groups + ff, depth), :],
        weights.at[:, pl.ds(0, filled * 3 // 8 * depth), :],
        weights.at[:, pl.ds(0, filled // 4 * depth), :],
        (in_local, in_z_send, in_z_recv, in_n_send, in_n_recv, in_rest),
    )
    outward = Gather(
        (out_pool_ref, out_heads_ref),
        lambda ref, to: ref.at[block(to, width), :],
        lambda zz, ff, m, n: outs.at[pl.ds(m, n), :, block(zz * groups + ff, out_width)],
        outs.at[:, :, pl.ds(0, filled * 3 // 8 * out_width)],
        outs.at[:, :, pl.ds(0, filled // 4 * out_width)],
        (out_local, out_z_send, out_z_recv, out_n_send, out_n_recv, out_rest),
    )

    piece_rows = half_rows // PIECES

    def chunk(b, side, p):
        return rows_all.at[block((2 * b + side) * PIECES + p, piece_rows), :]

    def right(b, p, step=1):
        view = chunk(b, c, p)
        return remote(view, view, token_send.at[0], token_recv.at[b, p], {"sp": z + step})

    def left(b, p, step=-1):
        view = chunk(b, c, p)
        return remote(view, view, token_send.at[1], token_recv.at[b, p], {"sp": z + step})

    def share(b, side, p):
        view = chunk(b, side, p)
        return remote(view, view, token_send.at[2], mate_recv.at[b], {"tp": mate})

    def sent_tokens(kind, blocks):
        view = rows_all.at[pl.ds(0, blocks * half_rows), :]
        return remote(view, view, token_send.at[kind], mate_recv.at[0], {"tp": mate})

    def each_place(act):
        for place in range(places):
            pl.when(z == place)(lambda place=place: act(place))

    def send_right(place, pieces=range(PIECES)):
        for p in pieces:
            right(place, p).start()

    def send_left(place):
        for p in range(PIECES):
            left(place, p).start()

    def take(place, b, pieces=range(PIECES)):
        for p in pieces:
            if b < place:
                right(b, p, -1).wait_recv()
                if place < places - 1:
                    right(b, p).start()
            else:
                left(b, p, 1).wait_recv()
                if place > 0:
                    left(b, p).start()
            share(b, c, p).start()

    first_half, second_half = range(PIECES // 2), range(PIECES // 2, PIECES)

    def prepare(place):
        for d in range(1, places):
            inward.start(d)
        for d in range(1, 2 if place == 0 else places):
            outward.start(d)

    def begin(place):
        if place == 0:
            send_right(place)
        if place == places - 1:
            send_left(place)
        for p in range(PIECES):
            share(place, c, p).start()

    def gather(place):
        inward.second(0)
        outward.second(0)
        inward.first(1)
        inward.first(2)
        if place == 0:
            inward.second(1)
            inward.first(3)
            inward.second(2)
            inward.second(3)
            outward.first(1)
            outward.first(2)
            take(place, 1)
            outward.second(1)
            for d in range(2, places):
                outward.start(d)
        if place == 1:
            send_left(place)
            inward.second(1)
            outward.first(1)
            inward.second(2)
            take(place, 0, first_half)
            inward.first(3)
            take(place, 0, second_half)
            send_right(place)
            outward.first(3)
            outward.second(1)
            inward.second(3)
            outward.first(2)
            take(place, 2, first_half)
            outward.second(3)
            take(place, 2, second_half)
        if place == 2:
            send_right(place)
            send_left(place)
            inward.second(1)
            outward.first(1)
            inward.second(2)
            inward.first(3)
            outward.first(3)
            outward.second(1)
            take(place, 0, first_half)
            inward.second(3)
            take(place, 0, second_half)
            outward.second(3)
            take(place, 3)
        if place == 3:
            inward.second(1)
            inward.first(3)
            outward.first(1)
            inward.second(2)
            outward.first(2)
            inward.second(3)
            outward.second(1)
            take(place, 2)
            outward.second(2)
        inward.third(0)
        inward.third(1)

    def relay_piece(p):
        def act(place):
            if place in (1, 2):
                take(place, (None, 3, 1, None)[place], (p,))

        each_place(act)

    def more(place):
        if place == 0:
            outward.first(3)
        if place == 1:
            outward.second(2)
        if place == 2:
            outward.first(2)
        if place == 3:
            take(place, 0)

    def relay(place):
        if place in (0, 2):
            outward.second(2)
        if place == 3:
            outward.first(3)

    def finish_gather(place):
        if place in (1, 2):
            take(place, (None, 3, 1, None)[place], second_half[1:])
        if place == places - 1:
            outward.second(3)
        outward.third(1)

    tokens_in = pltpu.make_async_copy(
        tokens_ref.at[block(c, half_rows), :], own_tokens, own_sem.at[0]
    )
    map_in = pltpu.make_async_copy(map_ref.at[z], own_map, own_sem.at[1])
    tokens_in.start()
    for copy in small:
        copy.start()
    inward.start_own()
    outward.start_own()
    map_in.start()
    pl.semaphore_wait(barrier, len(partners))
    each_place(prepare)
    tokens_in.wait()
    for copy in small:
        copy.wait()
    floated = own_tokens[...].astype(jnp.float32)
    rows_all[block(2 * z + c, half_rows), :] = (
        floated
        * lax.rsqrt(jnp.mean(floated * floated, -1, keepdims=True) + NORM_EPS)
        * norm_gain_ref[...]
    ).astype(jnp.bfloat16)
    inward.first(0)
    outward.first(0)
    pools[0:16, :] = jnp.zeros((16, width), jnp.bfloat16)
    keys[...] = jnp.zeros_like(keys)
    values[...] = jnp.zeros_like(values)
    each_place(begin)

    def table(index, carry):
        rows = block(index, row_count)
        half = HEAD_DIM // 2
        count = (
            index * row_count + lax.broadcasted_iota(jnp.int32, (row_count, HEAD_DIM), 0)
        ).astype(jnp.float32)
        lane = lax.broadcasted_iota(jnp.int32, (row_count, HEAD_DIM), 1)
        angles = count * freqs_ref[...]
        cos_ref[rows, :] = jnp.cos(angles)
        sine = jnp.sin(angles)
        sin_ref[rows, :] = jnp.where(lane < half, -sine, sine)
        return carry

    lax.fori_loop(0, places, table, 0)

    def turned(raw, cosine, sine):
        floated = raw.astype(jnp.float32)
        return (floated * cosine + pltpu.roll(floated, HEAD_DIM // 2, 1) * sine).astype(
            jnp.bfloat16
        )

    projected = [pick([row[i] for row in PROJECTED], z) for i in range(places)]
    late = [pick([row[i] for row in LATE], z) for i in range(2)]
    finished = [pick([row[i] for row in FINISHED], z) for i in range(places * PARTS)]

    def project(index):
        theirs = rows_all.at[block(2 * index + mate, half_rows), :]
        remote(theirs, theirs, token_send.at[2], mate_recv.at[index], {"tp": mate}).wait_recv()
        rows = block(index, row_count)
        normed = rows_all[rows, :]
        cosine = cos_ref[rows, :]
        sine = sin_ref[rows, :]

        def product(m):
            return jnp.dot(normed, weights[m], preferred_element_type=jnp.float32).astype(
                jnp.bfloat16
            )

        pools[pl.ds(pl.multiple_of(index * row_count + 16, 16), row_count), :] = product(0)
        raw = product(1)
        for m in range(2):
            part = slice(m * HEAD_DIM, (m + 1) * HEAD_DIM)
            queries[rows, part] = turned(raw[:, part], cosine, sine)
        raw = product(2)
        for m in range(2):
            part = slice(m * HEAD_DIM, (m + 1) * HEAD_DIM)
            keys[rows, part] = turned(raw[:, part], cosine, sine)
        values[rows, :] = product(3)

    upper = z >= places // 2

    each_place(gather)
    project(projected[0])
    each_place(more)
    relay_piece(0)
    project(projected[1])
    each_place(relay)
    relay_piece(1)

    map_in.wait()
    outward.third(0)

    level = lax.rem(c * map_ref.shape[0] + z, 4)
    window = jnp.where(
        level == 0, 2, jnp.where(level == 1, 4, jnp.where(level == 2, 8, 16))
    )
    head_lambda = lambda_ref[c * map_ref.shape[0] + z]

    part_rows = row_count // PARTS

    def to_sibling(step):
        return remote(
            to_mate.at[step],
            from_mate.at[step],
            half_send.at[0],
            half_recv.at[step],
            {"tp": mate},
        )

    outer = (z == 0) | (z == places - 1)
    pair = z + 1 - 2 * lax.rem(z, 2)

    def crossing(to, h):
        return lax.rem(to, 2) * PARTS + h

    def to_inner(to, h):
        return remote(
            to_peer.at[to * PARTS + h],
            merging.at[crossing(to, h)],
            peer_send.at[0],
            merge_recv.at[crossing(to, h)],
            {"sp": pair},
        )

    def to_place(to, h):
        return remote(
            to_peer.at[to * PARTS + h],
            from_peer.at[h],
            peer_send.at[0],
            peer_recv.at[h],
            {"sp": to},
        )

    def to_pair(h):
        return remote(
            to_peer.at[pair * PARTS + h],
            from_peer.at[PARTS + h],
            peer_send.at[0],
            peer_recv.at[PARTS + h],
            {"sp": pair},
        )

    def step_place(step):
        slot = finished[0]
        for i in range(1, places * PARTS):
            slot = jnp.where(step == i, finished[i], slot)
        return slot // PARTS, lax.rem(slot, PARTS)

    def attend(step, slot, span):
        rows = block(slot, part_rows)
        query_pos = slot * part_rows + lax.broadcasted_iota(jnp.int32, (part_rows, span), 0)
        key_pos = lax.broadcasted_iota(jnp.int32, (part_rows, span), 1)
        seen = query_pos >= key_pos
        mapped = []
        for m in range(2):
            part = slice(m * HEAD_DIM, (m + 1) * HEAD_DIM)
            scores = lax.dot_general(
                queries[rows, part],
                keys[:span, part],
                (((1,), (1,)), ((), ())),
                preferred_element_type=jnp.float32,
            ) * HEAD_DIM ** (-0.5)
            scores = jnp.where(seen, scores, -jnp.inf)
            expons = jnp.exp(scores - jnp.max(scores, -1, keepdims=True))
            totals = jnp.sum(expons, -1, keepdims=True)
            mapped.append(
                jnp.dot(
                    expons.astype(jnp.bfloat16), values[:span, :], preferred_element_type=jnp.float32
                )
                / totals
            )
        raw = mapped[0] - head_lambda * mapped[1]
        attn = (
            raw
            * lax.rsqrt(jnp.mean(raw * raw, -1, keepdims=True) + HEAD_EPS)
            * gain_ref[...]
            * HEAD_SCALE
        ).astype(jnp.bfloat16)
        extended = pools[
            pl.ds(pl.multiple_of(slot * part_rows, 16), part_rows + 16), :
        ].astype(jnp.float32)
        picked = extended + pltpu.roll(extended, 1, 0)
        sums = picked
        for shift in (2, 4, 8):
            sums = sums + pltpu.roll(sums, shift, 0)
            picked = lax.select_n(window >= 2 * shift, picked, sums)
        places_of = slot * part_rows + lax.broadcasted_iota(jnp.int32, (part_rows, 1), 0)
        counts = jnp.minimum(places_of + 1, window).astype(jnp.float32)
        mixed = (picked[16:] / counts - extended[16:]).astype(jnp.bfloat16)
        pooled = (
            jnp.dot(mixed, own_map[...], preferred_element_type=jnp.float32) * scale_ref[z]
        ).astype(jnp.bfloat16)

        features[step] = jnp.concatenate([pooled, attn], 1)

    def compute(step):
        to, h = step_place(step)
        slot = to * PARTS + h
        half = places // 2
        pl.when(to < half)(lambda: attend(step, slot, half * row_count))
        pl.when(to >= half)(lambda: attend(step, slot, length))
        return features[step, :, :width], features[step, :, width:]

    def partial_of(step, turn, pooled, attn, side):
        columns = block(side, half_out)
        value = jnp.dot(
            pooled, outs[0, :, columns], preferred_element_type=jnp.float32
        ) + jnp.dot(attn, outs[1, :, columns], preferred_element_type=jnp.float32)

        @pl.when(side == c)
        def _():
            mine[lax.rem(turn, 2)] = value

        @pl.when(side != c)
        def _():
            to_mate[step] = value.astype(jnp.bfloat16)
            to_sibling(step).start()

    def finish(step, turn):
        to, h = step_place(step)
        slot = to * PARTS + h
        crosses = to // 2 != z // 2
        to_sibling(step).wait_recv()
        summed = mine[lax.rem(turn, 2)] + from_mate[step].astype(jnp.float32)

        @pl.when(to == z)
        def _():
            final[h] = summed

        @pl.when(to == pair)
        def _():
            to_peer[slot] = summed.astype(jnp.bfloat16)
            to_pair(h).start()

        @pl.when(crosses & outer)
        def _():
            to_peer[slot] = summed.astype(jnp.bfloat16)
            to_inner(to, h).start()

        @pl.when(crosses & jnp.logical_not(outer))
        def _():
            kept[crossing(to, h)] = summed

    def merge(turn):
        place = turn // PARTS
        to = jnp.where(upper, place, places // 2 + place)
        h = lax.rem(turn, PARTS)
        to_inner(to, h).wait_recv()
        to_peer[to * PARTS + h] = (
            kept[crossing(to, h)] + merging[crossing(to, h)].astype(jnp.float32)
        ).astype(jnp.bfloat16)
        to_place(to, h).start()

    side = z // (places // 2)
    eager = side == c
    early = pick(EARLY, z)
    merged = jnp.where(upper, jnp.where(eager, 2, 3), jnp.where(eager, 3, 5))
    lag = jnp.where(outer, 0, 1)

    def grow(step):
        @pl.when((step == late[0]) | (step == late[1]))
        def _():
            @pl.when((z == 0) & (step == late[0]))
            def _():
                outward.second(3)
                take(0, 2)

            @pl.when((z == 0) & (step == late[1]))
            def _():
                take(0, 3)

            def project_late(i, carry):
                @pl.when((z == places - 1) & (i == 3))
                def _():
                    take(places - 1, 1)

                project(jnp.where(i == 2, projected[2], projected[3]))
                return carry

            lax.fori_loop(
                jnp.where(step == late[0], 2, 3), jnp.where(step == late[1], 4, 3), project_late, 0
            )

    ahead = pick(AHEAD, z)
    last = places * PARTS - 1
    seconds = [pick([row[i] for row in SECOND], z) for i in range(places * PARTS)]

    def second_step(turn):
        step = seconds[0]
        for i in range(1, places * PARTS):
            step = jnp.where(turn == i, seconds[i], step)
        return step

    def first_side(step, carry):
        grow(step)

        @pl.when(step == 1)
        def _():
            relay_piece(2)

        partial_of(step, step, *compute(step), side)

        @pl.when(eager & (step >= lag))
        def _():
            finish(step - lag, step - lag)

        return carry

    def second_side(turn):
        step = second_step(turn)
        pooled, attn = features[step, :, :width], features[step, :, width:]
        partial_of(step, turn, pooled, attn, 1 - side)

    def other_side(turn, carry):
        second_side(turn)

        @pl.when(jnp.logical_not(eager) & (turn > 0))
        def _():
            finish(second_step(turn - 1), turn - 1)

        return carry

    def both_sides(step, carry):
        grow(step)
        partial_of(step, step, *compute(step), side)
        at_once = eager & outer & (step == early)

        @pl.when(at_once)
        def _():
            finish(step, step)

        second_side(step - early + ahead)

        @pl.when((step != early + 1 - lag) & jnp.logical_not(at_once))
        def _():
            first = jnp.where(step == early, step, step - 1)
            turn = first - early + ahead
            finish(jnp.where(eager, first, second_step(turn)), jnp.where(eager, first, turn))

        again = upper & (step == last)

        @pl.when(jnp.logical_not(outer) & ((step == merged) | (step == merged + 1) | again))
        def _():
            merge(jnp.where(again, PARTS, step - merged))

        return carry

    lax.fori_loop(0, early, first_side, 0)
    each_place(finish_gather)

    @pl.when(eager & jnp.logical_not(outer))
    def _():
        finish(early - 1, early - 1)

    lax.fori_loop(0, ahead, other_side, 0)

    @pl.when(jnp.logical_not(eager))
    def _():
        finish(second_step(ahead - 1), ahead - 1)

    def merge_more(turn, carry):
        merge(turn)
        return carry

    lax.fori_loop(early, places * PARTS, both_sides, 0)
    def second_more(turn, carry):
        second_side(turn)

        @pl.when(jnp.logical_not(eager))
        def _():
            finish(second_step(turn - 1), turn - 1)

        return carry

    lax.fori_loop(last + 1 - early + ahead, last + 1, second_more, 0)
    finish(jnp.where(eager, last, second_step(last)), last)

    @pl.when(jnp.logical_not(outer))
    def _():
        lax.fori_loop(jnp.where(upper, PARTS + 1, PARTS), 2 * PARTS, merge_more, 0)

    for h in range(PARTS):
        to_pair(h).wait_recv()
        total = final[h] + from_peer[PARTS + h].astype(jnp.float32)
        to_place(z, h).wait_recv()
        out_ref[h * part_rows : (h + 1) * part_rows, :] = (
            total + from_peer[h].astype(jnp.float32)
        ).astype(out_ref.dtype)

    inward.drain()
    outward.drain()

    def drain(place):
        if place < places - 1:
            sent_tokens(0, place + 1).wait_send()
        if place > 0:
            sent_tokens(1, places - place).wait_send()

    each_place(drain)
    sent_tokens(2, places).wait_send()
    remote(to_mate, from_mate, half_send.at[0], half_recv.at[0], {"tp": mate}).wait_send()
    sent = to_peer.at[pl.ds(0, (places - 1) * PARTS)]
    remote(sent, sent, peer_send.at[0], peer_recv.at[0], {"sp": pair}).wait_send()


def fused(
    tokens,
    norm_gain,
    pool_input,
    query_weight,
    key_weight,
    value_weight,
    pool_map,
    pool_scale,
    head_gain,
    diff_lambda,
    out_pool,
    out_heads,
):
    places = lax.axis_size("sp")
    groups = lax.axis_size("fs")
    row_count, model = tokens.shape[1], tokens.shape[2]
    length = places * row_count
    half = HEAD_DIM // 2
    freqs = np.float32(1.0) / np.float32(THETA) ** (
        np.arange(half, dtype=np.float32) * np.float32(2.0) / np.float32(HEAD_DIM)
    )
    freqs = jnp.asarray(np.concatenate([freqs, freqs])[None, :], jnp.float32)
    group_count = pool_map.shape[0]
    half_out = model // 2
    vmem = pl.BlockSpec(memory_space=pltpu.VMEM)
    hbm = pl.BlockSpec(memory_space=pl.ANY)
    dma = pltpu.SemaphoreType.DMA
    low = jnp.bfloat16

    def gather_sems(count):
        return [
            dma((count,)),
            dma((places,)),
            dma((places,)),
            dma((2,)),
            dma((2, places)),
            dma((2,)),
        ]

    out = pl.pallas_call(
        lambda *refs: fused_kernel(places, groups, *refs),
        out_shape=jax.ShapeDtypeStruct((row_count, half_out), low),
        in_specs=[hbm] * 13,
        out_specs=vmem,
        scratch_shapes=[
            pltpu.VMEM((row_count // 2, model), low),
            pltpu.VMEM((GROUP_DIM, GROUP_DIM), low),
            pltpu.VMEM((1, model), jnp.float32),
            pltpu.VMEM((1, HEAD_DIM), jnp.float32),
            pltpu.VMEM((group_count, 1, GROUP_DIM), jnp.float32),
            pltpu.VMEM((1, 2 * HEAD_DIM), jnp.float32),
            pltpu.SMEM(diff_lambda.shape, jnp.float32),
            pltpu.VMEM((length, HEAD_DIM), jnp.float32),
            pltpu.VMEM((length, HEAD_DIM), jnp.float32),
            pltpu.VMEM((length, model), low),
            pltpu.VMEM((4, model, GROUP_DIM), low),
            pltpu.VMEM((2, GROUP_DIM, model), low),
            pltpu.VMEM((length, GROUP_DIM), low),
            pltpu.VMEM((length, GROUP_DIM), low),
            pltpu.VMEM((length, GROUP_DIM), low),
            pltpu.VMEM((length + 16, GROUP_DIM), low),
            pltpu.VMEM((places * PARTS, row_count // PARTS, 2 * GROUP_DIM), low),
            pltpu.VMEM((2, row_count // PARTS, half_out), jnp.float32),
            pltpu.VMEM((places * PARTS, row_count // PARTS, half_out), low),
            pltpu.VMEM((places * PARTS, row_count // PARTS, half_out), low),
            pltpu.VMEM((2 * PARTS, row_count // PARTS, half_out), jnp.float32),
            pltpu.VMEM((places * PARTS, row_count // PARTS, half_out), low),
            pltpu.VMEM((2 * PARTS, row_count // PARTS, half_out), low),
            pltpu.VMEM((2 * PARTS, row_count // PARTS, half_out), low),
            pltpu.VMEM((PARTS, row_count // PARTS, half_out), jnp.float32),
            dma((2,)),
            dma((5,)),
            *gather_sems(4),
            *gather_sems(2),
            dma((3,)),
            dma((places, PIECES)),
            dma((places,)),
            dma((1,)),
            dma((places * PARTS,)),
            dma((1,)),
            dma((2 * PARTS,)),
            dma((2 * PARTS,)),
        ],
        compiler_params=pltpu.CompilerParams(
            collective_id=0, has_side_effects=True, vmem_limit_bytes=56 * 1024 * 1024
        ),
    )(
        tokens[0],
        norm_gain.reshape(1, model),
        freqs,
        pool_input,
        query_weight,
        key_weight,
        value_weight,
        pool_map,
        pool_scale.reshape(group_count, 1, GROUP_DIM),
        head_gain.reshape(1, 2 * HEAD_DIM),
        diff_lambda,
        out_pool,
        out_heads,
    )
    return out[None]


def solution(mesh):
    placed = (
        P("fs", "sp", None),
        P(),
        P(("sp", "fs"), "tp"),
        P(("sp", "fs"), "tp"),
        P(("sp", "fs"), "tp"),
        P(("sp", "fs"), "tp"),
        P("tp", None, None),
        P("tp"),
        P(),
        P(),
        P("tp", ("sp", "fs")),
        P("tp", ("sp", "fs")),
    )
    shape = dict(mesh.shape)

    def body(tokens, *rest):
        head_count = rest[3].shape[1] // (2 * HEAD_DIM)
        group_count = rest[5].shape[0]
        fits = (
            shape["fs"] == 4
            and shape["tp"] == 2
            and shape["sp"] == head_count == group_count == 4
            and tokens.shape[0] == 1
        )
        return (fused if fits else local)(tokens, *rest)

    return jax.shard_map(
        body, mesh=mesh, in_specs=placed, out_specs=P("fs", "sp", "tp"), check_vma=False
    )
```

```python
import math

import jax
import jax.numpy as jnp
import numpy as np
from jax import lax
from jax.experimental import pallas as pl
from jax.experimental.pallas import tpu as pltpu
from jax.sharding import PartitionSpec as P

HEAD_DIM = 128
GROUP_DIM = 256


THETA = 500000.0
HEAD_SCALE = 0.8
NORM_EPS = 1e-06
HEAD_EPS = 1e-05


def from_behind(value, axis, steps):
    count = lax.axis_size(axis)
    first, last = (max(0, -steps), min(count, count - steps))
    return lax.ppermute(value, axis, [(source, source + steps) for source in range(first, last)])


def rotate(tensor, positions):
    half = HEAD_DIM // 2
    freqs = 1.0 / THETA ** (jnp.arange(half, dtype=jnp.float32) * 2.0 / HEAD_DIM)
    angles = positions[:, None] * freqs[None, :]
    cosine = jnp.cos(angles)[:, None, None, :]
    sine = jnp.sin(angles)[:, None, None, :]
    floated = tensor.astype(jnp.float32)
    first = floated[..., :half]
    second = floated[..., half:]
    turned = jnp.concatenate([first * cosine - second * sine, second * cosine + first * sine], -1)
    return turned.astype(jnp.bfloat16)


def local(
    tokens,
    norm_gain,
    pool_input,
    query_weight,
    key_weight,
    value_weight,
    pool_map,
    pool_scale,
    head_gain,
    diff_lambda,
    out_pool,
    out_heads,
):
    out_local = jnp.concatenate([out_pool, out_heads], 0)
    row_count = tokens.shape[1]
    floated = tokens[0].astype(jnp.float32)
    normed = (
        floated * lax.rsqrt(jnp.mean(floated * floated, -1, keepdims=True) + NORM_EPS) * norm_gain
    ).astype(jnp.bfloat16)
    fragments = (
        lax.all_gather(pool_input, ("sp", "fs"), axis=0, tiled=True),
        lax.all_gather(query_weight, ("sp", "fs"), axis=0, tiled=True),
        lax.all_gather(key_weight, ("sp", "fs"), axis=0, tiled=True),
        lax.all_gather(value_weight, ("sp", "fs"), axis=0, tiled=True),
    )
    projected = tuple(
        (jnp.dot(normed, fragment, preferred_element_type=jnp.float32) for fragment in fragments)
    )
    pool_in, queries, keys_flat, values_flat = [
        product.astype(jnp.bfloat16) for product in projected
    ]
    head_count = values_flat.shape[1] // (2 * HEAD_DIM)
    tp_index = lax.axis_index("tp")
    sp_index = lax.axis_index("sp")
    query_pos = sp_index * row_count + jnp.arange(row_count, dtype=jnp.int32)
    positions = query_pos.astype(jnp.float32)
    queries = rotate(queries.reshape(row_count, head_count, 2, HEAD_DIM), positions)
    keys_flat = rotate(keys_flat.reshape(row_count, head_count, 2, HEAD_DIM), positions).reshape(
        row_count, head_count * 2 * HEAD_DIM
    )
    lambdas = lax.dynamic_slice_in_dim(diff_lambda, tp_index * head_count, head_count, 0)

    def online_step(state, key_rows, value_rows, key_offset):
        largest, summed, accum = state
        width = key_rows.shape[0]
        shaped = key_rows.reshape(width, head_count, 2, HEAD_DIM)
        scores = jnp.einsum(
            "qhcd,khcd->chqk", queries, shaped, preferred_element_type=jnp.float32
        ) * HEAD_DIM ** (-0.5)
        key_pos = key_offset + jnp.arange(width, dtype=jnp.int32)
        scores = jnp.where(query_pos[:, None] >= key_pos[None, :], scores, -jnp.inf)
        newest = jnp.maximum(largest, jnp.max(scores, -1))
        anchor = jnp.where(jnp.isfinite(newest), newest, 0.0)
        rescale = jnp.exp(largest - anchor)
        expons = jnp.exp(scores - anchor[..., None])
        summed = summed * rescale + jnp.sum(expons, -1)
        value_shaped = value_rows.reshape(width, head_count, 2 * HEAD_DIM)
        added = jnp.einsum(
            "chqk,khe->chqe",
            expons.astype(jnp.bfloat16),
            value_shaped,
            preferred_element_type=jnp.float32,
        )
        accum = accum * rescale[..., None] + added
        return (newest, summed, accum)

    start_state = (
        jnp.full((2, head_count, row_count), -jnp.inf, jnp.float32),
        jnp.zeros((2, head_count, row_count), jnp.float32),
        jnp.zeros((2, head_count, row_count, 2 * HEAD_DIM), jnp.float32),
    )
    fragments = (
        lax.all_gather(keys_flat, "sp", axis=0, tiled=True),
        lax.all_gather(values_flat, "sp", axis=0, tiled=True),
    )
    span = math.gcd(fragments[0].shape[0], 1024)

    def inner_step(index, inner_state):
        key_rows = lax.dynamic_slice_in_dim(fragments[0], index * span, span, 0)
        value_rows = lax.dynamic_slice_in_dim(fragments[1], index * span, span, 0)
        return online_step(inner_state, key_rows, value_rows, index * span)

    final_state = lax.fori_loop(0, fragments[0].shape[0] // span, inner_step, start_state)
    summed_final = final_state[1]
    accum_final = final_state[2]
    heads_raw = (
        accum_final[0] / summed_final[0][..., None]
        - lambdas[:, None, None] * accum_final[1] / summed_final[1][..., None]
    )
    heads_raw = jnp.moveaxis(heads_raw, 0, 1)
    attn = (
        (
            heads_raw
            * lax.rsqrt(jnp.mean(heads_raw * heads_raw, -1, keepdims=True) + HEAD_EPS)
            * head_gain
            * HEAD_SCALE
        )
        .astype(jnp.bfloat16)
        .reshape(row_count, head_count * 2 * HEAD_DIM)
    )
    reach = 15
    rim_rows = from_behind(pool_in[row_count - reach :], "sp", 1)
    extended = jnp.concatenate([rim_rows, pool_in], 0).astype(jnp.float32)
    pair_sums = extended[1:] + extended[:-1]
    quad_sums = pair_sums[2:] + pair_sums[:-2]
    octet_sums = quad_sums[4:] + quad_sums[:-4]
    sixteen_sums = octet_sums[8:] + octet_sums[:-8]
    group_count = pool_in.shape[1] // GROUP_DIM
    stacked = jnp.stack(
        [
            pair_sums[14 : 14 + row_count],
            quad_sums[12 : 12 + row_count],
            octet_sums[8 : 8 + row_count],
            sixteen_sums,
        ],
        0,
    ).reshape(4, row_count, group_count, GROUP_DIM)
    levels = (tp_index * group_count + jnp.arange(group_count, dtype=jnp.int32)) % 4
    picked = jnp.sum(
        jnp.where(
            levels[None, None, :, None] == jnp.arange(4, dtype=jnp.int32)[:, None, None, None],
            stacked,
            0.0,
        ),
        0,
    )
    windows = 2 ** (1 + levels)
    counts = jnp.minimum(query_pos[:, None] + 1, windows[None, :]).astype(jnp.float32)
    window_mean = picked / counts[:, :, None]
    grouped = pool_in.reshape(row_count, group_count, GROUP_DIM).astype(jnp.float32)
    pool_mixed = (window_mean - grouped).astype(jnp.bfloat16)
    pooled = (
        (
            jnp.einsum("tgc,gce->tge", pool_mixed, pool_map, preferred_element_type=jnp.float32)
            * pool_scale.reshape(group_count, GROUP_DIM)
        )
        .astype(jnp.bfloat16)
        .reshape(row_count, group_count * GROUP_DIM)
    )
    branches = jnp.concatenate([pooled, attn], 1)
    partial_value = jnp.dot(
        branches,
        lax.all_gather(out_local, ("sp", "fs"), axis=1, tiled=True),
        preferred_element_type=jnp.float32,
    )
    layer_out = lax.psum_scatter(
        partial_value.astype(jnp.bfloat16), "tp", scatter_dimension=1, tiled=True
    )
    return layer_out[None]


MESH = pl.DeviceIdType.MESH
PIECES = 8
PARTS = 2

PROJECTED = ((0, 1, 2, 3), (1, 0, 2, 3), (2, 0, 3, 1), (3, 0, 2, 1))
LATE = ((2, 4), (0, 4), (2, 2), (2, 2))
FINISHED = (
    (2, 3, 4, 5, 6, 7, 0, 1),
    (4, 5, 0, 1, 6, 7, 2, 3),
    (0, 1, 6, 7, 2, 3, 4, 5),
    (0, 1, 2, 3, 4, 5, 6, 7),
)
EARLY = (4, 2, 2, 2)
SECOND = ((2, 3, 4, 5, 0, 1, 6, 7),) + 3 * ((0, 1, 2, 3, 4, 5, 6, 7),)
AHEAD = (2, 2, 2, 2)
ARRIVALS = ((0, 1, 2, 3), (1, 0, 3, 2), (2, 3, 0, 1), (3, 2, 1, 0))
SENDS = ((0, 1, 2, 3), (1, 3, 2, 0), (2, 0, 1, 3), (3, 2, 1, 0))
SLOTS = tuple(
    tuple(ARRIVALS[to].index(place) for to in SENDS[place]) for place in range(len(SENDS))
)


def pick(row, z):
    value = jnp.int32(row[0])
    for place in range(1, len(row)):
        value = jnp.where(z == place, row[place], value)
    return value


def fused_kernel(
    places,
    groups,
    tokens_ref,
    norm_gain_hbm,
    freqs_hbm,
    pool_ref,
    query_ref,
    key_ref,
    value_ref,
    map_ref,
    scale_hbm,
    gain_hbm,
    lambda_hbm,
    out_pool_ref,
    out_heads_ref,
    out_ref,
    own_tokens,
    own_map,
    norm_gain_ref,
    freqs_ref,
    scale_ref,
    gain_ref,
    lambda_ref,
    cos_ref,
    sin_ref,
    rows_all,
    weights,
    outs,
    queries,
    keys,
    values,
    pools,
    features,
    mine,
    to_mate,
    from_mate,
    kept,
    to_peer,
    from_peer,
    merging,
    final,
    *sems,
):
    (
        own_sem,
        small_sem,
        in_local,
        in_z_send,
        in_z_recv,
        in_n_send,
        in_n_recv,
        in_rest,
        out_local,
        out_z_send,
        out_z_recv,
        out_n_send,
        out_n_recv,
        out_rest,
        token_send,
        token_recv,
        mate_recv,
        half_send,
        half_recv,
        peer_send,
        peer_recv,
        merge_recv,
    ) = sems
    z = lax.axis_index("sp")
    f = lax.axis_index("fs")
    c = lax.axis_index("tp")
    fx = f + 1 - 2 * lax.rem(f, 2)
    fy = lax.rem(f + 2, groups)
    mate = 1 - c
    half_rows = tokens_ref.shape[0] // 2
    row_count = 2 * half_rows
    depth = pool_ref.shape[0]
    width = GROUP_DIM
    out_width = out_pool_ref.shape[1]
    half_out = out_ref.shape[1]
    length = places * row_count

    send_to = [pick([row[d] for row in SENDS], z) for d in range(places)]
    send_slot = [pick([row[d] for row in SLOTS], z) for d in range(places)]
    source = [pick([row[d] for row in ARRIVALS], z) for d in range(places)]

    def block(index, size):
        return pl.ds(pl.multiple_of(index * size, size), size)

    small = [
        pltpu.make_async_copy(source, target, small_sem.at[i])
        for i, (source, target) in enumerate(
            (
                (norm_gain_hbm, norm_gain_ref),
                (freqs_hbm, freqs_ref),
                (scale_hbm, scale_ref),
                (gain_hbm, gain_ref),
                (lambda_hbm, lambda_ref),
            )
        )
    ]
    barrier = pltpu.get_barrier_semaphore()
    partners = [{"sp": lax.rem(z + d, places)} for d in range(1, places)]
    partners += [{"fs": fx}, {"fs": fy}, {"tp": mate}]
    for partner in partners:
        pl.semaphore_signal(barrier, inc=1, device_id=partner, device_id_type=MESH)

    def remote(source, target, send, recv, device):
        return pltpu.make_async_remote_copy(
            src_ref=source,
            dst_ref=target,
            send_sem=send,
            recv_sem=recv,
            device_id=device,
            device_id_type=MESH,
        )

    class Gather:
        def __init__(self, sources, cut, view, sent, received, group):
            self.sources, self.cut, self.view = sources, cut, view
            self.sent, self.received = sent, received
            self.count = len(sources)
            (
                self.local,
                self.z_send,
                self.z_recv,
                self.n_send,
                self.n_recv,
                self.rest,
            ) = group
            self.low = (0, self.count // 2)
            self.high = (self.count // 2, self.count - self.count // 2)

        def own(self, m):
            return pltpu.make_async_copy(
                self.cut(self.sources[m], z), self.view(z, f, m, 1).at[0], self.local.at[m]
            )

        def across(self, d, m):
            to, slot = send_to[d], send_slot[d]
            return remote(
                self.cut(self.sources[m], to),
                self.view(z, f, m, 1).at[0],
                self.z_send.at[d],
                self.z_recv.at[slot],
                {"sp": to},
            )

        def arrive(self, d):
            view = self.view(source[d], f, 0, self.count)
            return remote(view, view, self.z_send.at[d], self.z_recv.at[d], {"sp": source[d]})

        def near(self, d, side, column, half):
            start, size = (self.low, self.high)[half]
            view = self.view(source[d], column, start, size)
            early = half == side
            return remote(
                view,
                view,
                self.n_send.at[side],
                self.n_recv.at[side, d] if early else self.rest.at[d // 2],
                {"fs": (fx, fy)[side]},
            )

        def forward(self, d, side, column):
            start, size = (self.high, self.low)[side]
            view = self.view(source[d], column, start, size)
            return remote(
                view, view, self.n_send.at[side], self.rest.at[d // 2], {"fs": (fx, fy)[side]}
            )

        def start_own(self):
            for m in range(self.count):
                self.own(m).start()

        def start(self, d):
            for m in range(self.count):
                self.across(d, m).start()

        def first(self, d):
            if d == 0:
                for m in range(self.count):
                    self.own(m).wait()
            else:
                self.arrive(d).wait_recv()
            for order in range(2):
                for side in range(2):
                    self.near(d, side, f, side ^ order).start()

        def second(self, d):
            self.near(d, 0, fx, 0).wait_recv()
            self.forward(d, 1, fx).start()
            self.near(d, 1, fy, 1).wait_recv()
            self.forward(d, 0, fy).start()

        def third(self, part):
            remote(
                self.received, self.received, self.n_send.at[0], self.rest.at[part], {"fs": fx}
            ).wait_recv()

        def drain(self):
            for d in range(1, places):
                self.arrive(d).wait_send()
            for side in range(2):
                remote(
                    self.sent, self.sent, self.n_send.at[side], self.rest.at[0], {"fs": fx}
                ).wait_send()

    filled = places * groups
    inward = Gather(
        (pool_ref, query_ref, key_ref, value_ref),
        lambda ref, to: ref.at[:, block(to, width)],
        lambda zz, ff, m, n: weights.at[pl.ds(m, n), block(zz * groups + ff, depth), :],
        weights.at[:, pl.ds(0, filled * 3 // 8 * depth), :],
        weights.at[:, pl.ds(0, filled // 4 * depth), :],
        (in_local, in_z_send, in_z_recv, in_n_send, in_n_recv, in_rest),
    )
    outward = Gather(
        (out_pool_ref, out_heads_ref),
        lambda ref, to: ref.at[block(to, width), :],
        lambda zz, ff, m, n: outs.at[pl.ds(m, n), :, block(zz * groups + ff, out_width)],
        outs.at[:, :, pl.ds(0, filled * 3 // 8 * out_width)],
        outs.at[:, :, pl.ds(0, filled // 4 * out_width)],
        (out_local, out_z_send, out_z_recv, out_n_send, out_n_recv, out_rest),
    )

    piece_rows = half_rows // PIECES

    def chunk(b, side, p):
        return rows_all.at[block((2 * b + side) * PIECES + p, piece_rows), :]

    def right(b, p, step=1):
        view = chunk(b, c, p)
        return remote(view, view, token_send.at[0], token_recv.at[b, p], {"sp": z + step})

    def left(b, p, step=-1):
        view = chunk(b, c, p)
        return remote(view, view, token_send.at[1], token_recv.at[b, p], {"sp": z + step})

    def share(b, side, p):
        view = chunk(b, side, p)
        return remote(view, view, token_send.at[2], mate_recv.at[b], {"tp": mate})

    def sent_tokens(kind, blocks):
        view = rows_all.at[pl.ds(0, blocks * half_rows), :]
        return remote(view, view, token_send.at[kind], mate_recv.at[0], {"tp": mate})

    def each_place(act):
        for place in range(places):
            pl.when(z == place)(lambda place=place: act(place))

    def send_right(place, pieces=range(PIECES)):
        for p in pieces:
            right(place, p).start()

    def send_left(place):
        for p in range(PIECES):
            left(place, p).start()

    def take(place, b, pieces=range(PIECES)):
        for p in pieces:
            if b < place:
                right(b, p, -1).wait_recv()
                if place < places - 1:
                    right(b, p).start()
            else:
                left(b, p, 1).wait_recv()
                if place > 0:
                    left(b, p).start()
            share(b, c, p).start()

    first_half, second_half = range(PIECES // 2), range(PIECES // 2, PIECES)

    def prepare(place):
        for d in range(1, places):
            inward.start(d)
        for d in range(1, 2 if place == 0 else places):
            outward.start(d)

    def begin(place):
        if place == 0:
            send_right(place)
        if place == places - 1:
            send_left(place)
        for p in range(PIECES):
            share(place, c, p).start()

    def gather(place):
        inward.second(0)
        outward.second(0)
        inward.first(1)
        inward.first(2)
        if place == 0:
            inward.second(1)
            inward.first(3)
            inward.second(2)
            inward.second(3)
            outward.first(1)
            outward.first(2)
            take(place, 1)
            outward.second(1)
            for d in range(2, places):
                outward.start(d)
        if place == 1:
            send_left(place)
            inward.second(1)
            outward.first(1)
            inward.second(2)
            take(place, 0, first_half)
            inward.first(3)
            take(place, 0, second_half)
            send_right(place)
            outward.first(3)
            outward.second(1)
            inward.second(3)
            outward.first(2)
            take(place, 2, first_half)
            outward.second(3)
            take(place, 2, second_half)
        if place == 2:
            send_right(place)
            send_left(place)
            inward.second(1)
            outward.first(1)
            inward.second(2)
            inward.first(3)
            outward.first(3)
            outward.second(1)
            take(place, 0, first_half)
            inward.second(3)
            take(place, 0, second_half)
            outward.second(3)
            take(place, 3)
        if place == 3:
            inward.second(1)
            inward.first(3)
            outward.first(1)
            inward.second(2)
            outward.first(2)
            inward.second(3)
            outward.second(1)
            take(place, 2)
            outward.second(2)
        inward.third(0)
        inward.third(1)

    def relay_piece(p):
        def act(place):
            if place in (1, 2):
                take(place, (None, 3, 1, None)[place], range(p * PIECES // 4, (p + 1) * PIECES // 4))

        each_place(act)

    def more(place):
        if place == 0:
            outward.first(3)
        if place == 1:
            outward.second(2)
        if place == 2:
            outward.first(2)
        if place == 3:
            take(place, 0)

    def relay(place):
        if place in (0, 2):
            outward.second(2)
        if place == 3:
            outward.first(3)

    def finish_gather(place):
        if place in (1, 2):
            take(place, (None, 3, 1, None)[place], range(3 * PIECES // 4, PIECES))
        if place == places - 1:
            outward.second(3)
        outward.third(1)

    tokens_in = pltpu.make_async_copy(
        tokens_ref.at[block(c, half_rows), :], own_tokens, own_sem.at[0]
    )
    map_in = pltpu.make_async_copy(map_ref.at[z], own_map, own_sem.at[1])
    tokens_in.start()
    for copy in small:
        copy.start()
    inward.start_own()
    outward.start_own()
    map_in.start()
    pl.semaphore_wait(barrier, len(partners))
    each_place(prepare)
    tokens_in.wait()
    for copy in small:
        copy.wait()
    floated = own_tokens[...].astype(jnp.float32)
    rows_all[block(2 * z + c, half_rows), :] = (
        floated
        * lax.rsqrt(jnp.mean(floated * floated, -1, keepdims=True) + NORM_EPS)
        * norm_gain_ref[...]
    ).astype(jnp.bfloat16)
    inward.first(0)
    outward.first(0)
    pools[0:16, :] = jnp.zeros((16, width), jnp.bfloat16)
    keys[...] = jnp.zeros_like(keys)
    values[...] = jnp.zeros_like(values)
    each_place(begin)

    def table(index, carry):
        rows = block(index, row_count)
        half = HEAD_DIM // 2
        count = (
            index * row_count + lax.broadcasted_iota(jnp.int32, (row_count, HEAD_DIM), 0)
        ).astype(jnp.float32)
        lane = lax.broadcasted_iota(jnp.int32, (row_count, HEAD_DIM), 1)
        angles = count * freqs_ref[...]
        cos_ref[rows, :] = jnp.cos(angles)
        sine = jnp.sin(angles)
        sin_ref[rows, :] = jnp.where(lane < half, -sine, sine)
        return carry

    lax.fori_loop(0, places, table, 0)

    def turned(raw, cosine, sine):
        floated = raw.astype(jnp.float32)
        return (floated * cosine + pltpu.roll(floated, HEAD_DIM // 2, 1) * sine).astype(
            jnp.bfloat16
        )

    projected = [pick([row[i] for row in PROJECTED], z) for i in range(places)]
    late = [pick([row[i] for row in LATE], z) for i in range(2)]
    finished = [pick([row[i] for row in FINISHED], z) for i in range(places * PARTS)]

    def project(index):
        theirs = rows_all.at[block(2 * index + mate, half_rows), :]
        remote(theirs, theirs, token_send.at[2], mate_recv.at[index], {"tp": mate}).wait_recv()
        rows = block(index, row_count)
        normed = rows_all[rows, :]
        cosine = cos_ref[rows, :]
        sine = sin_ref[rows, :]

        def product(m):
            return jnp.dot(normed, weights[m], preferred_element_type=jnp.float32).astype(
                jnp.bfloat16
            )

        pools[pl.ds(pl.multiple_of(index * row_count + 16, 16), row_count), :] = product(0)
        raw = product(1)
        for m in range(2):
            part = slice(m * HEAD_DIM, (m + 1) * HEAD_DIM)
            queries[rows, part] = turned(raw[:, part], cosine, sine)
        raw = product(2)
        for m in range(2):
            part = slice(m * HEAD_DIM, (m + 1) * HEAD_DIM)
            keys[rows, part] = turned(raw[:, part], cosine, sine)
        values[rows, :] = product(3)

    upper = z >= places // 2

    each_place(gather)
    project(projected[0])
    each_place(more)
    relay_piece(0)
    project(projected[1])
    each_place(relay)
    relay_piece(1)

    map_in.wait()
    outward.third(0)

    level = lax.rem(c * map_ref.shape[0] + z, 4)
    window = jnp.where(
        level == 0, 2, jnp.where(level == 1, 4, jnp.where(level == 2, 8, 16))
    )
    head_lambda = lambda_ref[c * map_ref.shape[0] + z]

    part_rows = row_count // PARTS

    def to_sibling(step):
        return remote(
            to_mate.at[step],
            from_mate.at[step],
            half_send.at[0],
            half_recv.at[step],
            {"tp": mate},
        )

    outer = (z == 0) | (z == places - 1)
    pair = z + 1 - 2 * lax.rem(z, 2)

    def crossing(to, h):
        return lax.rem(to, 2) * PARTS + h

    def to_inner(to, h):
        return remote(
            to_peer.at[to * PARTS + h],
            merging.at[crossing(to, h)],
            peer_send.at[0],
            merge_recv.at[crossing(to, h)],
            {"sp": pair},
        )

    def to_place(to, h):
        return remote(
            to_peer.at[to * PARTS + h],
            from_peer.at[h],
            peer_send.at[0],
            peer_recv.at[h],
            {"sp": to},
        )

    def to_pair(h):
        return remote(
            to_peer.at[pair * PARTS + h],
            from_peer.at[PARTS + h],
            peer_send.at[0],
            peer_recv.at[PARTS + h],
            {"sp": pair},
        )

    def step_place(step):
        slot = finished[0]
        for i in range(1, places * PARTS):
            slot = jnp.where(step == i, finished[i], slot)
        return slot // PARTS, lax.rem(slot, PARTS)

    def attend(step, slot, span):
        rows = block(slot, part_rows)
        query_pos = slot * part_rows + lax.broadcasted_iota(jnp.int32, (part_rows, span), 0)
        key_pos = lax.broadcasted_iota(jnp.int32, (part_rows, span), 1)
        seen = query_pos >= key_pos
        mapped = []
        for m in range(2):
            part = slice(m * HEAD_DIM, (m + 1) * HEAD_DIM)
            scores = lax.dot_general(
                queries[rows, part],
                keys[:span, part],
                (((1,), (1,)), ((), ())),
                preferred_element_type=jnp.float32,
            ) * HEAD_DIM ** (-0.5)
            scores = jnp.where(seen, scores, -jnp.inf)
            expons = jnp.exp(scores - jnp.max(scores, -1, keepdims=True))
            totals = jnp.sum(expons, -1, keepdims=True)
            mapped.append(
                jnp.dot(
                    expons.astype(jnp.bfloat16), values[:span, :], preferred_element_type=jnp.float32
                )
                / totals
            )
        raw = mapped[0] - head_lambda * mapped[1]
        attn = (
            raw
            * lax.rsqrt(jnp.mean(raw * raw, -1, keepdims=True) + HEAD_EPS)
            * gain_ref[...]
            * HEAD_SCALE
        ).astype(jnp.bfloat16)
        extended = pools[
            pl.ds(pl.multiple_of(slot * part_rows, 16), part_rows + 16), :
        ].astype(jnp.float32)
        picked = extended + pltpu.roll(extended, 1, 0)
        sums = picked
        for shift in (2, 4, 8):
            sums = sums + pltpu.roll(sums, shift, 0)
            picked = lax.select_n(window >= 2 * shift, picked, sums)
        places_of = slot * part_rows + lax.broadcasted_iota(jnp.int32, (part_rows, 1), 0)
        counts = jnp.minimum(places_of + 1, window).astype(jnp.float32)
        mixed = (picked[16:] / counts - extended[16:]).astype(jnp.bfloat16)
        pooled = (
            jnp.dot(mixed, own_map[...], preferred_element_type=jnp.float32) * scale_ref[z]
        ).astype(jnp.bfloat16)

        features[step] = jnp.concatenate([pooled, attn], 1)

    def compute(step):
        to, h = step_place(step)
        slot = to * PARTS + h
        half = places // 2
        pl.when(to < half)(lambda: attend(step, slot, half * row_count))
        pl.when(to >= half)(lambda: attend(step, slot, length))
        return features[step, :, :width], features[step, :, width:]

    def partial_of(step, turn, pooled, attn, side):
        columns = block(side, half_out)
        value = jnp.dot(
            pooled, outs[0, :, columns], preferred_element_type=jnp.float32
        ) + jnp.dot(attn, outs[1, :, columns], preferred_element_type=jnp.float32)

        @pl.when(side == c)
        def _():
            mine[lax.rem(turn, 2)] = value

        @pl.when(side != c)
        def _():
            to_mate[step] = value.astype(jnp.bfloat16)
            to_sibling(step).start()

    def finish(step, turn):
        to, h = step_place(step)
        slot = to * PARTS + h
        crosses = to // 2 != z // 2
        to_sibling(step).wait_recv()
        summed = mine[lax.rem(turn, 2)] + from_mate[step].astype(jnp.float32)

        @pl.when(to == z)
        def _():
            final[h] = summed

        @pl.when(to == pair)
        def _():
            to_peer[slot] = summed.astype(jnp.bfloat16)
            to_pair(h).start()

        @pl.when(crosses & outer)
        def _():
            to_peer[slot] = summed.astype(jnp.bfloat16)
            to_inner(to, h).start()

        @pl.when(crosses & jnp.logical_not(outer))
        def _():
            kept[crossing(to, h)] = summed

    def merge(turn):
        place = turn // PARTS
        to = jnp.where(upper, place, places // 2 + place)
        h = lax.rem(turn, PARTS)
        to_inner(to, h).wait_recv()
        to_peer[to * PARTS + h] = (
            kept[crossing(to, h)] + merging[crossing(to, h)].astype(jnp.float32)
        ).astype(jnp.bfloat16)
        to_place(to, h).start()

    side = z // (places // 2)
    eager = side == c
    early = pick(EARLY, z)
    merged = jnp.where(upper, jnp.where(eager, 2, 3), jnp.where(eager, 3, 5))
    lag = jnp.where(outer, 0, 1)

    def grow(step):
        @pl.when((step == late[0]) | (step == late[1]))
        def _():
            @pl.when((z == 0) & (step == late[0]))
            def _():
                outward.second(3)
                take(0, 2)

            @pl.when((z == 0) & (step == late[1]))
            def _():
                take(0, 3)

            def project_late(i, carry):
                @pl.when((z == places - 1) & (i == 3))
                def _():
                    take(places - 1, 1)

                project(jnp.where(i == 2, projected[2], projected[3]))
                return carry

            lax.fori_loop(
                jnp.where(step == late[0], 2, 3), jnp.where(step == late[1], 4, 3), project_late, 0
            )

    ahead = pick(AHEAD, z)
    last = places * PARTS - 1
    seconds = [pick([row[i] for row in SECOND], z) for i in range(places * PARTS)]

    def second_step(turn):
        step = seconds[0]
        for i in range(1, places * PARTS):
            step = jnp.where(turn == i, seconds[i], step)
        return step

    def first_side(step, carry):
        grow(step)

        @pl.when(step == 1)
        def _():
            relay_piece(2)

        partial_of(step, step, *compute(step), side)

        @pl.when(eager & (step >= lag))
        def _():
            finish(step - lag, step - lag)

        return carry

    def second_side(turn):
        step = second_step(turn)
        pooled, attn = features[step, :, :width], features[step, :, width:]
        partial_of(step, turn, pooled, attn, 1 - side)

    def other_side(turn, carry):
        second_side(turn)

        @pl.when(jnp.logical_not(eager) & (turn > 0))
        def _():
            finish(second_step(turn - 1), turn - 1)

        return carry

    def both_sides(step, carry):
        grow(step)
        partial_of(step, step, *compute(step), side)
        at_once = eager & outer & (step == early)

        @pl.when(at_once)
        def _():
            finish(step, step)

        second_side(step - early + ahead)

        @pl.when((step != early + 1 - lag) & jnp.logical_not(at_once))
        def _():
            first = jnp.where(step == early, step, step - 1)
            turn = first - early + ahead
            finish(jnp.where(eager, first, second_step(turn)), jnp.where(eager, first, turn))

        again = upper & (step == last)

        @pl.when(jnp.logical_not(outer) & ((step == merged) | (step == merged + 1) | again))
        def _():
            merge(jnp.where(again, PARTS, step - merged))

        return carry

    lax.fori_loop(0, early, first_side, 0)
    each_place(finish_gather)

    @pl.when(eager & jnp.logical_not(outer))
    def _():
        finish(early - 1, early - 1)

    lax.fori_loop(0, ahead, other_side, 0)

    @pl.when(jnp.logical_not(eager))
    def _():
        finish(second_step(ahead - 1), ahead - 1)

    def merge_more(turn, carry):
        merge(turn)
        return carry

    lax.fori_loop(early, places * PARTS, both_sides, 0)
    def second_more(turn, carry):
        second_side(turn)

        @pl.when(jnp.logical_not(eager))
        def _():
            finish(second_step(turn - 1), turn - 1)

        return carry

    lax.fori_loop(last + 1 - early + ahead, last + 1, second_more, 0)
    finish(jnp.where(eager, last, second_step(last)), last)

    @pl.when(jnp.logical_not(outer))
    def _():
        lax.fori_loop(jnp.where(upper, PARTS + 1, PARTS), 2 * PARTS, merge_more, 0)

    for h in range(PARTS):
        to_pair(h).wait_recv()
        total = final[h] + from_peer[PARTS + h].astype(jnp.float32)
        to_place(z, h).wait_recv()
        out_ref[h * part_rows : (h + 1) * part_rows, :] = (
            total + from_peer[h].astype(jnp.float32)
        ).astype(out_ref.dtype)

    inward.drain()
    outward.drain()

    def drain(place):
        if place < places - 1:
            sent_tokens(0, place + 1).wait_send()
        if place > 0:
            sent_tokens(1, places - place).wait_send()

    each_place(drain)
    sent_tokens(2, places).wait_send()
    remote(to_mate, from_mate, half_send.at[0], half_recv.at[0], {"tp": mate}).wait_send()
    sent = to_peer.at[pl.ds(0, (places - 1) * PARTS)]
    remote(sent, sent, peer_send.at[0], peer_recv.at[0], {"sp": pair}).wait_send()


def fused(
    tokens,
    norm_gain,
    pool_input,
    query_weight,
    key_weight,
    value_weight,
    pool_map,
    pool_scale,
    head_gain,
    diff_lambda,
    out_pool,
    out_heads,
):
    places = lax.axis_size("sp")
    groups = lax.axis_size("fs")
    row_count, model = tokens.shape[1], tokens.shape[2]
    length = places * row_count
    half = HEAD_DIM // 2
    freqs = np.float32(1.0) / np.float32(THETA) ** (
        np.arange(half, dtype=np.float32) * np.float32(2.0) / np.float32(HEAD_DIM)
    )
    freqs = jnp.asarray(np.concatenate([freqs, freqs])[None, :], jnp.float32)
    group_count = pool_map.shape[0]
    half_out = model // 2
    vmem = pl.BlockSpec(memory_space=pltpu.VMEM)
    hbm = pl.BlockSpec(memory_space=pl.ANY)
    dma = pltpu.SemaphoreType.DMA
    low = jnp.bfloat16

    def gather_sems(count):
        return [
            dma((count,)),
            dma((places,)),
            dma((places,)),
            dma((2,)),
            dma((2, places)),
            dma((2,)),
        ]

    out = pl.pallas_call(
        lambda *refs: fused_kernel(places, groups, *refs),
        out_shape=jax.ShapeDtypeStruct((row_count, half_out), low),
        in_specs=[hbm] * 13,
        out_specs=vmem,
        scratch_shapes=[
            pltpu.VMEM((row_count // 2, model), low),
            pltpu.VMEM((GROUP_DIM, GROUP_DIM), low),
            pltpu.VMEM((1, model), jnp.float32),
            pltpu.VMEM((1, HEAD_DIM), jnp.float32),
            pltpu.VMEM((group_count, 1, GROUP_DIM), jnp.float32),
            pltpu.VMEM((1, 2 * HEAD_DIM), jnp.float32),
            pltpu.SMEM(diff_lambda.shape, jnp.float32),
            pltpu.VMEM((length, HEAD_DIM), jnp.float32),
            pltpu.VMEM((length, HEAD_DIM), jnp.float32),
            pltpu.VMEM((length, model), low),
            pltpu.VMEM((4, model, GROUP_DIM), low),
            pltpu.VMEM((2, GROUP_DIM, model), low),
            pltpu.VMEM((length, GROUP_DIM), low),
            pltpu.VMEM((length, GROUP_DIM), low),
            pltpu.VMEM((length, GROUP_DIM), low),
            pltpu.VMEM((length + 16, GROUP_DIM), low),
            pltpu.VMEM((places * PARTS, row_count // PARTS, 2 * GROUP_DIM), low),
            pltpu.VMEM((2, row_count // PARTS, half_out), jnp.float32),
            pltpu.VMEM((places * PARTS, row_count // PARTS, half_out), low),
            pltpu.VMEM((places * PARTS, row_count // PARTS, half_out), low),
            pltpu.VMEM((2 * PARTS, row_count // PARTS, half_out), jnp.float32),
            pltpu.VMEM((places * PARTS, row_count // PARTS, half_out), low),
            pltpu.VMEM((2 * PARTS, row_count // PARTS, half_out), low),
            pltpu.VMEM((2 * PARTS, row_count // PARTS, half_out), low),
            pltpu.VMEM((PARTS, row_count // PARTS, half_out), jnp.float32),
            dma((2,)),
            dma((5,)),
            *gather_sems(4),
            *gather_sems(2),
            dma((3,)),
            dma((places, PIECES)),
            dma((places,)),
            dma((1,)),
            dma((places * PARTS,)),
            dma((1,)),
            dma((2 * PARTS,)),
            dma((2 * PARTS,)),
        ],
        compiler_params=pltpu.CompilerParams(
            collective_id=0, has_side_effects=True, vmem_limit_bytes=56 * 1024 * 1024
        ),
    )(
        tokens[0],
        norm_gain.reshape(1, model),
        freqs,
        pool_input,
        query_weight,
        key_weight,
        value_weight,
        pool_map,
        pool_scale.reshape(group_count, 1, GROUP_DIM),
        head_gain.reshape(1, 2 * HEAD_DIM),
        diff_lambda,
        out_pool,
        out_heads,
    )
    return out[None]


def solution(mesh):
    placed = (
        P("fs", "sp", None),
        P(),
        P(("sp", "fs"), "tp"),
        P(("sp", "fs"), "tp"),
        P(("sp", "fs"), "tp"),
        P(("sp", "fs"), "tp"),
        P("tp", None, None),
        P("tp"),
        P(),
        P(),
        P("tp", ("sp", "fs")),
        P("tp", ("sp", "fs")),
    )
    shape = dict(mesh.shape)

    def body(tokens, *rest):
        head_count = rest[3].shape[1] // (2 * HEAD_DIM)
        group_count = rest[5].shape[0]
        fits = (
            shape["fs"] == 4
            and shape["tp"] == 2
            and shape["sp"] == head_count == group_count == 4
            and tokens.shape[0] == 1
        )
        return (fused if fits else local)(tokens, *rest)

    return jax.shard_map(
        body, mesh=mesh, in_specs=placed, out_specs=P("fs", "sp", "tp"), check_vma=False
    )
```

```python
import math

import jax
import jax.numpy as jnp
import numpy as np
from jax import lax
from jax.experimental import pallas as pl
from jax.experimental.pallas import tpu as pltpu
from jax.sharding import PartitionSpec as P

HEAD_DIM = 128
GROUP_DIM = 256


THETA = 500000.0
HEAD_SCALE = 0.8
NORM_EPS = 1e-06
HEAD_EPS = 1e-05


def from_behind(value, axis, steps):
    count = lax.axis_size(axis)
    first, last = (max(0, -steps), min(count, count - steps))
    return lax.ppermute(value, axis, [(source, source + steps) for source in range(first, last)])


def rotate(tensor, positions):
    half = HEAD_DIM // 2
    freqs = 1.0 / THETA ** (jnp.arange(half, dtype=jnp.float32) * 2.0 / HEAD_DIM)
    angles = positions[:, None] * freqs[None, :]
    cosine = jnp.cos(angles)[:, None, None, :]
    sine = jnp.sin(angles)[:, None, None, :]
    floated = tensor.astype(jnp.float32)
    first = floated[..., :half]
    second = floated[..., half:]
    turned = jnp.concatenate([first * cosine - second * sine, second * cosine + first * sine], -1)
    return turned.astype(jnp.bfloat16)


def local(
    tokens,
    norm_gain,
    pool_input,
    query_weight,
    key_weight,
    value_weight,
    pool_map,
    pool_scale,
    head_gain,
    diff_lambda,
    out_pool,
    out_heads,
):
    out_local = jnp.concatenate([out_pool, out_heads], 0)
    row_count = tokens.shape[1]
    floated = tokens[0].astype(jnp.float32)
    normed = (
        floated * lax.rsqrt(jnp.mean(floated * floated, -1, keepdims=True) + NORM_EPS) * norm_gain
    ).astype(jnp.bfloat16)
    fragments = (
        lax.all_gather(pool_input, ("sp", "fs"), axis=0, tiled=True),
        lax.all_gather(query_weight, ("sp", "fs"), axis=0, tiled=True),
        lax.all_gather(key_weight, ("sp", "fs"), axis=0, tiled=True),
        lax.all_gather(value_weight, ("sp", "fs"), axis=0, tiled=True),
    )
    projected = tuple(
        (jnp.dot(normed, fragment, preferred_element_type=jnp.float32) for fragment in fragments)
    )
    pool_in, queries, keys_flat, values_flat = [
        product.astype(jnp.bfloat16) for product in projected
    ]
    head_count = values_flat.shape[1] // (2 * HEAD_DIM)
    tp_index = lax.axis_index("tp")
    sp_index = lax.axis_index("sp")
    query_pos = sp_index * row_count + jnp.arange(row_count, dtype=jnp.int32)
    positions = query_pos.astype(jnp.float32)
    queries = rotate(queries.reshape(row_count, head_count, 2, HEAD_DIM), positions)
    keys_flat = rotate(keys_flat.reshape(row_count, head_count, 2, HEAD_DIM), positions).reshape(
        row_count, head_count * 2 * HEAD_DIM
    )
    lambdas = lax.dynamic_slice_in_dim(diff_lambda, tp_index * head_count, head_count, 0)

    def online_step(state, key_rows, value_rows, key_offset):
        largest, summed, accum = state
        width = key_rows.shape[0]
        shaped = key_rows.reshape(width, head_count, 2, HEAD_DIM)
        scores = jnp.einsum(
            "qhcd,khcd->chqk", queries, shaped, preferred_element_type=jnp.float32
        ) * HEAD_DIM ** (-0.5)
        key_pos = key_offset + jnp.arange(width, dtype=jnp.int32)
        scores = jnp.where(query_pos[:, None] >= key_pos[None, :], scores, -jnp.inf)
        newest = jnp.maximum(largest, jnp.max(scores, -1))
        anchor = jnp.where(jnp.isfinite(newest), newest, 0.0)
        rescale = jnp.exp(largest - anchor)
        expons = jnp.exp(scores - anchor[..., None])
        summed = summed * rescale + jnp.sum(expons, -1)
        value_shaped = value_rows.reshape(width, head_count, 2 * HEAD_DIM)
        added = jnp.einsum(
            "chqk,khe->chqe",
            expons.astype(jnp.bfloat16),
            value_shaped,
            preferred_element_type=jnp.float32,
        )
        accum = accum * rescale[..., None] + added
        return (newest, summed, accum)

    start_state = (
        jnp.full((2, head_count, row_count), -jnp.inf, jnp.float32),
        jnp.zeros((2, head_count, row_count), jnp.float32),
        jnp.zeros((2, head_count, row_count, 2 * HEAD_DIM), jnp.float32),
    )
    fragments = (
        lax.all_gather(keys_flat, "sp", axis=0, tiled=True),
        lax.all_gather(values_flat, "sp", axis=0, tiled=True),
    )
    span = math.gcd(fragments[0].shape[0], 1024)

    def inner_step(index, inner_state):
        key_rows = lax.dynamic_slice_in_dim(fragments[0], index * span, span, 0)
        value_rows = lax.dynamic_slice_in_dim(fragments[1], index * span, span, 0)
        return online_step(inner_state, key_rows, value_rows, index * span)

    final_state = lax.fori_loop(0, fragments[0].shape[0] // span, inner_step, start_state)
    summed_final = final_state[1]
    accum_final = final_state[2]
    heads_raw = (
        accum_final[0] / summed_final[0][..., None]
        - lambdas[:, None, None] * accum_final[1] / summed_final[1][..., None]
    )
    heads_raw = jnp.moveaxis(heads_raw, 0, 1)
    attn = (
        (
            heads_raw
            * lax.rsqrt(jnp.mean(heads_raw * heads_raw, -1, keepdims=True) + HEAD_EPS)
            * head_gain
            * HEAD_SCALE
        )
        .astype(jnp.bfloat16)
        .reshape(row_count, head_count * 2 * HEAD_DIM)
    )
    reach = 15
    rim_rows = from_behind(pool_in[row_count - reach :], "sp", 1)
    extended = jnp.concatenate([rim_rows, pool_in], 0).astype(jnp.float32)
    pair_sums = extended[1:] + extended[:-1]
    quad_sums = pair_sums[2:] + pair_sums[:-2]
    octet_sums = quad_sums[4:] + quad_sums[:-4]
    sixteen_sums = octet_sums[8:] + octet_sums[:-8]
    group_count = pool_in.shape[1] // GROUP_DIM
    stacked = jnp.stack(
        [
            pair_sums[14 : 14 + row_count],
            quad_sums[12 : 12 + row_count],
            octet_sums[8 : 8 + row_count],
            sixteen_sums,
        ],
        0,
    ).reshape(4, row_count, group_count, GROUP_DIM)
    levels = (tp_index * group_count + jnp.arange(group_count, dtype=jnp.int32)) % 4
    picked = jnp.sum(
        jnp.where(
            levels[None, None, :, None] == jnp.arange(4, dtype=jnp.int32)[:, None, None, None],
            stacked,
            0.0,
        ),
        0,
    )
    windows = 2 ** (1 + levels)
    counts = jnp.minimum(query_pos[:, None] + 1, windows[None, :]).astype(jnp.float32)
    window_mean = picked / counts[:, :, None]
    grouped = pool_in.reshape(row_count, group_count, GROUP_DIM).astype(jnp.float32)
    pool_mixed = (window_mean - grouped).astype(jnp.bfloat16)
    pooled = (
        (
            jnp.einsum("tgc,gce->tge", pool_mixed, pool_map, preferred_element_type=jnp.float32)
            * pool_scale.reshape(group_count, GROUP_DIM)
        )
        .astype(jnp.bfloat16)
        .reshape(row_count, group_count * GROUP_DIM)
    )
    branches = jnp.concatenate([pooled, attn], 1)
    partial_value = jnp.dot(
        branches,
        lax.all_gather(out_local, ("sp", "fs"), axis=1, tiled=True),
        preferred_element_type=jnp.float32,
    )
    layer_out = lax.psum_scatter(
        partial_value.astype(jnp.bfloat16), "tp", scatter_dimension=1, tiled=True
    )
    return layer_out[None]


MESH = pl.DeviceIdType.MESH
PIECES = 8
PARTS = 2

PROJECTED = ((0, 1, 2, 3), (1, 0, 2, 3), (2, 0, 3, 1), (3, 0, 2, 1))
LATE = ((2, 4), (0, 4), (2, 2), (2, 2))
FINISHED = (
    (2, 3, 4, 5, 6, 7, 0, 1),
    (4, 5, 0, 1, 6, 7, 2, 3),
    (0, 1, 6, 7, 2, 3, 4, 5),
    (0, 1, 2, 3, 4, 5, 6, 7),
)
EARLY = (4, 2, 2, 2)
SECOND = ((2, 3, 4, 5, 0, 1, 6, 7),) + 3 * ((0, 1, 2, 3, 4, 5, 6, 7),)
AHEAD = (2, 2, 2, 2)
ARRIVALS = ((0, 1, 2, 3), (1, 0, 3, 2), (2, 3, 0, 1), (3, 2, 1, 0))
SENDS = ((0, 1, 2, 3), (1, 3, 2, 0), (2, 0, 1, 3), (3, 2, 1, 0))
SLOTS = tuple(
    tuple(ARRIVALS[to].index(place) for to in SENDS[place]) for place in range(len(SENDS))
)


def pick(row, z):
    value = jnp.int32(row[0])
    for place in range(1, len(row)):
        value = jnp.where(z == place, row[place], value)
    return value


def fused_kernel(
    places,
    groups,
    tokens_ref,
    norm_gain_hbm,
    freqs_hbm,
    pool_ref,
    query_ref,
    key_ref,
    value_ref,
    map_ref,
    scale_hbm,
    gain_hbm,
    lambda_hbm,
    out_pool_ref,
    out_heads_ref,
    out_ref,
    own_tokens,
    own_map,
    norm_gain_ref,
    freqs_ref,
    scale_ref,
    gain_ref,
    lambda_ref,
    cos_ref,
    sin_ref,
    rows_all,
    weights,
    outs,
    queries,
    keys,
    values,
    pools,
    features,
    mine,
    to_mate,
    from_mate,
    kept,
    to_peer,
    from_peer,
    merging,
    final,
    result,
    result_sem,
    *sems,
):
    (
        own_sem,
        small_sem,
        in_local,
        in_z_send,
        in_z_recv,
        in_n_send,
        in_n_recv,
        in_rest,
        out_local,
        out_z_send,
        out_z_recv,
        out_n_send,
        out_n_recv,
        out_rest,
        token_send,
        token_recv,
        mate_recv,
        half_send,
        half_recv,
        peer_send,
        peer_recv,
        merge_recv,
    ) = sems
    z = lax.axis_index("sp")
    f = lax.axis_index("fs")
    c = lax.axis_index("tp")
    fx = f + 1 - 2 * lax.rem(f, 2)
    fy = lax.rem(f + 2, groups)
    mate = 1 - c
    half_rows = tokens_ref.shape[0] // 2
    row_count = 2 * half_rows
    depth = pool_ref.shape[0]
    width = GROUP_DIM
    out_width = out_pool_ref.shape[1]
    half_out = out_ref.shape[1]
    length = places * row_count

    send_to = [pick([row[d] for row in SENDS], z) for d in range(places)]
    send_slot = [pick([row[d] for row in SLOTS], z) for d in range(places)]
    source = [pick([row[d] for row in ARRIVALS], z) for d in range(places)]

    def block(index, size):
        return pl.ds(pl.multiple_of(index * size, size), size)

    small = [
        pltpu.make_async_copy(source, target, small_sem.at[i])
        for i, (source, target) in enumerate(
            (
                (norm_gain_hbm, norm_gain_ref),
                (freqs_hbm, freqs_ref),
                (scale_hbm, scale_ref),
                (gain_hbm, gain_ref),
                (lambda_hbm, lambda_ref),
            )
        )
    ]
    barrier = pltpu.get_barrier_semaphore()
    partners = [{"sp": lax.rem(z + d, places)} for d in range(1, places)]
    partners += [{"fs": fx}, {"fs": fy}, {"tp": mate}]
    for partner in partners:
        pl.semaphore_signal(barrier, inc=1, device_id=partner, device_id_type=MESH)

    def remote(source, target, send, recv, device):
        return pltpu.make_async_remote_copy(
            src_ref=source,
            dst_ref=target,
            send_sem=send,
            recv_sem=recv,
            device_id=device,
            device_id_type=MESH,
        )

    class Gather:
        def __init__(self, sources, cut, view, sent, received, group):
            self.sources, self.cut, self.view = sources, cut, view
            self.sent, self.received = sent, received
            self.count = len(sources)
            (
                self.local,
                self.z_send,
                self.z_recv,
                self.n_send,
                self.n_recv,
                self.rest,
            ) = group
            self.low = (0, self.count // 2)
            self.high = (self.count // 2, self.count - self.count // 2)

        def own(self, m):
            return pltpu.make_async_copy(
                self.cut(self.sources[m], z), self.view(z, f, m, 1).at[0], self.local.at[m]
            )

        def across(self, d, m):
            to, slot = send_to[d], send_slot[d]
            return remote(
                self.cut(self.sources[m], to),
                self.view(z, f, m, 1).at[0],
                self.z_send.at[d],
                self.z_recv.at[slot],
                {"sp": to},
            )

        def arrive(self, d):
            view = self.view(source[d], f, 0, self.count)
            return remote(view, view, self.z_send.at[d], self.z_recv.at[d], {"sp": source[d]})

        def near(self, d, side, column, half):
            start, size = (self.low, self.high)[half]
            view = self.view(source[d], column, start, size)
            early = half == side
            return remote(
                view,
                view,
                self.n_send.at[side],
                self.n_recv.at[side, d] if early else self.rest.at[d // 2],
                {"fs": (fx, fy)[side]},
            )

        def forward(self, d, side, column):
            start, size = (self.high, self.low)[side]
            view = self.view(source[d], column, start, size)
            return remote(
                view, view, self.n_send.at[side], self.rest.at[d // 2], {"fs": (fx, fy)[side]}
            )

        def start_own(self):
            for m in range(self.count):
                self.own(m).start()

        def start(self, d):
            for m in range(self.count):
                self.across(d, m).start()

        def first(self, d):
            if d == 0:
                for m in range(self.count):
                    self.own(m).wait()
            else:
                self.arrive(d).wait_recv()
            for order in range(2):
                for side in range(2):
                    self.near(d, side, f, side ^ order).start()

        def second(self, d):
            self.near(d, 0, fx, 0).wait_recv()
            self.forward(d, 1, fx).start()
            self.near(d, 1, fy, 1).wait_recv()
            self.forward(d, 0, fy).start()

        def third(self, part):
            remote(
                self.received, self.received, self.n_send.at[0], self.rest.at[part], {"fs": fx}
            ).wait_recv()

        def drain(self):
            for d in range(1, places):
                self.arrive(d).wait_send()
            for side in range(2):
                remote(
                    self.sent, self.sent, self.n_send.at[side], self.rest.at[0], {"fs": fx}
                ).wait_send()

    filled = places * groups
    inward = Gather(
        (pool_ref, query_ref, key_ref, value_ref),
        lambda ref, to: ref.at[:, block(to, width)],
        lambda zz, ff, m, n: weights.at[pl.ds(m, n), block(zz * groups + ff, depth), :],
        weights.at[:, pl.ds(0, filled * 3 // 8 * depth), :],
        weights.at[:, pl.ds(0, filled // 4 * depth), :],
        (in_local, in_z_send, in_z_recv, in_n_send, in_n_recv, in_rest),
    )
    outward = Gather(
        (out_pool_ref, out_heads_ref),
        lambda ref, to: ref.at[block(to, width), :],
        lambda zz, ff, m, n: outs.at[pl.ds(m, n), :, block(zz * groups + ff, out_width)],
        outs.at[:, :, pl.ds(0, filled * 3 // 8 * out_width)],
        outs.at[:, :, pl.ds(0, filled // 4 * out_width)],
        (out_local, out_z_send, out_z_recv, out_n_send, out_n_recv, out_rest),
    )

    piece_rows = half_rows // PIECES

    def chunk(b, side, p):
        return rows_all.at[block((2 * b + side) * PIECES + p, piece_rows), :]

    def right(b, p, step=1):
        view = chunk(b, c, p)
        return remote(view, view, token_send.at[0], token_recv.at[b, p], {"sp": z + step})

    def left(b, p, step=-1):
        view = chunk(b, c, p)
        return remote(view, view, token_send.at[1], token_recv.at[b, p], {"sp": z + step})

    def share(b, side, p):
        view = chunk(b, side, p)
        return remote(view, view, token_send.at[2], mate_recv.at[b], {"tp": mate})

    def sent_tokens(kind, blocks):
        view = rows_all.at[pl.ds(0, blocks * half_rows), :]
        return remote(view, view, token_send.at[kind], mate_recv.at[0], {"tp": mate})

    def each_place(act):
        for place in range(places):
            pl.when(z == place)(lambda place=place: act(place))

    def send_right(place, pieces=range(PIECES)):
        for p in pieces:
            right(place, p).start()

    def send_left(place):
        for p in range(PIECES):
            left(place, p).start()

    def take(place, b, pieces=range(PIECES)):
        for p in pieces:
            if b < place:
                right(b, p, -1).wait_recv()
                if place < places - 1:
                    right(b, p).start()
            else:
                left(b, p, 1).wait_recv()
                if place > 0:
                    left(b, p).start()
            share(b, c, p).start()

    first_half, second_half = range(PIECES // 2), range(PIECES // 2, PIECES)

    def prepare(place):
        for d in range(1, places):
            inward.start(d)
        for d in range(1, 2 if place == 0 else places):
            outward.start(d)

    def begin(place):
        if place == 0:
            send_right(place)
        if place == places - 1:
            send_left(place)
        for p in range(PIECES):
            share(place, c, p).start()

    def gather(place):
        inward.second(0)
        outward.second(0)
        inward.first(1)
        inward.first(2)
        if place == 0:
            inward.second(1)
            inward.first(3)
            inward.second(2)
            inward.second(3)
            outward.first(1)
            outward.first(2)
            take(place, 1)
            outward.second(1)
            for d in range(2, places):
                outward.start(d)
        if place == 1:
            send_left(place)
            inward.second(1)
            outward.first(1)
            inward.second(2)
            take(place, 0, first_half)
            inward.first(3)
            take(place, 0, second_half)
            send_right(place)
            outward.first(3)
            outward.second(1)
            inward.second(3)
            outward.first(2)
            take(place, 2, first_half)
            outward.second(3)
            take(place, 2, second_half)
        if place == 2:
            send_right(place)
            send_left(place)
            inward.second(1)
            outward.first(1)
            inward.second(2)
            inward.first(3)
            outward.first(3)
            outward.second(1)
            take(place, 0, first_half)
            inward.second(3)
            take(place, 0, second_half)
            outward.second(3)
            take(place, 3)
        if place == 3:
            inward.second(1)
            inward.first(3)
            outward.first(1)
            inward.second(2)
            outward.first(2)
            inward.second(3)
            outward.second(1)
            take(place, 2)
            outward.second(2)
        inward.third(0)
        inward.third(1)

    def relay_piece(p):
        def act(place):
            if place in (1, 2):
                take(place, (None, 3, 1, None)[place], range(p * PIECES // 4, (p + 1) * PIECES // 4))

        each_place(act)

    def more(place):
        if place == 0:
            outward.first(3)
        if place == 1:
            outward.second(2)
        if place == 2:
            outward.first(2)
        if place == 3:
            take(place, 0)

    def relay(place):
        if place in (0, 2):
            outward.second(2)
        if place == 3:
            outward.first(3)

    def finish_gather(place):
        if place in (1, 2):
            take(place, (None, 3, 1, None)[place], range(3 * PIECES // 4, PIECES))
        if place == places - 1:
            outward.second(3)
        outward.third(1)

    tokens_in = pltpu.make_async_copy(
        tokens_ref.at[block(c, half_rows), :], own_tokens, own_sem.at[0]
    )
    map_in = pltpu.make_async_copy(map_ref.at[z], own_map, own_sem.at[1])
    tokens_in.start()
    for copy in small:
        copy.start()
    inward.start_own()
    outward.start_own()
    map_in.start()
    pl.semaphore_wait(barrier, len(partners))
    each_place(prepare)
    tokens_in.wait()
    for copy in small:
        copy.wait()
    floated = own_tokens[...].astype(jnp.float32)
    rows_all[block(2 * z + c, half_rows), :] = (
        floated
        * lax.rsqrt(jnp.mean(floated * floated, -1, keepdims=True) + NORM_EPS)
        * norm_gain_ref[...]
    ).astype(jnp.bfloat16)
    inward.first(0)
    outward.first(0)
    pools[0:16, :] = jnp.zeros((16, width), jnp.bfloat16)
    keys[...] = jnp.zeros_like(keys)
    values[...] = jnp.zeros_like(values)
    each_place(begin)

    def table(index, carry):
        rows = block(index, row_count)
        half = HEAD_DIM // 2
        count = (
            index * row_count + lax.broadcasted_iota(jnp.int32, (row_count, HEAD_DIM), 0)
        ).astype(jnp.float32)
        lane = lax.broadcasted_iota(jnp.int32, (row_count, HEAD_DIM), 1)
        angles = count * freqs_ref[...]
        cos_ref[rows, :] = jnp.cos(angles)
        sine = jnp.sin(angles)
        sin_ref[rows, :] = jnp.where(lane < half, -sine, sine)
        return carry

    lax.fori_loop(0, places, table, 0)

    def turned(raw, cosine, sine):
        floated = raw.astype(jnp.float32)
        return (floated * cosine + pltpu.roll(floated, HEAD_DIM // 2, 1) * sine).astype(
            jnp.bfloat16
        )

    projected = [pick([row[i] for row in PROJECTED], z) for i in range(places)]
    late = [pick([row[i] for row in LATE], z) for i in range(2)]
    finished = [pick([row[i] for row in FINISHED], z) for i in range(places * PARTS)]

    def project(index):
        theirs = rows_all.at[block(2 * index + mate, half_rows), :]
        remote(theirs, theirs, token_send.at[2], mate_recv.at[index], {"tp": mate}).wait_recv()
        rows = block(index, row_count)
        normed = rows_all[rows, :]
        cosine = cos_ref[rows, :]
        sine = sin_ref[rows, :]

        def product(m):
            return jnp.dot(normed, weights[m], preferred_element_type=jnp.float32).astype(
                jnp.bfloat16
            )

        pools[pl.ds(pl.multiple_of(index * row_count + 16, 16), row_count), :] = product(0)
        raw = product(1)
        for m in range(2):
            part = slice(m * HEAD_DIM, (m + 1) * HEAD_DIM)
            queries[rows, part] = turned(raw[:, part], cosine, sine)
        raw = product(2)
        for m in range(2):
            part = slice(m * HEAD_DIM, (m + 1) * HEAD_DIM)
            keys[rows, part] = turned(raw[:, part], cosine, sine)
        values[rows, :] = product(3)

    upper = z >= places // 2

    each_place(gather)
    project(projected[0])
    each_place(more)
    relay_piece(0)
    project(projected[1])
    each_place(relay)
    relay_piece(1)

    map_in.wait()
    outward.third(0)

    level = lax.rem(c * map_ref.shape[0] + z, 4)
    window = jnp.where(
        level == 0, 2, jnp.where(level == 1, 4, jnp.where(level == 2, 8, 16))
    )
    head_lambda = lambda_ref[c * map_ref.shape[0] + z]

    part_rows = row_count // PARTS

    def to_sibling(step):
        return remote(
            to_mate.at[step],
            from_mate.at[step],
            half_send.at[0],
            half_recv.at[step],
            {"tp": mate},
        )

    outer = (z == 0) | (z == places - 1)
    pair = z + 1 - 2 * lax.rem(z, 2)

    def crossing(to, h):
        return lax.rem(to, 2) * PARTS + h

    def to_inner(to, h):
        return remote(
            to_peer.at[to * PARTS + h],
            merging.at[crossing(to, h)],
            peer_send.at[0],
            merge_recv.at[crossing(to, h)],
            {"sp": pair},
        )

    def to_place(to, h):
        return remote(
            to_peer.at[to * PARTS + h],
            from_peer.at[h],
            peer_send.at[0],
            peer_recv.at[h],
            {"sp": to},
        )

    def to_pair(h):
        return remote(
            to_peer.at[pair * PARTS + h],
            from_peer.at[PARTS + h],
            peer_send.at[0],
            peer_recv.at[PARTS + h],
            {"sp": pair},
        )

    def step_place(step):
        slot = finished[0]
        for i in range(1, places * PARTS):
            slot = jnp.where(step == i, finished[i], slot)
        return slot // PARTS, lax.rem(slot, PARTS)

    def attend(step, slot, span):
        rows = block(slot, part_rows)
        query_pos = slot * part_rows + lax.broadcasted_iota(jnp.int32, (part_rows, span), 0)
        key_pos = lax.broadcasted_iota(jnp.int32, (part_rows, span), 1)
        seen = query_pos >= key_pos
        mapped = []
        for m in range(2):
            part = slice(m * HEAD_DIM, (m + 1) * HEAD_DIM)
            scores = lax.dot_general(
                queries[rows, part],
                keys[:span, part],
                (((1,), (1,)), ((), ())),
                preferred_element_type=jnp.float32,
            ) * HEAD_DIM ** (-0.5)
            scores = jnp.where(seen, scores, -jnp.inf)
            expons = jnp.exp(scores - jnp.max(scores, -1, keepdims=True))
            totals = jnp.sum(expons, -1, keepdims=True)
            mapped.append(
                jnp.dot(
                    expons.astype(jnp.bfloat16), values[:span, :], preferred_element_type=jnp.float32
                )
                / totals
            )
        raw = mapped[0] - head_lambda * mapped[1]
        attn = (
            raw
            * lax.rsqrt(jnp.mean(raw * raw, -1, keepdims=True) + HEAD_EPS)
            * gain_ref[...]
            * HEAD_SCALE
        ).astype(jnp.bfloat16)
        extended = pools[
            pl.ds(pl.multiple_of(slot * part_rows, 16), part_rows + 16), :
        ].astype(jnp.float32)
        picked = extended + pltpu.roll(extended, 1, 0)
        sums = picked
        for shift in (2, 4, 8):
            sums = sums + pltpu.roll(sums, shift, 0)
            picked = lax.select_n(window >= 2 * shift, picked, sums)
        places_of = slot * part_rows + lax.broadcasted_iota(jnp.int32, (part_rows, 1), 0)
        counts = jnp.minimum(places_of + 1, window).astype(jnp.float32)
        mixed = (picked[16:] / counts - extended[16:]).astype(jnp.bfloat16)
        pooled = (
            jnp.dot(mixed, own_map[...], preferred_element_type=jnp.float32) * scale_ref[z]
        ).astype(jnp.bfloat16)

        features[step] = jnp.concatenate([pooled, attn], 1)

    def compute(step):
        to, h = step_place(step)
        slot = to * PARTS + h
        half = places // 2
        pl.when(to < half)(lambda: attend(step, slot, half * row_count))
        pl.when(to >= half)(lambda: attend(step, slot, length))
        return features[step, :, :width], features[step, :, width:]

    def partial_of(step, turn, pooled, attn, side):
        columns = block(side, half_out)
        value = jnp.dot(
            pooled, outs[0, :, columns], preferred_element_type=jnp.float32
        ) + jnp.dot(attn, outs[1, :, columns], preferred_element_type=jnp.float32)

        @pl.when(side == c)
        def _():
            mine[lax.rem(turn, 2)] = value

        @pl.when(side != c)
        def _():
            to_mate[step] = value.astype(jnp.bfloat16)
            to_sibling(step).start()

    def finish(step, turn):
        to, h = step_place(step)
        slot = to * PARTS + h
        crosses = to // 2 != z // 2
        to_sibling(step).wait_recv()
        summed = mine[lax.rem(turn, 2)] + from_mate[step].astype(jnp.float32)

        @pl.when(to == z)
        def _():
            final[h] = summed

        @pl.when(to == pair)
        def _():
            to_peer[slot] = summed.astype(jnp.bfloat16)
            to_pair(h).start()

        @pl.when(crosses & outer)
        def _():
            to_peer[slot] = summed.astype(jnp.bfloat16)
            to_inner(to, h).start()

        @pl.when(crosses & jnp.logical_not(outer))
        def _():
            kept[crossing(to, h)] = summed

    def merge(turn):
        place = turn // PARTS
        to = jnp.where(upper, place, places // 2 + place)
        h = lax.rem(turn, PARTS)
        to_inner(to, h).wait_recv()
        to_peer[to * PARTS + h] = (
            kept[crossing(to, h)] + merging[crossing(to, h)].astype(jnp.float32)
        ).astype(jnp.bfloat16)
        to_place(to, h).start()

    side = z // (places // 2)
    eager = side == c
    early = pick(EARLY, z)
    merged = jnp.where(upper, jnp.where(eager, 2, 3), jnp.where(eager, 3, 5))
    lag = jnp.where(outer, 0, 1)

    def grow(step):
        @pl.when((step == late[0]) | (step == late[1]))
        def _():
            @pl.when((z == 0) & (step == late[0]))
            def _():
                outward.second(3)
                take(0, 2)

            @pl.when((z == 0) & (step == late[1]))
            def _():
                take(0, 3)

            def project_late(i, carry):
                @pl.when((z == places - 1) & (i == 3))
                def _():
                    take(places - 1, 1)

                project(jnp.where(i == 2, projected[2], projected[3]))
                return carry

            lax.fori_loop(
                jnp.where(step == late[0], 2, 3), jnp.where(step == late[1], 4, 3), project_late, 0
            )

    ahead = pick(AHEAD, z)
    last = places * PARTS - 1
    seconds = [pick([row[i] for row in SECOND], z) for i in range(places * PARTS)]

    def second_step(turn):
        step = seconds[0]
        for i in range(1, places * PARTS):
            step = jnp.where(turn == i, seconds[i], step)
        return step

    def first_side(step, carry):
        grow(step)

        @pl.when(step == 1)
        def _():
            relay_piece(2)

        partial_of(step, step, *compute(step), side)

        @pl.when(eager & (step >= lag))
        def _():
            finish(step - lag, step - lag)

        return carry

    def second_side(turn):
        step = second_step(turn)
        pooled, attn = features[step, :, :width], features[step, :, width:]
        partial_of(step, turn, pooled, attn, 1 - side)

    def other_side(turn, carry):
        second_side(turn)

        @pl.when(jnp.logical_not(eager) & (turn > 0))
        def _():
            finish(second_step(turn - 1), turn - 1)

        return carry

    def both_sides(step, carry):
        grow(step)
        partial_of(step, step, *compute(step), side)
        at_once = eager & outer & (step == early)

        @pl.when(at_once)
        def _():
            finish(step, step)

        second_side(step - early + ahead)

        @pl.when((step != early + 1 - lag) & jnp.logical_not(at_once))
        def _():
            first = jnp.where(step == early, step, step - 1)
            turn = first - early + ahead
            finish(jnp.where(eager, first, second_step(turn)), jnp.where(eager, first, turn))

        again = upper & (step == last)

        @pl.when(jnp.logical_not(outer) & ((step == merged) | (step == merged + 1) | again))
        def _():
            merge(jnp.where(again, PARTS, step - merged))

        return carry

    lax.fori_loop(0, early, first_side, 0)
    each_place(finish_gather)

    @pl.when(eager & jnp.logical_not(outer))
    def _():
        finish(early - 1, early - 1)

    lax.fori_loop(0, ahead, other_side, 0)

    @pl.when(jnp.logical_not(eager))
    def _():
        finish(second_step(ahead - 1), ahead - 1)

    def merge_more(turn, carry):
        merge(turn)
        return carry

    lax.fori_loop(early, places * PARTS, both_sides, 0)
    def second_more(turn, carry):
        second_side(turn)

        @pl.when(jnp.logical_not(eager))
        def _():
            finish(second_step(turn - 1), turn - 1)

        return carry

    lax.fori_loop(last + 1 - early + ahead, last + 1, second_more, 0)
    finish(jnp.where(eager, last, second_step(last)), last)

    @pl.when(jnp.logical_not(outer))
    def _():
        lax.fori_loop(jnp.where(upper, PARTS + 1, PARTS), 2 * PARTS, merge_more, 0)

    def result_out(h):
        return pltpu.make_async_copy(
            result.at[h], out_ref.at[pl.ds(h * part_rows, part_rows), :], result_sem.at[h]
        )

    for h in range(PARTS):
        to_pair(h).wait_recv()
        total = final[h] + from_peer[PARTS + h].astype(jnp.float32)
        to_place(z, h).wait_recv()
        result[h] = (total + from_peer[h].astype(jnp.float32)).astype(out_ref.dtype)
        result_out(h).start()

    inward.drain()
    outward.drain()
    for h in range(PARTS):
        result_out(h).wait()

    def drain(place):
        if place < places - 1:
            sent_tokens(0, place + 1).wait_send()
        if place > 0:
            sent_tokens(1, places - place).wait_send()

    each_place(drain)
    sent_tokens(2, places).wait_send()
    remote(to_mate, from_mate, half_send.at[0], half_recv.at[0], {"tp": mate}).wait_send()
    sent = to_peer.at[pl.ds(0, (places - 1) * PARTS)]
    remote(sent, sent, peer_send.at[0], peer_recv.at[0], {"sp": pair}).wait_send()


def fused(
    tokens,
    norm_gain,
    pool_input,
    query_weight,
    key_weight,
    value_weight,
    pool_map,
    pool_scale,
    head_gain,
    diff_lambda,
    out_pool,
    out_heads,
):
    places = lax.axis_size("sp")
    groups = lax.axis_size("fs")
    row_count, model = tokens.shape[1], tokens.shape[2]
    length = places * row_count
    half = HEAD_DIM // 2
    freqs = np.float32(1.0) / np.float32(THETA) ** (
        np.arange(half, dtype=np.float32) * np.float32(2.0) / np.float32(HEAD_DIM)
    )
    freqs = jnp.asarray(np.concatenate([freqs, freqs])[None, :], jnp.float32)
    group_count = pool_map.shape[0]
    half_out = model // 2
    hbm = pl.BlockSpec(memory_space=pl.ANY)
    dma = pltpu.SemaphoreType.DMA
    low = jnp.bfloat16

    def gather_sems(count):
        return [
            dma((count,)),
            dma((places,)),
            dma((places,)),
            dma((2,)),
            dma((2, places)),
            dma((2,)),
        ]

    out = pl.pallas_call(
        lambda *refs: fused_kernel(places, groups, *refs),
        out_shape=jax.ShapeDtypeStruct((row_count, half_out), low),
        in_specs=[hbm] * 13,
        out_specs=hbm,
        scratch_shapes=[
            pltpu.VMEM((row_count // 2, model), low),
            pltpu.VMEM((GROUP_DIM, GROUP_DIM), low),
            pltpu.VMEM((1, model), jnp.float32),
            pltpu.VMEM((1, HEAD_DIM), jnp.float32),
            pltpu.VMEM((group_count, 1, GROUP_DIM), jnp.float32),
            pltpu.VMEM((1, 2 * HEAD_DIM), jnp.float32),
            pltpu.SMEM(diff_lambda.shape, jnp.float32),
            pltpu.VMEM((length, HEAD_DIM), jnp.float32),
            pltpu.VMEM((length, HEAD_DIM), jnp.float32),
            pltpu.VMEM((length, model), low),
            pltpu.VMEM((4, model, GROUP_DIM), low),
            pltpu.VMEM((2, GROUP_DIM, model), low),
            pltpu.VMEM((length, GROUP_DIM), low),
            pltpu.VMEM((length, GROUP_DIM), low),
            pltpu.VMEM((length, GROUP_DIM), low),
            pltpu.VMEM((length + 16, GROUP_DIM), low),
            pltpu.VMEM((places * PARTS, row_count // PARTS, 2 * GROUP_DIM), low),
            pltpu.VMEM((2, row_count // PARTS, half_out), jnp.float32),
            pltpu.VMEM((places * PARTS, row_count // PARTS, half_out), low),
            pltpu.VMEM((places * PARTS, row_count // PARTS, half_out), low),
            pltpu.VMEM((2 * PARTS, row_count // PARTS, half_out), jnp.float32),
            pltpu.VMEM((places * PARTS, row_count // PARTS, half_out), low),
            pltpu.VMEM((2 * PARTS, row_count // PARTS, half_out), low),
            pltpu.VMEM((2 * PARTS, row_count // PARTS, half_out), low),
            pltpu.VMEM((PARTS, row_count // PARTS, half_out), jnp.float32),
            pltpu.VMEM((PARTS, row_count // PARTS, half_out), low),
            dma((PARTS,)),
            dma((2,)),
            dma((5,)),
            *gather_sems(4),
            *gather_sems(2),
            dma((3,)),
            dma((places, PIECES)),
            dma((places,)),
            dma((1,)),
            dma((places * PARTS,)),
            dma((1,)),
            dma((2 * PARTS,)),
            dma((2 * PARTS,)),
        ],
        compiler_params=pltpu.CompilerParams(
            collective_id=0, has_side_effects=True, vmem_limit_bytes=56 * 1024 * 1024
        ),
    )(
        tokens[0],
        norm_gain.reshape(1, model),
        freqs,
        pool_input,
        query_weight,
        key_weight,
        value_weight,
        pool_map,
        pool_scale.reshape(group_count, 1, GROUP_DIM),
        head_gain.reshape(1, 2 * HEAD_DIM),
        diff_lambda,
        out_pool,
        out_heads,
    )
    return out[None]


def solution(mesh):
    placed = (
        P("fs", "sp", None),
        P(),
        P(("sp", "fs"), "tp"),
        P(("sp", "fs"), "tp"),
        P(("sp", "fs"), "tp"),
        P(("sp", "fs"), "tp"),
        P("tp", None, None),
        P("tp"),
        P(),
        P(),
        P("tp", ("sp", "fs")),
        P("tp", ("sp", "fs")),
    )
    shape = dict(mesh.shape)

    def body(tokens, *rest):
        head_count = rest[3].shape[1] // (2 * HEAD_DIM)
        group_count = rest[5].shape[0]
        fits = (
            shape["fs"] == 4
            and shape["tp"] == 2
            and shape["sp"] == head_count == group_count == 4
            and tokens.shape[0] == 1
        )
        return (fused if fits else local)(tokens, *rest)

    return jax.shard_map(
        body, mesh=mesh, in_specs=placed, out_specs=P("fs", "sp", "tp"), check_vma=False
    )
```
